128 devices in a mesh: sp: 16 (over z, x), tp: 4 (over y), dp: 2 (over core).
Axes of the slice: x: 4, y: 4, z: 4, core: 2. Of those that a mesh axis runs over, the one named last changes fastest.
Arguments:
- latent_tokens: bfloat16 [16384, 2048], P(('dp', 'sp', 'tp')), parts along dimension 0, may hold values from -6 to 6
- condition: bfloat16 [4096], P(('dp', 'sp')), parts along dimension 0, may hold values from -6 to 6
- shift_weight: bfloat16 [2048, 2048], P('sp', 'tp'), may hold values from -0.125 to 0.125
- scale_weight: bfloat16 [2048, 2048], P('sp', 'tp'), may hold values from -0.125 to 0.125
- gate_weight: bfloat16 [2048, 2048], P('sp', 'tp'), may hold values from -0.125 to 0.125
- norm_gain: float32 [2048], replicated, may hold values from 0.1 to 1.9
- query_down: bfloat16 [2048, 512], replicated, may hold values from -0.125 to 0.125
- query_gain: float32 [512], replicated, may hold values from 0.1 to 1.9
- kv_down: bfloat16 [2048, 256], replicated, may hold values from -0.125 to 0.125
- kv_gain: float32 [256], replicated, may hold values from 0.1 to 1.9
- rope_down: bfloat16 [2048, 32], replicated, may hold values from -0.125 to 0.125
- query_up: bfloat16 [512, 1536], P(None, 'tp'), may hold values from -0.25 to 0.25
- key_up: bfloat16 [256, 1024], P(None, 'tp'), may hold values from -0.375 to 0.375
- value_up: bfloat16 [256, 1024], P(None, 'tp'), may hold values from -0.375 to 0.375
- query_norm_gain: float32 [96], replicated, may hold values from 0.47 to 16
- key_norm_gain: float32 [96], replicated, may hold values from 0.47 to 16
- out_weight: bfloat16 [1024, 2048], P('tp'), may hold values from -0.1875 to 0.1875
- context_latent: bfloat16 [2048, 256], P(('dp', 'sp')), parts along dimension 0, may hold values from -6 to 6
- context_rope: bfloat16 [2048, 32], P(('dp', 'sp')), parts along dimension 0, may hold values from -6 to 6
- context_lift: float32 [16], P('tp'), may hold values from 0 to 2
Outputs:
- output: bfloat16 [16384, 2048], P(('dp', 'sp', 'tp')), parts along dimension 0
The draws below stay inside these ranges and needn't reach their ends.
There are 2 independent parts, one for each index of `dp`. The reference program is written for one: setup_inputs(seed, part) draws one part's arguments, and reference() takes and returns one part's arrays. A program takes and returns all parts, laid end to end along the dimension named above; an argument that names none is the same for every part. Nothing has to cross between parts.
All inputs are finite; a program needn't handle non-finite values.
Results may differ from the reference program's by a relative error of at most 0.015.
The reference program's roundings to bfloat16 on the way count: a program that leaves them out, or rounds other values in their place, can miss the bound.
Values may be sent and summed in bfloat16 or wider, within the bound.
A program may use at most 128 MiB of HBM per device.

```python
import jax
import jax.numpy as jnp
from jax import lax

D_MODEL = 2048
HEADS = 16
NOPE_DIM = 64
ROPE_DIM = 32
VALUE_DIM = 64
QK_DIM = 96
Q_RANK = 512
KV_RANK = 256
GRID_W = 64
CONTEXT = 1024
TOKENS = 8192
N_TP = 4


def gain_draw(key, salt):
    own_key = jax.random.fold_in(key, salt)
    normal_values = jax.random.normal(own_key, (QK_DIM,), jnp.float32)
    return 1.7 * (1.0 + 0.18 * jnp.clip(normal_values, -4.0, 4.0))


def draw_query_norm_gain(key, part):
    return gain_draw(key, 31)


def draw_key_norm_gain(key, part):
    return gain_draw(key, 57)


def block_scale(rng, dims, cuts, least, top_value):
    loudness = 1.0
    for dim, shards_of in cuts:
        heights = jax.random.uniform(jax.random.fold_in(jax.random.fold_in(rng, 6), dim), (shards_of,), jnp.float32, least / len(cuts), top_value / len(cuts))
        loudness = loudness * jnp.repeat(jnp.exp(heights), dims[dim] // shards_of).reshape((-1,) + (1,) * (len(dims) - 1 - dim))
    return loudness


def bell_draw(key, shape, spread, bound, shards=(), kind=jnp.bfloat16):
    drawn = spread * jax.random.normal(key, shape, jnp.float32)
    if shards:
        drawn = drawn * block_scale(key, shape, shards, -0.22, 0.18)
    return jnp.clip(drawn, -bound, bound).astype(kind)


def setup_inputs(seed: int = 0, part: int = 0) -> dict:
    key_of = jax.random.split(jax.random.key(seed), 21)
    part_keys = jax.random.split(jax.random.fold_in(key_of[20], part), 21)
    latent_tokens = bell_draw(part_keys[0], (TOKENS, D_MODEL), 1.0, 6.0, ((0, 64),))
    condition = bell_draw(part_keys[1], (D_MODEL,), 1.0, 6.0, ((0, 16),))
    shift_weight = bell_draw(key_of[2], (D_MODEL, D_MODEL), D_MODEL ** -0.5, 0.125, ((0, 16), (1, 4)))
    scale_weight = bell_draw(key_of[3], (D_MODEL, D_MODEL), D_MODEL ** -0.5, 0.125, ((0, 16), (1, 4)))
    gate_weight = bell_draw(key_of[4], (D_MODEL, D_MODEL), D_MODEL ** -0.5, 0.125, ((0, 16), (1, 4)))
    norm_gain = jnp.clip(1.0 + 0.18 * jax.random.normal(key_of[5], (D_MODEL,), jnp.float32), 0.1, 1.9)
    query_down = bell_draw(key_of[6], (D_MODEL, Q_RANK), D_MODEL ** -0.5, 0.125)
    query_gain = jnp.clip(1.0 + 0.18 * jax.random.normal(key_of[7], (Q_RANK,), jnp.float32), 0.1, 1.9)
    kv_down = bell_draw(key_of[8], (D_MODEL, KV_RANK), D_MODEL ** -0.5, 0.125)
    kv_gain = jnp.clip(1.0 + 0.18 * jax.random.normal(key_of[9], (KV_RANK,), jnp.float32), 0.1, 1.9)
    rope_down = bell_draw(key_of[10], (D_MODEL, ROPE_DIM), D_MODEL ** -0.5, 0.125)
    query_up = bell_draw(key_of[11], (Q_RANK, HEADS * QK_DIM), Q_RANK ** -0.5, 0.25, ((1, 4),))
    key_up = bell_draw(key_of[12], (KV_RANK, HEADS * NOPE_DIM), KV_RANK ** -0.5, 0.375, ((1, 4),))
    value_up = bell_draw(key_of[13], (KV_RANK, HEADS * VALUE_DIM), KV_RANK ** -0.5, 0.375, ((1, 4),))
    query_norm_gain = draw_query_norm_gain(jax.random.fold_in(key_of[20], 71), part)
    key_norm_gain = draw_key_norm_gain(jax.random.fold_in(key_of[20], 71), part)
    out_weight = bell_draw(key_of[16], (HEADS * VALUE_DIM, D_MODEL), (HEADS * VALUE_DIM) ** -0.5, 0.1875, ((0, 4),))
    context_latent = bell_draw(part_keys[17], (CONTEXT, KV_RANK), 1.0, 6.0, ((0, 16),))
    context_rope = bell_draw(part_keys[18], (CONTEXT, ROPE_DIM), 1.0, 6.0, ((0, 16),))
    context_lift = jnp.clip(2.0 * jax.random.uniform(key_of[19], (HEADS,), jnp.float32) ** block_scale(key_of[19], (HEADS,), ((0, 4),), -0.2, 0.2), 0.0, 2.0)
    return {"latent_tokens": latent_tokens, "condition": condition, "shift_weight": shift_weight, "scale_weight": scale_weight, "gate_weight": gate_weight, "norm_gain": norm_gain, "query_down": query_down, "query_gain": query_gain, "kv_down": kv_down, "kv_gain": kv_gain, "rope_down": rope_down, "query_up": query_up, "key_up": key_up, "value_up": value_up, "query_norm_gain": query_norm_gain, "key_norm_gain": key_norm_gain, "out_weight": out_weight, "context_latent": context_latent, "context_rope": context_rope, "context_lift": context_lift}


EPS = 1e-06
THETA = 10000.0

def rms_scaled(values, gain_vector):
    mean_square = lax.optimization_barrier(jnp.mean(values * values, axis=-1, keepdims=True))
    return values * lax.rsqrt(mean_square + EPS) * gain_vector

def rotate(rope_part, positions):
    row_count = rope_part.shape[0]
    freq_count = ROPE_DIM // 4
    inverse = THETA ** (-4.0 * jnp.arange(freq_count, dtype=jnp.float32) / ROPE_DIM)
    grid_row = (positions // GRID_W).astype(jnp.float32)
    grid_col = (positions % GRID_W).astype(jnp.float32)
    angles = jnp.stack([grid_row[:, None] * inverse, grid_col[:, None] * inverse], axis=1)
    cosine_table = jnp.cos(angles)[:, None]
    sine_table = jnp.sin(angles)[:, None]
    split_rows = rope_part.reshape(row_count, rope_part.shape[1], 2, 2, freq_count)
    first_half = split_rows[:, :, :, 0]
    second_half = split_rows[:, :, :, 1]
    turned = jnp.stack([first_half * cosine_table - second_half * sine_table, second_half * cosine_table + first_half * sine_table], axis=3)
    return turned.reshape(rope_part.shape)

def expand(latent_rows, rope_rows, key_up, value_up, key_norm_gain):
    row_count = latent_rows.shape[0]
    nope_part = jnp.dot(latent_rows, key_up, preferred_element_type=jnp.float32).reshape(row_count, HEADS, NOPE_DIM)
    value_rows = jnp.dot(latent_rows, value_up, preferred_element_type=jnp.float32).astype(jnp.bfloat16)
    shared = jnp.broadcast_to(rope_rows.astype(jnp.float32)[:, None, :], (row_count, HEADS, ROPE_DIM))
    normal_keys = rms_scaled(jnp.concatenate([nope_part, shared], axis=-1), key_norm_gain)
    return (normal_keys, value_rows.reshape(row_count, HEADS, VALUE_DIM))

def reference(latent_tokens, condition, shift_weight, scale_weight, gate_weight, norm_gain, query_down, query_gain, kv_down, kv_gain, rope_down, query_up, key_up, value_up, query_norm_gain, key_norm_gain, out_weight, context_latent, context_rope, context_lift):
    activated = jax.nn.silu(condition.astype(jnp.float32)).astype(jnp.bfloat16)[None]
    mod_shift = jnp.dot(activated, shift_weight, preferred_element_type=jnp.float32)[0]
    mod_scale = jnp.dot(activated, scale_weight, preferred_element_type=jnp.float32)[0]
    mod_gate = jnp.dot(activated, gate_weight, preferred_element_type=jnp.float32)[0]
    token_values = latent_tokens.astype(jnp.float32)
    normed = (rms_scaled(token_values, norm_gain) * (1.0 + mod_scale) + mod_shift).astype(jnp.bfloat16)
    query_latent = rms_scaled(jnp.dot(normed, query_down, preferred_element_type=jnp.float32), query_gain).astype(jnp.bfloat16)
    key_latent = rms_scaled(jnp.dot(normed, kv_down, preferred_element_type=jnp.float32), kv_gain).astype(jnp.bfloat16)
    rope_key = jnp.dot(normed, rope_down, preferred_element_type=jnp.float32).astype(jnp.bfloat16)
    positions = jnp.arange(TOKENS, dtype=jnp.int32)
    query_heads = rms_scaled(jnp.dot(query_latent, query_up, preferred_element_type=jnp.float32).reshape(TOKENS, HEADS, QK_DIM), query_norm_gain)
    queries = jnp.concatenate([query_heads[..., :NOPE_DIM], rotate(query_heads[..., NOPE_DIM:], positions)], axis=-1).astype(jnp.bfloat16)
    latent_normal, latent_values = expand(key_latent, rope_key, key_up, value_up, key_norm_gain)
    latent_keys = jnp.concatenate([latent_normal[..., :NOPE_DIM], rotate(latent_normal[..., NOPE_DIM:], positions)], axis=-1).astype(jnp.bfloat16)
    context_normal, context_values = expand(context_latent, context_rope, key_up, value_up, key_norm_gain)
    context_keys = context_normal.astype(jnp.bfloat16)
    all_keys = jnp.concatenate([latent_keys, context_keys], axis=0)
    all_values = jnp.concatenate([latent_values, context_values], axis=0)
    is_context = jnp.arange(TOKENS + CONTEXT, dtype=jnp.int32) >= TOKENS

    def one_head(inputs):
        query_head, key_head, value_head, lift_head = inputs
        scores = jnp.dot(query_head, key_head.T, preferred_element_type=jnp.float32) * QK_DIM ** (-0.5)
        scores = scores + jnp.where(is_context, lift_head, jnp.zeros((), jnp.float32))[None, :]
        top_score = lax.optimization_barrier(jnp.max(scores, axis=-1, keepdims=True))
        weights = jnp.exp(scores - top_score)
        weight_total = lax.optimization_barrier(jnp.sum(weights, axis=-1, keepdims=True))
        summed = jnp.dot(weights.astype(jnp.bfloat16), value_head, preferred_element_type=jnp.float32)
        return (summed / weight_total).astype(jnp.bfloat16)
    attended = lax.map(one_head, (jnp.transpose(queries, (1, 0, 2)), jnp.transpose(all_keys, (1, 0, 2)), jnp.transpose(all_values, (1, 0, 2)), context_lift))
    attended = jnp.transpose(attended, (1, 0, 2)).reshape(TOKENS, HEADS * VALUE_DIM)
    group_width = HEADS // N_TP * VALUE_DIM
    mixed_sum = jnp.zeros((TOKENS, D_MODEL), jnp.float32)
    for head_group in range(N_TP):
        group_term = jnp.dot(attended[:, head_group * group_width:(head_group + 1) * group_width], out_weight[head_group * group_width:(head_group + 1) * group_width], preferred_element_type=jnp.float32)
        rounded = lax.optimization_barrier(group_term.astype(jnp.bfloat16))
        mixed_sum = mixed_sum + rounded.astype(jnp.float32)
    return (token_values + mod_gate * mixed_sum).astype(jnp.bfloat16)
```

```python
import functools

import jax
import jax.numpy as jnp
from jax import lax
from jax.experimental import pallas as pl
from jax.experimental.pallas import tpu as pltpu
from jax.sharding import PartitionSpec as P

NOPE_DIM = 64
ROPE_DIM = 32
VALUE_DIM = 64
QK_DIM = 96
GRID_W = 64
EPS = 1e-06
THETA = 10000.0
LOG2E = 1.4426950408889634

F32 = jnp.float32
BF16 = jnp.bfloat16
MESH = pl.DeviceIdType.MESH
VMEM = pl.BlockSpec(memory_space=pltpu.VMEM)


def remote(src, dst, send, recv, sp, tp):
    return pltpu.make_async_remote_copy(
        src_ref=src, dst_ref=dst, send_sem=send, recv_sem=recv,
        device_id={"sp": sp, "tp": tp}, device_id_type=MESH,
    )


def greet(peers):
    barrier = pltpu.get_barrier_semaphore()
    for sp, tp in peers:
        pl.semaphore_signal(barrier, inc=1, device_id={"sp": sp, "tp": tp}, device_id_type=MESH)
    pl.semaphore_wait(barrier, len(peers))


def modulation_kernel(
    part_ref, lat_ref, rope_ref, mod_ref, clat_ref, crope_ref, slots,
    s_part, r_part, s_lat, r_lat, s_rope, r_rope, s_mod, r_mod, local_sem,
):
    sp, tp = lax.axis_index("sp"), lax.axis_index("tp")
    greet(
        [(lax.rem(sp + r, 16), tp) for r in range(1, 16)]
        + [(sp, lax.rem(tp + r, 4)) for r in range(1, 4)]
    )
    parts, wide = [], []
    for r in range(1, 16):
        to = lax.rem(sp + r, 16)
        c = remote(part_ref, slots.at[r], s_part.at[r], r_part.at[r], to, tp)
        c.start()
        parts.append(c)
    for r in range(1, 16):
        to = lax.rem(sp + r, 16)
        a = remote(lat_ref, clat_ref.at[r], s_lat.at[r], r_lat.at[r], to, tp)
        a.start()
        b = remote(rope_ref, crope_ref.at[r], s_rope.at[r], r_rope.at[r], to, tp)
        b.start()
        wide += [a, b]
    own = [
        pltpu.make_async_copy(lat_ref, clat_ref.at[0], local_sem.at[0]),
        pltpu.make_async_copy(rope_ref, crope_ref.at[0], local_sem.at[1]),
    ]
    for c in own:
        c.start()
    total = part_ref[...]
    for r in range(1, 16):
        parts[r - 1].wait_recv()
        total = total + slots[r]
    mod_ref[tp] = total
    mods = []
    for r in range(1, 4):
        c = remote(mod_ref.at[tp], mod_ref.at[tp], s_mod.at[r], r_mod.at[r], sp, lax.rem(tp + r, 4))
        c.start()
        mods.append(c)
    for c in mods:
        c.wait()
    for c in parts:
        c.wait_send()
    for c in wide:
        c.wait()
    for c in own:
        c.wait()


def modulation(part, lat, rope):
    dma = pltpu.SemaphoreType.DMA
    return pl.pallas_call(
        modulation_kernel,
        out_shape=(
            jax.ShapeDtypeStruct((4, 16, 128), F32),
            jax.ShapeDtypeStruct((16, 64, 256), BF16),
            jax.ShapeDtypeStruct((16, 64, 32), BF16),
        ),
        in_specs=[VMEM] * 3,
        out_specs=(VMEM,) * 3,
        scratch_shapes=[
            pltpu.VMEM((16, 16, 128), F32),
            dma((16,)), dma((16,)), dma((16,)), dma((16,)), dma((16,)), dma((16,)),
            dma((4,)), dma((4,)), dma((2,)),
        ],
        compiler_params=pltpu.CompilerParams(collective_id=0, has_side_effects=True),
        cost_estimate=pl.CostEstimate(flops=20_000_000, bytes_accessed=2_000_000, transcendentals=0),
        name="modulation",
    )(part, lat, rope)


def turned(rows, cos_ref, sin_ref):
    out = []
    for a in range(2):
        u, w = rows[16 * a : 16 * a + 8], rows[16 * a + 8 : 16 * a + 16]
        c, s = cos_ref[a], sin_ref[a]
        out += [u * c - w * s, w * c + u * s]
    return jnp.concatenate(out, axis=0)


def expand_kernel(
    x_ref, mod_ref, ng_ref, qd_ref, kvd_ref, rd_ref, qgain_ref, kvgain_ref, cos_ref, sin_ref, qg_ref, kg_ref,
    qw_ref, kw_ref, vw_ref,
    qa1, qa2, qa3, qb1, qb2, qb3, ka1, ka2, ka3, kb1, kb2, kb3, out_ref,
):
    core = lax.axis_index("dp")
    v = x_ref[...].astype(F32)
    ms = jnp.mean(v * v, axis=-1, keepdims=True)
    normed = v * lax.rsqrt(ms + EPS) * ng_ref[...]
    normed = (normed * (1.0 + mod_ref[1:2, :]) + mod_ref[0:1, :]).astype(BF16)

    def scaled(w_ref, gain_ref):
        y = jnp.dot(normed, w_ref[...], preferred_element_type=F32)
        m = jnp.mean(y * y, axis=-1, keepdims=True)
        return (y * lax.rsqrt(m + EPS) * gain_ref[...]).astype(BF16)

    ql = scaled(qd_ref, qgain_ref)
    kl = scaled(kvd_ref, kvgain_ref)
    rk = jnp.dot(normed, rd_ref[...], preferred_element_type=F32).astype(BF16).astype(F32)
    rk = rk.T[:ROPE_DIM]
    rk_square = jnp.sum(rk * rk, axis=0, keepdims=True)
    first = core == 0
    q_mine = jnp.where(first, ql[:, :256], ql[:, 256:])
    q_other = jnp.where(first, ql[:, 256:], ql[:, :256])
    k_mine = jnp.where(first, kl[:, :128], kl[:, 128:])
    k_other = jnp.where(first, kl[:, 128:], kl[:, :128])

    def dot(a, b):
        return jnp.dot(a, b, preferred_element_type=F32)

    for k in range(4):
        if k == 0:
            q = dot(ql, qw_ref[...])
            kn = dot(kl, kw_ref[...])
            vv = dot(kl, vw_ref[...])
        else:
            a, b = (qa1, qa2, qa3)[k - 1], (qb1, qb2, qb3)[k - 1]
            q = dot(q_mine, a[...]) + dot(q_other, b[...])
            a, b = (ka1, ka2, ka3)[k - 1], (kb1, kb2, kb3)[k - 1]
            both = dot(k_mine, a[...]) + dot(k_other, b[...])
            kn, vv = both[:, :256], both[:, 256:]
        q, kn, vv = q.T, kn.T, vv.T
        for j in range(4):
            qh = q[QK_DIM * j : QK_DIM * (j + 1)]
            inv = lax.rsqrt(jnp.sum(qh * qh, axis=0, keepdims=True) * (1.0 / QK_DIM) + EPS)
            qh = qh * inv * qg_ref[...]
            qh = jnp.concatenate([qh[:NOPE_DIM], turned(qh[NOPE_DIM:], cos_ref, sin_ref)], axis=0)
            out_ref[k, j, 0:QK_DIM, :] = qh.astype(BF16)
            kh = kn[NOPE_DIM * j : NOPE_DIM * (j + 1)]
            square = jnp.sum(kh * kh, axis=0, keepdims=True) + rk_square
            inv = lax.rsqrt(square * (1.0 / QK_DIM) + EPS)
            kr = turned(rk * inv * kg_ref[NOPE_DIM:, :], cos_ref, sin_ref)
            kh = kh * inv * kg_ref[:NOPE_DIM, :]
            out_ref[k, j, QK_DIM : QK_DIM + NOPE_DIM, :] = kh.astype(BF16)
            out_ref[k, j, QK_DIM + NOPE_DIM : 2 * QK_DIM, :] = kr.astype(BF16)
            out_ref[k, j, 2 * QK_DIM : 256, :] = vv[VALUE_DIM * j : VALUE_DIM * (j + 1)].astype(BF16)


def expand(*args):
    return pl.pallas_call(
        expand_kernel,
        out_shape=jax.ShapeDtypeStruct((4, 4, 256, 128), BF16),
        in_specs=[VMEM] * len(args),
        out_specs=VMEM,
        cost_estimate=pl.CostEstimate(flops=800_000_000, bytes_accessed=6_000_000, transcendentals=10_000),
        name="expand",
    )(*args)


CHUNK = 1024


def attend_kernel(
    qkv_ref, clat_ref, crope_ref, kuh_ref, vuh_ref, kgrow_ref, lift_ref, out_ref,
    q_in, kvs, q_s, k_s, v_s, m_s, acc_s,
    s_q, r_q, s_kv, r_kv, s_up, r_up, s_down, r_down, s_fup, r_fup, s_fdown, r_fdown, local_sem,
):
    sp, tp = lax.axis_index("sp"), lax.axis_index("tp")
    z, x = sp // 4, lax.rem(sp, 4)

    def at(dz, dx, dy):
        return (lax.rem(z + dz, 4) * 4 + lax.rem(x + dx, 4), lax.rem(tp + dy, 4))

    plane = [(dx, dy) for dy in range(4) for dx in range(4)]
    up, down = at(1, 0, 0), at(3, 0, 0)
    greet([at(0, dx, dy) for dx, dy in plane[1:]] + [up, down])
    q_copies, kv_copies = [None], [None]
    for r in range(1, 16):
        dx, dy = plane[r]
        head = lax.rem(x + dx, 4)
        c = remote(qkv_ref.at[dy, head, 0:96], q_in.at[r], s_q.at[r], r_q.at[r], *at(0, dx, dy))
        c.start()
        q_copies.append(c)
    for r in range(1, 16):
        dx, dy = plane[r]
        head = lax.rem(x + dx, 4)
        c = remote(qkv_ref.at[dy, head, 96:256], kvs.at[0, r], s_kv.at[r], r_kv.at[r], *at(0, dx, dy))
        c.start()
        kv_copies.append(c)
    own_q = pltpu.make_async_copy(qkv_ref.at[0, x, 0:96], q_in.at[0], local_sem.at[0])
    own_kv = pltpu.make_async_copy(qkv_ref.at[0, x, 96:256], kvs.at[0, 0], local_sem.at[1])
    own_q.start()
    own_kv.start()

    clat = clat_ref[...].reshape(CHUNK, 256)
    kn = jnp.dot(clat, kuh_ref[...], preferred_element_type=F32)
    rope = crope_ref[...].reshape(CHUNK, ROPE_DIM).astype(F32)
    key = jnp.concatenate([kn[:, :NOPE_DIM], rope, jnp.zeros((CHUNK, 32), F32)], axis=1)
    inv = lax.rsqrt(jnp.sum(key * key, axis=1, keepdims=True) * (1.0 / QK_DIM) + EPS)
    k_s[...] = (key * inv * kgrow_ref[...]).astype(BF16)
    vv = jnp.dot(clat, vuh_ref[...], preferred_element_type=F32).T
    v_s[0:VALUE_DIM, :] = vv[:VALUE_DIM].astype(BF16)
    v_s[VALUE_DIM:80, :] = jnp.ones((16, CHUNK), BF16)

    for t in range(8):
        q_s[t, QK_DIM:128, :] = jnp.zeros((32, 256), BF16)
    own_q.wait()
    q_s[0, 0:QK_DIM, 0:128] = q_in[0]
    for r in range(1, 16):
        q_copies[r].wait_recv()
        q_s[r // 2, 0:QK_DIM, 128 * (r % 2) : 128 * (r % 2) + 128] = q_in[r]

    def fold(first):
        def one_tile(t, carry):
            s = jnp.dot(k_s[...], q_s[t], preferred_element_type=F32)
            top = jnp.max(s, axis=0, keepdims=True)
            if first:
                new = top + lift_ref[...]
                p = jnp.exp2(s - top).astype(BF16)
                acc_s[t] = jnp.dot(v_s[...], p, preferred_element_type=F32)
            else:
                old = m_s[t]
                new = jnp.maximum(old, top)
                p = jnp.exp2(s - new).astype(BF16)
                acc_s[t] = acc_s[t] * jnp.exp2(old - new) + jnp.dot(v_s[...], p, preferred_element_type=F32)
            m_s[t] = new
            return carry

        lax.fori_loop(0, 8, one_tile, 0)

    def take(slot, half):
        for i in range(8):
            block = kvs[slot, 8 * half + i]
            rows = pl.ds(128 * i, 128)
            kt = jnp.concatenate([block[:QK_DIM].astype(F32), jnp.zeros((32, 128), F32)], axis=0)
            k_s[rows, :] = kt.T.astype(BF16)
            v_s[0:VALUE_DIM, 128 * i : 128 * i + 128] = block[QK_DIM:]
        fold(False)

    fold(True)

    ups, downs = [], []

    def spread(g):
        rows = pl.ds(4 * g, 4)
        c = remote(kvs.at[0, rows], kvs.at[1, rows], s_up.at[g], r_up.at[g], *up)
        c.start()
        ups.append(c)
        c = remote(kvs.at[0, rows], kvs.at[2, rows], s_down.at[g], r_down.at[g], *down)
        c.start()
        downs.append(c)

    own_kv.wait()
    for g in range(2):
        for r in range(max(1, 4 * g), 4 * g + 4):
            kv_copies[r].wait_recv()
        spread(g)
    take(0, 0)
    for g in range(2, 4):
        for r in range(4 * g, 4 * g + 4):
            kv_copies[r].wait_recv()
        spread(g)
    take(0, 1)
    far = []
    for g in range(2):
        rows = pl.ds(4 * g, 4)
        ups[g].wait_recv()
        c = remote(kvs.at[1, rows], kvs.at[3, rows], s_fup.at[g], r_fup.at[g], *up)
        c.start()
        far.append(c)
    take(1, 0)
    for g in range(2):
        downs[g].wait_recv()
    take(2, 0)
    for g in range(2, 4):
        rows = pl.ds(4 * g, 4)
        downs[g].wait_recv()
        c = remote(kvs.at[2, rows], kvs.at[3, rows], s_fdown.at[g], r_fdown.at[g], *down)
        c.start()
        far.append(c)
    take(2, 1)
    for g in range(2, 4):
        ups[g].wait_recv()
    take(1, 1)
    far[0].wait_recv()
    far[1].wait_recv()
    take(3, 0)
    far[2].wait_recv()
    far[3].wait_recv()
    take(3, 1)

    def finish(t, carry):
        acc = acc_s[t]
        o = (acc[:VALUE_DIM] / acc[VALUE_DIM : VALUE_DIM + 1]).astype(BF16)
        out_ref[2 * t] = o[:, :128]
        out_ref[2 * t + 1] = o[:, 128:]
        return carry

    lax.fori_loop(0, 8, finish, 0)
    for c in q_copies[1:] + kv_copies[1:] + ups + downs + far:
        c.wait_send()


def attend(*args):
    dma = pltpu.SemaphoreType.DMA
    return pl.pallas_call(
        attend_kernel,
        out_shape=jax.ShapeDtypeStruct((16, VALUE_DIM, 128), BF16),
        in_specs=[VMEM] * len(args),
        out_specs=VMEM,
        scratch_shapes=[
            pltpu.VMEM((16, QK_DIM, 128), BF16),
            pltpu.VMEM((4, 16, 160, 128), BF16),
            pltpu.VMEM((8, 128, 256), BF16),
            pltpu.VMEM((CHUNK, 128), BF16),
            pltpu.VMEM((80, CHUNK), BF16),
            pltpu.VMEM((8, 1, 256), F32),
            pltpu.VMEM((8, 80, 256), F32),
            dma((16,)), dma((16,)), dma((16,)), dma((16,)),
            dma((4,)), dma((4,)), dma((4,)), dma((4,)),
            dma((4,)), dma((4,)), dma((4,)), dma((4,)), dma((2,)),
        ],
        compiler_params=pltpu.CompilerParams(collective_id=1, has_side_effects=True),
        cost_estimate=pl.CostEstimate(
            flops=10_000_000_000, bytes_accessed=8_000_000, transcendentals=19_000_000
        ),
        name="attend",
    )(*args)


def output_kernel(att_ref, x_ref, gate_ref, wown, wa1, wa2, wa3, wb1, wb2, wb3, out_ref, slots, s_a, r_a, local_sem):
    sp, tp = lax.axis_index("sp"), lax.axis_index("tp")
    core = lax.axis_index("dp")
    z, x = sp // 4, lax.rem(sp, 4)

    def at(dx, dy):
        return (z * 4 + lax.rem(x + dx, 4), lax.rem(tp + dy, 4))

    plane = [(dx, dy) for dy in range(4) for dx in range(4)]
    greet([at(dx, dy) for dx, dy in plane[1:]])
    copies = []
    for r in range(1, 16):
        dx, dy = plane[r]
        c = remote(
            att_ref.at[r], slots.at[dy, pl.ds(x, 1)].at[0], s_a.at[r], r_a.at[r],
            *at((4 - dx) % 4, (4 - dy) % 4),
        )
        c.start()
        copies.append(c)
    own = pltpu.make_async_copy(att_ref.at[0], slots.at[0, x], local_sem)
    own.start()
    own.wait()
    for c in copies:
        c.wait_recv()
    mixed = None
    for k in range(4):
        if k == 0:
            att = slots[0].reshape(256, 128).astype(F32).T.astype(BF16)
            term = jnp.dot(att, wown[...], preferred_element_type=F32)
        else:
            a = slots[k, pl.ds(2 * core, 2)].reshape(128, 128).astype(F32).T.astype(BF16)
            b = slots[k, pl.ds(2 - 2 * core, 2)].reshape(128, 128).astype(F32).T.astype(BF16)
            wa, wb = (wa1, wa2, wa3)[k - 1], (wb1, wb2, wb3)[k - 1]
            term = jnp.dot(a, wa[...], preferred_element_type=F32)
            term = term + jnp.dot(b, wb[...], preferred_element_type=F32)
        term = term.astype(BF16).astype(F32)
        mixed = term if mixed is None else mixed + term
    out_ref[...] = (x_ref[...].astype(F32) + gate_ref[...] * mixed).astype(BF16)
    for c in copies:
        c.wait_send()


def output_step(*args):
    dma = pltpu.SemaphoreType.DMA
    return pl.pallas_call(
        output_kernel,
        out_shape=jax.ShapeDtypeStruct((128, 2048), BF16),
        in_specs=[VMEM] * len(args),
        out_specs=VMEM,
        scratch_shapes=[pltpu.VMEM((4, 4, VALUE_DIM, 128), BF16), dma((16,)), dma((16,)), dma(())],
        compiler_params=pltpu.CompilerParams(collective_id=2, has_side_effects=True),
        cost_estimate=pl.CostEstimate(flops=1_100_000_000, bytes_accessed=6_000_000, transcendentals=0),
        name="output_step",
    )(*args)


def ring_pieces(half):
    return [lax.ppermute(half, "tp", [((d + k) % 4, d) for d in range(4)]) for k in range(1, 4)]


def swapped(pieces):
    return [lax.ppermute(p, "dp", [(0, 1), (1, 0)]) for p in pieces]


def half_of(weight, core):
    rows = weight.shape[0] // 2
    return lax.dynamic_slice_in_dim(weight, core * rows, rows, axis=0)


def local(
    latent_tokens, condition, shift_weight, scale_weight, gate_weight, norm_gain, query_down, query_gain,
    kv_down, kv_gain, rope_down, query_up, key_up, value_up, query_norm_gain, key_norm_gain, out_weight,
    context_latent, context_rope, context_lift,
):
    sp, tp, core = lax.axis_index("sp"), lax.axis_index("tp"), lax.axis_index("dp")
    x = lax.rem(sp, 4)
    activated = jax.nn.silu(condition.astype(F32)).astype(BF16)[None]
    part = jnp.concatenate(
        [
            jnp.dot(activated, w, preferred_element_type=F32).reshape(4, 128)
            for w in (shift_weight, scale_weight, gate_weight)
        ]
        + [jnp.zeros((4, 128), F32)],
        axis=0,
    )
    q_mine = ring_pieces(half_of(query_up, core))
    kv_mine = ring_pieces(half_of(jnp.concatenate([key_up, value_up], axis=1), core))
    q_other, kv_other = swapped(q_mine), swapped(kv_mine)

    mods, clat, crope = modulation(part, context_latent, context_rope)
    mod = jnp.transpose(mods[:, :12].reshape(4, 3, 4, 128), (1, 0, 2, 3)).reshape(3, 2048)

    out_half, mod = lax.optimization_barrier((half_of(out_weight, core), mod))
    w_mine = ring_pieces(out_half)
    w_other = swapped(w_mine)

    positions = (sp * 4 + tp) * 128 + jnp.arange(128, dtype=jnp.int32)
    inverse = THETA ** (-4.0 * jnp.arange(8, dtype=F32) / ROPE_DIM)
    places = jnp.stack([(positions // GRID_W).astype(F32), (positions % GRID_W).astype(F32)])
    angles = places[:, None, :] * inverse[None, :, None]
    cosine, sine = jnp.cos(angles), jnp.sin(angles)
    query_scale = (query_norm_gain * (LOG2E * QK_DIM**-0.5)).reshape(QK_DIM, 1)
    qkv = expand(
        latent_tokens, mod, norm_gain.reshape(1, -1), query_down, kv_down,
        jnp.pad(rope_down, ((0, 0), (0, 96))), query_gain.reshape(1, -1), kv_gain.reshape(1, -1),
        cosine, sine, query_scale, key_norm_gain.reshape(QK_DIM, 1),
        query_up, key_up, value_up, *q_mine, *q_other, *kv_mine, *kv_other,
    )

    def own_head(w):
        return jnp.pad(lax.dynamic_slice_in_dim(w, x * 64, 64, axis=1), ((0, 0), (0, 64)))

    lift = lax.dynamic_slice_in_dim(context_lift, x, 1) * LOG2E
    att = attend(
        qkv, clat, crope, own_head(key_up), own_head(value_up),
        jnp.pad(key_norm_gain, (0, 32)).reshape(1, 128), jnp.broadcast_to(lift[None], (1, 256)),
    )
    return output_step(att, latent_tokens, mod[2:3], out_weight, *w_mine, *w_other)


def solution(mesh):
    in_specs = (
        P(("dp", "sp", "tp"), None), P(("dp", "sp")), P("sp", "tp"), P("sp", "tp"), P("sp", "tp"),
        P(), P(), P(), P(), P(), P(), P(None, "tp"), P(None, "tp"), P(None, "tp"), P(), P(),
        P("tp", None), P(("dp", "sp"), None), P(("dp", "sp"), None), P("tp"),
    )
    return jax.shard_map(
        local, mesh=mesh, in_specs=in_specs, out_specs=P(("dp", "sp", "tp"), None), check_vma=False
    )
```

```python
import functools

import jax
import jax.numpy as jnp
from jax import lax
from jax.experimental import pallas as pl
from jax.experimental.pallas import tpu as pltpu
from jax.sharding import PartitionSpec as P

NOPE_DIM = 64
ROPE_DIM = 32
VALUE_DIM = 64
QK_DIM = 96
GRID_W = 64
EPS = 1e-06
THETA = 10000.0
LOG2E = 1.4426950408889634

F32 = jnp.float32
BF16 = jnp.bfloat16
MESH = pl.DeviceIdType.MESH
VMEM = pl.BlockSpec(memory_space=pltpu.VMEM)


def remote(src, dst, send, recv, sp, tp):
    return pltpu.make_async_remote_copy(
        src_ref=src, dst_ref=dst, send_sem=send, recv_sem=recv,
        device_id={"sp": sp, "tp": tp}, device_id_type=MESH,
    )


def greet(peers):
    barrier = pltpu.get_barrier_semaphore()
    for sp, tp in peers:
        pl.semaphore_signal(barrier, inc=1, device_id={"sp": sp, "tp": tp}, device_id_type=MESH)
    pl.semaphore_wait(barrier, len(peers))


def modulation_kernel(
    part_ref, lat_ref, rope_ref, mod_ref, clat_ref, crope_ref, slots,
    s_part, r_part, s_lat, r_lat, s_rope, r_rope, s_mod, r_mod, local_sem,
):
    sp, tp = lax.axis_index("sp"), lax.axis_index("tp")
    greet(
        [(lax.rem(sp + r, 16), tp) for r in range(1, 16)]
        + [(sp, lax.rem(tp + r, 4)) for r in range(1, 4)]
    )
    parts, wide = [], []
    for r in range(1, 16):
        to = lax.rem(sp + r, 16)
        c = remote(part_ref, slots.at[r], s_part.at[r], r_part.at[r], to, tp)
        c.start()
        parts.append(c)
    for r in range(1, 16):
        to = lax.rem(sp + r, 16)
        a = remote(lat_ref, clat_ref.at[r], s_lat.at[r], r_lat.at[r], to, tp)
        a.start()
        b = remote(rope_ref, crope_ref.at[r], s_rope.at[r], r_rope.at[r], to, tp)
        b.start()
        wide += [a, b]
    own = [
        pltpu.make_async_copy(lat_ref, clat_ref.at[0], local_sem.at[0]),
        pltpu.make_async_copy(rope_ref, crope_ref.at[0], local_sem.at[1]),
    ]
    for c in own:
        c.start()
    total = part_ref[...]
    for r in range(1, 16):
        parts[r - 1].wait_recv()
        total = total + slots[r]
    mod_ref[tp] = total
    mods = []
    for r in range(1, 4):
        c = remote(mod_ref.at[tp], mod_ref.at[tp], s_mod.at[r], r_mod.at[r], sp, lax.rem(tp + r, 4))
        c.start()
        mods.append(c)
    for c in mods:
        c.wait()
    for c in parts:
        c.wait_send()
    for c in wide:
        c.wait()
    for c in own:
        c.wait()


def modulation(part, lat, rope):
    dma = pltpu.SemaphoreType.DMA
    return pl.pallas_call(
        modulation_kernel,
        out_shape=(
            jax.ShapeDtypeStruct((4, 16, 128), F32),
            jax.ShapeDtypeStruct((16, 64, 256), BF16),
            jax.ShapeDtypeStruct((16, 64, 32), BF16),
        ),
        in_specs=[VMEM] * 3,
        out_specs=(VMEM,) * 3,
        scratch_shapes=[
            pltpu.VMEM((16, 16, 128), F32),
            dma((16,)), dma((16,)), dma((16,)), dma((16,)), dma((16,)), dma((16,)),
            dma((4,)), dma((4,)), dma((2,)),
        ],
        compiler_params=pltpu.CompilerParams(collective_id=0, has_side_effects=True),
        cost_estimate=pl.CostEstimate(flops=20_000_000, bytes_accessed=2_000_000, transcendentals=0),
        name="modulation",
    )(part, lat, rope)


def turned(rows, cos_ref, sin_ref):
    out = []
    for a in range(2):
        u, w = rows[16 * a : 16 * a + 8], rows[16 * a + 8 : 16 * a + 16]
        c, s = cos_ref[a], sin_ref[a]
        out += [u * c - w * s, w * c + u * s]
    return jnp.concatenate(out, axis=0)


def expand_kernel(
    x_ref, mod_ref, ng_ref, qd_ref, kvd_ref, rd_ref, qgain_ref, kvgain_ref, cos_ref, sin_ref, qg_ref, kg_ref,
    qw_ref, kw_ref, vw_ref,
    qa1, qa2, qa3, qb1, qb2, qb3, ka1, ka2, ka3, kb1, kb2, kb3, out_ref,
):
    core = lax.axis_index("dp")
    v = x_ref[...].astype(F32)
    ms = jnp.mean(v * v, axis=-1, keepdims=True)
    normed = v * lax.rsqrt(ms + EPS) * ng_ref[...]
    normed = (normed * (1.0 + mod_ref[1:2, :]) + mod_ref[0:1, :]).astype(BF16)

    def scaled(w_ref, gain_ref):
        y = jnp.dot(normed, w_ref[...], preferred_element_type=F32)
        m = jnp.mean(y * y, axis=-1, keepdims=True)
        return (y * lax.rsqrt(m + EPS) * gain_ref[...]).astype(BF16)

    ql = scaled(qd_ref, qgain_ref)
    kl = scaled(kvd_ref, kvgain_ref)
    rk = jnp.dot(normed, rd_ref[...], preferred_element_type=F32).astype(BF16).astype(F32)
    rk = rk.T[:ROPE_DIM]
    rk_square = jnp.sum(rk * rk, axis=0, keepdims=True)
    first = core == 0
    q_mine = jnp.where(first, ql[:, :256], ql[:, 256:])
    q_other = jnp.where(first, ql[:, 256:], ql[:, :256])
    k_mine = jnp.where(first, kl[:, :128], kl[:, 128:])
    k_other = jnp.where(first, kl[:, 128:], kl[:, :128])

    def dot(a, b):
        return jnp.dot(a, b, preferred_element_type=F32)

    for k in range(4):
        if k == 0:
            q = dot(ql, qw_ref[...])
            kn = dot(kl, kw_ref[...])
            vv = dot(kl, vw_ref[...])
        else:
            a, b = (qa1, qa2, qa3)[k - 1], (qb1, qb2, qb3)[k - 1]
            q = dot(q_mine, a[...]) + dot(q_other, b[...])
            a, b = (ka1, ka2, ka3)[k - 1], (kb1, kb2, kb3)[k - 1]
            both = dot(k_mine, a[...]) + dot(k_other, b[...])
            kn, vv = both[:, :256], both[:, 256:]
        q, kn, vv = q.T, kn.T, vv.T
        for j in range(4):
            qh = q[QK_DIM * j : QK_DIM * (j + 1)]
            inv = lax.rsqrt(jnp.sum(qh * qh, axis=0, keepdims=True) * (1.0 / QK_DIM) + EPS)
            qh = qh * inv * qg_ref[...]
            qh = jnp.concatenate([qh[:NOPE_DIM], turned(qh[NOPE_DIM:], cos_ref, sin_ref)], axis=0)
            out_ref[k, j, 0:QK_DIM, :] = qh.astype(BF16)
            kh = kn[NOPE_DIM * j : NOPE_DIM * (j + 1)]
            square = jnp.sum(kh * kh, axis=0, keepdims=True) + rk_square
            inv = lax.rsqrt(square * (1.0 / QK_DIM) + EPS)
            kr = turned(rk * inv * kg_ref[NOPE_DIM:, :], cos_ref, sin_ref)
            kh = kh * inv * kg_ref[:NOPE_DIM, :]
            out_ref[k, j, QK_DIM : QK_DIM + NOPE_DIM, :] = kh.astype(BF16)
            out_ref[k, j, QK_DIM + NOPE_DIM : 2 * QK_DIM, :] = kr.astype(BF16)
            out_ref[k, j, 2 * QK_DIM : 256, :] = vv[VALUE_DIM * j : VALUE_DIM * (j + 1)].astype(BF16)


def expand(*args):
    return pl.pallas_call(
        expand_kernel,
        out_shape=jax.ShapeDtypeStruct((4, 4, 256, 128), BF16),
        in_specs=[VMEM] * len(args),
        out_specs=VMEM,
        cost_estimate=pl.CostEstimate(flops=800_000_000, bytes_accessed=6_000_000, transcendentals=10_000),
        name="expand",
    )(*args)


CHUNK = 1536
TILE = 512
SUB = 256
STEPS = CHUNK // SUB
PLANE = [(db, dy) for dy in range(4) for db in range(4)]


def back_kernel(
    qkv_ref, clat_ref, crope_ref, kup_ref, vup_ref, kg_ref, lift_ref, x_hbm, mods_ref, wout_hbm, out_ref,
    q_in, kvs, q_s, k_s, v_s, s_s, m_s, top_s, acc_s, att_s, slots, w_s, x_s,
    s_q, r_q, s_kv, r_kv, s_up, r_up, s_down, r_down, s_far, r_far, s_att, r_att,
    s_w, r_w, s_wc, r_wc, local_sem,
):
    sp, tp, core = lax.axis_index("sp"), lax.axis_index("tp"), lax.axis_index("dp")
    z, x = sp // 4, lax.rem(sp, 4)
    a, b = z + core * (x - z), x + core * (z - x)

    def at(da, db, dy):
        aa, bb = lax.rem(a + da, 4), lax.rem(b + db, 4)
        return {"sp": aa * (4 - 3 * core) + bb * (1 + 3 * core), "tp": lax.rem(tp + dy, 4)}

    def send(src, dst, send_sem, recv_sem, to):
        c = pltpu.make_async_remote_copy(
            src_ref=src, dst_ref=dst, send_sem=send_sem, recv_sem=recv_sem, device_id=to, device_id_type=MESH
        )
        c.start()
        return c

    up, down, partner = at(1, 0, 0), at(3, 0, 0), {"dp": 1 - core}
    barrier = pltpu.get_barrier_semaphore()
    for to in [at(0, db, dy) for db, dy in PLANE[1:]] + [up, down, partner]:
        pl.semaphore_signal(barrier, inc=1, device_id=to, device_id_type=MESH)
    own = [
        pltpu.make_async_copy(qkv_ref.at[0, b, 0:96], q_in.at[0], local_sem.at[0]),
        pltpu.make_async_copy(qkv_ref.at[0, b, 96:256], kvs.at[0, 0], local_sem.at[1]),
        pltpu.make_async_copy(x_hbm, x_s, local_sem.at[2]),
        pltpu.make_async_copy(wout_hbm.at[0:128], w_s.at[0, 0], local_sem.at[3]),
        pltpu.make_async_copy(wout_hbm.at[128:256], w_s.at[0, 1], local_sem.at[4]),
    ]
    for c in own:
        c.start()
    pl.semaphore_wait(barrier, 18)
    q_copies, kv_copies = [None], [None]
    for r in range(1, 16):
        db, dy = PLANE[r]
        head = lax.rem(b + db, 4)
        q_copies.append(send(qkv_ref.at[dy, head, 0:96], q_in.at[r], s_q.at[r], r_q.at[r], at(0, db, dy)))
    for r in range(1, 16):
        db, dy = PLANE[r]
        head = lax.rem(b + db, 4)
        kv_copies.append(send(qkv_ref.at[dy, head, 96:256], kvs.at[0, r], s_kv.at[r], r_kv.at[r], at(0, db, dy)))

    def own_head(w_ref):
        w = w_ref[...].astype(F32)
        w = jnp.where(b < 2, w[:, :128], w[:, 128:])
        return jnp.where(lax.rem(b, 2) == 0, w, pltpu.roll(w, 64, 1)).astype(BF16)

    clat = clat_ref[...].reshape(1024, 256)
    kn = jnp.dot(clat, own_head(kup_ref), preferred_element_type=F32)
    rope = crope_ref[...].reshape(1024, ROPE_DIM).astype(F32)
    key = jnp.concatenate([kn[:, :NOPE_DIM], rope, jnp.zeros((1024, 32), F32)], axis=1)
    inv = lax.rsqrt(jnp.sum(key * key, axis=1, keepdims=True) * (1.0 / QK_DIM) + EPS)
    gain = jnp.concatenate([kg_ref[...], jnp.zeros((1, 32), F32)], axis=1)
    lift = jnp.full((1, 128), lift_ref[b] * LOG2E, F32)
    high = lift.astype(BF16).astype(F32)
    middle = (lift - high).astype(BF16).astype(F32)
    low = lift - high - middle
    lane = lax.broadcasted_iota(jnp.int32, (1, 128), 1)
    extra = jnp.where(lane == 96, high, jnp.where(lane == 97, middle, jnp.where(lane == 98, low, 0.0)))
    k_s[0, 0:1024, :] = (key * inv * gain + extra).astype(BF16)
    vv = jnp.dot(clat, own_head(vup_ref), preferred_element_type=F32).T
    v_s[0, 0:VALUE_DIM, 0:1024] = vv[:VALUE_DIM].astype(BF16)
    for i in range(2):
        v_s[i, VALUE_DIM:80, :] = jnp.ones((16, CHUNK), BF16)
    for t in range(4):
        q_s[t, QK_DIM:128, :] = jnp.ones((32, TILE), BF16)
    m_s[...] = jnp.full(m_s.shape, -1e30, F32)
    acc_s[...] = jnp.zeros(acc_s.shape, F32)

    def place(chunk, first, blocks):
        for i, (slot, r) in enumerate(blocks):
            at_key = first + 128 * i
            block = kvs[slot, r]
            kt = jnp.concatenate([block[:QK_DIM].astype(F32), jnp.zeros((32, 128), F32)], axis=0)
            k_s[chunk % 2, at_key : at_key + 128, :] = kt.T.astype(BF16)
            v_s[chunk % 2, 0:VALUE_DIM, at_key : at_key + 128] = block[QK_DIM:]

    ups, downs, far, wides = [], [], [], []

    def spread(g):
        for r in range(max(1, 4 * g), 4 * g + 4):
            kv_copies[r].wait_recv()
        rows = pl.ds(4 * g, 4)
        ups.append(send(kvs.at[0, rows], kvs.at[1, rows], s_up.at[g], r_up.at[g], up))
        downs.append(send(kvs.at[0, rows], kvs.at[2, rows], s_down.at[g], r_down.at[g], down))

    def farther(g):
        rows = pl.ds(4 * g, 4)
        slot, to = (1, up) if g < 2 else (2, down)
        far.append(send(kvs.at[slot, rows], kvs.at[3, rows], s_far.at[g], r_far.at[g], to))

    def rows_of(slot, *groups):
        return [(slot, 4 * g + i) for g in groups for i in range(4)]

    y_up, y_down = at(0, 0, 1), at(0, 0, 3)

    def weights_near():
        own[3].wait()
        own[4].wait()
        wides.append(send(w_s.at[0, core], w_s.at[3, core], s_w.at[0], r_w.at[0], y_up))
        wides.append(send(w_s.at[0, core], w_s.at[1, core], s_w.at[1], r_w.at[1], y_down))

    wide_far, shared = [], []

    def weights_far():
        wides[0].wait_recv()
        wides[1].wait_recv()
        wide_far.append(
            send(w_s.at[3, core, 0:64], w_s.at[2, core, 0:64], s_w.at[2], r_w.at[2], y_up)
        )
        wide_far.append(
            send(w_s.at[1, core, 64:128], w_s.at[2, core, 64:128], s_w.at[3], r_w.at[3], y_down)
        )
        for k in (3, 1):
            shared.append(send(w_s.at[k, core], w_s.at[k, core], s_wc.at[k], r_wc.at[k], partner))

    def weights_share():
        for c in wide_far:
            c.wait_recv()
        shared.append(send(w_s.at[2, core], w_s.at[2, core], s_wc.at[2], r_wc.at[2], partner))

    def prepare(chunk):
        if chunk == 0:
            own[1].wait()
            spread(0)
            place(0, 1024, rows_of(0, 0))
        elif chunk == 1:
            for g in range(1, 4):
                spread(g)
            weights_near()
            place(1, 0, rows_of(0, 1, 2, 3))
        elif chunk == 2:
            for g in range(3):
                ups[g].wait_recv()
            farther(0)
            farther(1)
            place(2, 0, rows_of(1, 0, 1, 2))
        elif chunk == 3:
            for g in range(1, 4):
                downs[g].wait_recv()
            farther(2)
            farther(3)
            place(3, 0, rows_of(2, 1, 2, 3))
        elif chunk == 4:
            ups[3].wait_recv()
            downs[0].wait_recv()
            far[0].wait_recv()
            place(4, 0, rows_of(1, 3) + rows_of(2, 0) + rows_of(3, 0))
            weights_far()
        else:
            for g in range(1, 4):
                far[g].wait_recv()
            place(5, 0, rows_of(3, 1, 2, 3))

    def score(chunk, t, i):
        rows = slice(i * SUB, (i + 1) * SUB)
        s = jnp.dot(k_s[chunk % 2, rows], q_s[t], preferred_element_type=F32)
        s_s[rows] = s
        return jnp.max(s.reshape(SUB // 8, 8, TILE), axis=0)

    def step(chunk, t, later_chunk, later):
        old = m_s[t]
        new = jnp.maximum(old, jnp.max(top_s[...], axis=0, keepdims=True))
        m_s[t] = new
        acc = acc_s[t] * jnp.exp2(old - new)
        top = None
        for i in range(STEPS):
            rows = slice(i * SUB, (i + 1) * SUB)
            p = jnp.exp2(s_s[rows] - new).astype(BF16)
            acc = acc + jnp.dot(v_s[chunk % 2, :, rows], p, preferred_element_type=F32)
            if later is not None:
                part = score(later_chunk, later, i)
                top = part if top is None else jnp.maximum(top, part)
        acc_s[t] = acc
        if later is not None:
            top_s[...] = top

    att_copies = []

    def finish(t):
        acc = acc_s[t]
        o = (acc[:VALUE_DIM] / acc[VALUE_DIM : VALUE_DIM + 1]).astype(BF16)
        for i in range(4):
            att_s[4 * t + i] = o[:, 128 * i : 128 * i + 128]

    def give(t):
        for r in range(4 * t, 4 * t + 4):
            db, dy = PLANE[r]
            if r:
                att_copies.append(
                    send(
                        att_s.at[r], slots.at[dy, b], s_att.at[r], r_att.at[r],
                        at(0, (4 - db) % 4, (4 - dy) % 4),
                    )
                )
            else:
                slots[0, b] = att_s[0]

    own[0].wait()
    q_s[0, 0:QK_DIM, 0:128] = q_in[0]
    for r in range(1, 16):
        q_copies[r].wait_recv()
        q_s[r // 4, 0:QK_DIM, 128 * (r % 4) : 128 * (r % 4) + 128] = q_in[r]
    prepare(0)
    top = None
    for i in range(STEPS):
        part = score(0, 0, i)
        top = part if top is None else jnp.maximum(top, part)
    top_s[...] = top
    for chunk in range(6):
        if chunk < 5:

            def some_tile(t, carry, chunk=chunk):
                step(chunk, t, chunk, t + 1)
                return carry

            lax.fori_loop(0, 3, some_tile, 0)
            prepare(chunk + 1)
            step(chunk, 3, chunk + 1, 0)
        else:
            for t in range(4):
                step(chunk, t, chunk, t + 1 if t < 3 else None)
                finish(t)
                if t:
                    give(t - 1)
                if t == 1:
                    weights_share()
            give(3)

    own[2].wait()
    for c in shared:
        c.wait_recv()
    for c in att_copies:
        c.wait_recv()
    atts = []
    for k in range(4):
        atts.append(slots[k].reshape(256, 128).astype(F32).T.astype(BF16))
    gate = [mods_ref[i, 8 + j : 9 + j, :] for i in range(4) for j in range(4)]
    for n in range(4):
        cols = slice(512 * n, 512 * n + 512)
        mixed = None
        for k in range(4):
            w = w_s[k, :, :, cols].reshape(256, 512)
            term = jnp.dot(atts[k], w, preferred_element_type=F32).astype(BF16).astype(F32)
            mixed = term if mixed is None else mixed + term
        gated = jnp.concatenate(gate[4 * n : 4 * n + 4], axis=1)
        out_ref[:, cols] = (x_s[:, cols].astype(F32) + gated * mixed).astype(BF16)
    for c in q_copies[1:] + kv_copies[1:] + ups + downs + far + wides + wide_far + shared + att_copies:
        c.wait_send()


def back(*args):
    dma = pltpu.SemaphoreType.DMA
    hbm = pl.BlockSpec(memory_space=pl.ANY)
    return pl.pallas_call(
        back_kernel,
        out_shape=jax.ShapeDtypeStruct((128, 2048), BF16),
        in_specs=[VMEM] * 6 + [pl.BlockSpec(memory_space=pltpu.SMEM), hbm, VMEM, hbm],
        out_specs=VMEM,
        scratch_shapes=[
            pltpu.VMEM((16, QK_DIM, 128), BF16),
            pltpu.VMEM((4, 16, 160, 128), BF16),
            pltpu.VMEM((4, 128, TILE), BF16),
            pltpu.VMEM((2, CHUNK, 128), BF16),
            pltpu.VMEM((2, 80, CHUNK), BF16),
            pltpu.VMEM((CHUNK, TILE), F32),
            pltpu.VMEM((4, 1, TILE), F32),
            pltpu.VMEM((8, TILE), F32),
            pltpu.VMEM((4, 80, TILE), F32),
            pltpu.VMEM((16, VALUE_DIM, 128), BF16),
            pltpu.VMEM((4, 4, VALUE_DIM, 128), BF16),
            pltpu.VMEM((4, 2, 128, 2048), BF16),
            pltpu.VMEM((128, 2048), BF16),
            dma((16,)), dma((16,)), dma((16,)), dma((16,)),
            dma((4,)), dma((4,)), dma((4,)), dma((4,)), dma((4,)), dma((4,)), dma((16,)), dma((16,)),
            dma((4,)), dma((4,)), dma((4,)), dma((4,)), dma((5,)),
        ],
        compiler_params=pltpu.CompilerParams(
            collective_id=1, has_side_effects=True, vmem_limit_bytes=48 * 1024 * 1024
        ),
        cost_estimate=pl.CostEstimate(
            flops=10_000_000_000, bytes_accessed=8_000_000, transcendentals=19_000_000
        ),
        name="back",
    )(*args)


def ring_pieces(half):
    return [lax.ppermute(half, "tp", [((d + k) % 4, d) for d in range(4)]) for k in range(1, 4)]


def swapped(pieces):
    return [lax.ppermute(p, "dp", [(0, 1), (1, 0)]) for p in pieces]


def half_of(weight, core):
    rows = weight.shape[0] // 2
    return lax.dynamic_slice_in_dim(weight, core * rows, rows, axis=0)


def local(
    latent_tokens, condition, shift_weight, scale_weight, gate_weight, norm_gain, query_down, query_gain,
    kv_down, kv_gain, rope_down, query_up, key_up, value_up, query_norm_gain, key_norm_gain, out_weight,
    context_latent, context_rope, context_lift,
):
    sp, tp, core = lax.axis_index("sp"), lax.axis_index("tp"), lax.axis_index("dp")
    activated = jax.nn.silu(condition.astype(F32)).astype(BF16)[None]
    part = jnp.concatenate(
        [
            jnp.dot(activated, w, preferred_element_type=F32).reshape(4, 128)
            for w in (shift_weight, scale_weight, gate_weight)
        ]
        + [jnp.zeros((4, 128), F32)],
        axis=0,
    )
    q_mine = ring_pieces(half_of(query_up, core))
    kv_mine = ring_pieces(half_of(jnp.concatenate([key_up, value_up], axis=1), core))
    q_other, kv_other = swapped(q_mine), swapped(kv_mine)

    mods, clat, crope = modulation(part, context_latent, context_rope)
    mod = jnp.transpose(mods[:, :12].reshape(4, 3, 4, 128), (1, 0, 2, 3)).reshape(3, 2048)

    positions = (sp * 4 + tp) * 128 + jnp.arange(128, dtype=jnp.int32)
    inverse = THETA ** (-4.0 * jnp.arange(8, dtype=F32) / ROPE_DIM)
    places = jnp.stack([(positions // GRID_W).astype(F32), (positions % GRID_W).astype(F32)])
    angles = places[:, None, :] * inverse[None, :, None]
    cosine, sine = jnp.cos(angles), jnp.sin(angles)
    query_scale = (query_norm_gain * (LOG2E * QK_DIM**-0.5)).reshape(QK_DIM, 1)
    qkv = expand(
        latent_tokens, mod, norm_gain.reshape(1, -1), query_down, kv_down,
        jnp.pad(rope_down, ((0, 0), (0, 96))), query_gain.reshape(1, -1), kv_gain.reshape(1, -1),
        cosine, sine, query_scale, key_norm_gain.reshape(QK_DIM, 1),
        query_up, key_up, value_up, *q_mine, *q_other, *kv_mine, *kv_other,
    )

    return back(
        qkv, clat, crope, key_up, value_up, key_norm_gain.reshape(1, QK_DIM), context_lift,
        latent_tokens, mods, out_weight,
    )


def solution(mesh):
    in_specs = (
        P(("dp", "sp", "tp"), None), P(("dp", "sp")), P("sp", "tp"), P("sp", "tp"), P("sp", "tp"),
        P(), P(), P(), P(), P(), P(), P(None, "tp"), P(None, "tp"), P(None, "tp"), P(), P(),
        P("tp", None), P(("dp", "sp"), None), P(("dp", "sp"), None), P("tp"),
    )
    return jax.shard_map(
        local, mesh=mesh, in_specs=in_specs, out_specs=P(("dp", "sp", "tp"), None), check_vma=False
    )
```

```python
import jax
import jax.numpy as jnp
from jax import lax
from jax.experimental import pallas as pl
from jax.experimental.pallas import tpu as pltpu
from jax.sharding import PartitionSpec as P

NOPE_DIM = 64
ROPE_DIM = 32
VALUE_DIM = 64
QK_DIM = 96
GRID_W = 64
EPS = 1e-06
THETA = 10000.0
LOG2E = 1.4426950408889634

F32 = jnp.float32
BF16 = jnp.bfloat16
MESH = pl.DeviceIdType.MESH
VMEM = pl.BlockSpec(memory_space=pltpu.VMEM)


def send(src, dst, send_sem, recv_sem, to):
    c = pltpu.make_async_remote_copy(
        src_ref=src, dst_ref=dst, send_sem=send_sem, recv_sem=recv_sem, device_id=to, device_id_type=MESH
    )
    c.start()
    return c


def turned(rows, cosine, sine):
    out = []
    for a in range(2):
        u, w = rows[16 * a : 16 * a + 8], rows[16 * a + 8 : 16 * a + 16]
        out += [u * cosine[a] - w * sine[a], w * cosine[a] + u * sine[a]]
    return jnp.concatenate(out, axis=0)


def column(row):
    row = jnp.concatenate([row, jnp.zeros((1, 32), F32)], axis=1)
    return jnp.broadcast_to(row, (128, 128)).T[:QK_DIM]


def front_kernel(
    cond_ref, shift_ref, scale_ref, gate_ref, ng_ref, qgain_ref, kvgain_ref, qng_ref, kng_ref, freq_ref,
    x_hbm, qd_hbm, kvd_hbm, rd_hbm, qw_hbm, kw_hbm, vw_hbm, lat_hbm, rope_hbm,
    out_ref, gate_out, clat_ref, crope_ref,
    x_s, qd_s, kvd_s, rd_s, wq_s, wkv_s, near_s, near_g, wide_s, wide_g,
    s_near, r_near, s_neg, r_neg, s_wide, r_wide, s_wig, r_wig, s_lat, r_lat, s_rope, r_rope,
    s_q, r_q, s_kv, r_kv, s_qc, r_qc, s_kvc, r_kvc, local_sem,
):
    sp, tp, core = lax.axis_index("sp"), lax.axis_index("tp"), lax.axis_index("dp")
    partner = {"dp": 1 - core}

    def along_tp(k):
        return {"tp": lax.rem(tp + k, 4)}

    def along_sp(r):
        return {"sp": lax.rem(sp + r, 16)}

    barrier = pltpu.get_barrier_semaphore()
    for to in [along_tp(k) for k in range(1, 4)] + [along_sp(r) for r in range(1, 16)] + [partner]:
        pl.semaphore_signal(barrier, inc=1, device_id=to, device_id_type=MESH)
    own = []

    def fetch(src, dst):
        c = pltpu.make_async_copy(src, dst, local_sem.at[len(own)])
        c.start()
        own.append(c)

    for h in range(2):
        fetch(qw_hbm.at[256 * h : 256 * h + 256], wq_s.at[0, h])
        fetch(kw_hbm.at[128 * h : 128 * h + 128], wkv_s.at[0, h, :, 0:256])
        fetch(vw_hbm.at[128 * h : 128 * h + 128], wkv_s.at[0, h, :, 256:512])
    fetch(x_hbm, x_s)
    fetch(qd_hbm, qd_s)
    fetch(kvd_hbm, kvd_s)
    fetch(rd_hbm, rd_s)
    fetch(lat_hbm, clat_ref.at[0])
    fetch(rope_hbm, crope_ref.at[0])

    cond = cond_ref[...].astype(F32)
    active = cond / (1.0 + jnp.exp(-cond))
    active = jnp.broadcast_to(active, (16, 128)).astype(BF16)
    for i, w_ref in enumerate((shift_ref, scale_ref, gate_ref)):
        row = jnp.dot(active, w_ref[...], preferred_element_type=F32)
        for j in range(4):
            piece = row[0:1, 128 * j : 128 * j + 128]
            if i < 2:
                near_s[tp, 4 * i + j : 4 * i + j + 1, :] = piece
            else:
                near_g[tp, j : j + 1, :] = piece
    near_g[tp, 4:8, :] = jnp.zeros((4, 128), F32)
    pl.semaphore_wait(barrier, 19)

    nears, negs = [], []
    for k in range(1, 4):
        nears.append(send(near_s.at[tp], near_s.at[tp], s_near.at[k], r_near.at[k], along_tp(k)))
    for k in range(1, 4):
        negs.append(send(near_g.at[tp], near_g.at[tp], s_neg.at[k], r_neg.at[k], along_tp(k)))
    for i in range(6):
        own[i].wait()
    near_w = []
    for k in (1, 3):
        near_w.append(send(wq_s.at[0, core], wq_s.at[4 - k, core], s_q.at[k], r_q.at[k], along_tp(k)))
        near_w.append(send(wkv_s.at[0, core], wkv_s.at[4 - k, core], s_kv.at[k], r_kv.at[k], along_tp(k)))

    for c in nears:
        c.wait_recv()
    wides, wigs, rest = [], [], []
    for r in range(1, 16):
        wides.append(send(near_s, wide_s.at[r], s_wide.at[r], r_wide.at[r], along_sp(r)))
    for c in negs:
        c.wait_recv()
    for r in range(1, 16):
        wigs.append(send(near_g, wide_g.at[r], s_wig.at[r], r_wig.at[r], along_sp(r)))
    for r in range(1, 16):
        rest.append(send(lat_hbm, clat_ref.at[r], s_lat.at[r], r_lat.at[r], along_sp(r)))
        rest.append(send(rope_hbm, crope_ref.at[r], s_rope.at[r], r_rope.at[r], along_sp(r)))

    lane = lax.broadcasted_iota(jnp.int32, (8, 128), 1)
    first = (sp * 4 + tp) * 2
    angles = [
        (first + lane // GRID_W).astype(F32) * freq_ref[...],
        lax.rem(lane, GRID_W).astype(F32) * freq_ref[...],
    ]
    cosine, sine = [jnp.cos(v) for v in angles], [jnp.sin(v) for v in angles]
    q_gain = column(qng_ref[...] * (LOG2E * QK_DIM**-0.5))
    k_gain = column(kng_ref[...])
    for c in own[6:]:
        c.wait()
    values = x_s[...].astype(F32)
    mean_square = jnp.mean(values * values, axis=-1, keepdims=True)
    scaled = values * lax.rsqrt(mean_square + EPS) * ng_ref[...]

    total = near_s[...]
    for r in range(1, 16):
        wides[r - 1].wait_recv()
        total = total + wide_s[r]
    mod = [
        jnp.concatenate([total[i, 4 * k + j : 4 * k + j + 1] for i in range(4) for j in range(4)], axis=1)
        for k in range(2)
    ]
    normed = (scaled * (1.0 + mod[1]) + mod[0]).astype(BF16)

    def latent(w, gain_ref):
        y = jnp.dot(normed, w[...], preferred_element_type=F32)
        m = jnp.mean(y * y, axis=-1, keepdims=True)
        return (y * lax.rsqrt(m + EPS) * gain_ref[...]).astype(BF16)

    ql = latent(qd_s, qgain_ref)
    kl = latent(kvd_s, kvgain_ref)
    rk = lax.dot_general(rd_s[...], normed, (((1,), (1,)), ((), ())), preferred_element_type=F32)
    rk = rk.astype(BF16).astype(F32)
    rk_square = jnp.sum(rk * rk, axis=0, keepdims=True)

    shared = []

    def share(k):
        shared.append(send(wq_s.at[k, core], wq_s.at[k, core], s_qc.at[k], r_qc.at[k], partner))
        shared.append(send(wkv_s.at[k, core], wkv_s.at[k, core], s_kvc.at[k], r_kvc.at[k], partner))

    for c in near_w:
        c.wait_recv()
    far_w = [
        send(wq_s.at[3, core], wq_s.at[2, core], s_q.at[2], r_q.at[2], along_tp(1)),
        send(wkv_s.at[1, core], wkv_s.at[2, core], s_kv.at[2], r_kv.at[2], along_tp(3)),
    ]
    share(3)
    share(1)

    def expand(k):
        q = jnp.dot(ql, wq_s[k].reshape(512, 384), preferred_element_type=F32).T
        kv = jnp.dot(kl, wkv_s[k].reshape(256, 512), preferred_element_type=F32).T
        for j in range(4):
            qh = q[QK_DIM * j : QK_DIM * (j + 1)]
            inv = lax.rsqrt(jnp.sum(qh * qh, axis=0, keepdims=True) * (1.0 / QK_DIM) + EPS)
            qh = qh * inv * q_gain
            qh = jnp.concatenate([qh[:NOPE_DIM], turned(qh[NOPE_DIM:], cosine, sine)], axis=0)
            out_ref[k, j, 0:QK_DIM, :] = qh.astype(BF16)
            kh = kv[NOPE_DIM * j : NOPE_DIM * (j + 1)]
            square = jnp.sum(kh * kh, axis=0, keepdims=True) + rk_square
            inv = lax.rsqrt(square * (1.0 / QK_DIM) + EPS)
            kr = turned(rk * inv * k_gain[NOPE_DIM:], cosine, sine)
            kh = kh * inv * k_gain[:NOPE_DIM]
            out_ref[k, j, QK_DIM : QK_DIM + NOPE_DIM, :] = kh.astype(BF16)
            out_ref[k, j, QK_DIM + NOPE_DIM : 2 * QK_DIM, :] = kr.astype(BF16)
            vh = kv[256 + VALUE_DIM * j : 256 + VALUE_DIM * (j + 1)]
            out_ref[k, j, 2 * QK_DIM : 256, :] = vh.astype(BF16)

    expand(0)
    for c in shared[0:4]:
        c.wait_recv()
    expand(3)
    expand(1)
    for c in far_w:
        c.wait_recv()
    share(2)
    gates = near_g[...]
    for r in range(1, 16):
        wigs[r - 1].wait_recv()
        gates = gates + wide_g[r]
    gate_out[...] = gates
    for c in shared[4:6]:
        c.wait_recv()
    expand(2)
    for c in rest:
        c.wait()
    for c in nears + negs + near_w + wides + wigs + far_w + shared:
        c.wait_send()


def front(*args):
    dma = pltpu.SemaphoreType.DMA
    hbm = pl.BlockSpec(memory_space=pltpu.HBM)
    return pl.pallas_call(
        front_kernel,
        out_shape=(
            jax.ShapeDtypeStruct((4, 4, 256, 128), BF16),
            jax.ShapeDtypeStruct((4, 8, 128), F32),
            jax.ShapeDtypeStruct((16, 64, 256), BF16),
            jax.ShapeDtypeStruct((16, 32, 64), BF16),
        ),
        in_specs=[VMEM] * 10 + [hbm] * 9,
        out_specs=(VMEM,) * 4,
        scratch_shapes=[
            pltpu.VMEM((128, 2048), BF16),
            pltpu.VMEM((2048, 512), BF16),
            pltpu.VMEM((2048, 256), BF16),
            pltpu.VMEM((32, 2048), BF16),
            pltpu.VMEM((4, 2, 256, 384), BF16),
            pltpu.VMEM((4, 2, 128, 512), BF16),
            pltpu.VMEM((4, 8, 128), F32),
            pltpu.VMEM((4, 8, 128), F32),
            pltpu.VMEM((16, 4, 8, 128), F32),
            pltpu.VMEM((16, 4, 8, 128), F32),
            dma((4,)), dma((4,)), dma((4,)), dma((4,)),
            dma((16,)), dma((16,)), dma((16,)), dma((16,)), dma((16,)), dma((16,)), dma((16,)), dma((16,)),
            dma((4,)), dma((4,)), dma((4,)), dma((4,)), dma((4,)), dma((4,)), dma((4,)), dma((4,)),
            dma((12,)),
        ],
        compiler_params=pltpu.CompilerParams(
            collective_id=0, has_side_effects=True, vmem_limit_bytes=32 * 1024 * 1024
        ),
        cost_estimate=pl.CostEstimate(flops=800_000_000, bytes_accessed=8_000_000, transcendentals=10_000),
        name="front",
    )(*args)


CHUNK = 1536
TILE = 512
SUB = 256
STEPS = CHUNK // SUB
PLANE = [(db, dy) for dy in range(4) for db in range(4)]


def back_kernel(
    qkv_ref, clat_ref, crope_ref, kup_ref, vup_ref, kg_ref, lift_ref, x_hbm, gate_ref, wout_hbm, out_ref,
    q_in, kvs, q_s, k_s, v_s, s_s, m_s, top_s, acc_s, att_s, slots, w_s, x_s,
    s_q, r_q, s_kv, r_kv, s_up, r_up, s_down, r_down, s_far, r_far, s_att, r_att,
    s_w, r_w, s_wc, r_wc, local_sem,
):
    sp, tp, core = lax.axis_index("sp"), lax.axis_index("tp"), lax.axis_index("dp")
    z, x = sp // 4, lax.rem(sp, 4)
    a, b = z + core * (x - z), x + core * (z - x)

    def at(da, db, dy):
        aa, bb = lax.rem(a + da, 4), lax.rem(b + db, 4)
        return {"sp": aa * (4 - 3 * core) + bb * (1 + 3 * core), "tp": lax.rem(tp + dy, 4)}

    up, down, partner = at(1, 0, 0), at(3, 0, 0), {"dp": 1 - core}
    barrier = pltpu.get_barrier_semaphore()
    for to in [at(0, db, dy) for db, dy in PLANE[1:]] + [up, down, partner]:
        pl.semaphore_signal(barrier, inc=1, device_id=to, device_id_type=MESH)
    own = [
        pltpu.make_async_copy(qkv_ref.at[0, b, 0:96], q_in.at[0], local_sem.at[0]),
        pltpu.make_async_copy(qkv_ref.at[0, b, 96:256], kvs.at[0, 0], local_sem.at[1]),
        pltpu.make_async_copy(x_hbm, x_s, local_sem.at[2]),
        pltpu.make_async_copy(wout_hbm.at[0:128], w_s.at[0, 0], local_sem.at[3]),
        pltpu.make_async_copy(wout_hbm.at[128:256], w_s.at[0, 1], local_sem.at[4]),
    ]
    for c in own:
        c.start()
    pl.semaphore_wait(barrier, 18)
    q_copies, kv_copies = [None], [None]
    for r in range(1, 16):
        db, dy = PLANE[r]
        head = lax.rem(b + db, 4)
        q_copies.append(send(qkv_ref.at[dy, head, 0:96], q_in.at[r], s_q.at[r], r_q.at[r], at(0, db, dy)))
    for r in range(1, 16):
        db, dy = PLANE[r]
        head = lax.rem(b + db, 4)
        kv_copies.append(send(qkv_ref.at[dy, head, 96:256], kvs.at[0, r], s_kv.at[r], r_kv.at[r], at(0, db, dy)))

    def own_head(w_ref):
        w = w_ref[...].astype(F32)
        w = jnp.where(b < 2, w[:, :128], w[:, 128:])
        return jnp.where(lax.rem(b, 2) == 0, w, pltpu.roll(w, 64, 1)).astype(BF16)

    clat = clat_ref[...].reshape(1024, 256)
    kn = jnp.dot(clat, own_head(kup_ref), preferred_element_type=F32)
    lane = lax.broadcasted_iota(jnp.int32, (1, 128), 1)
    ropes = []
    for i in range(8):
        two = jnp.concatenate([crope_ref[2 * i], crope_ref[2 * i + 1]], axis=1).astype(F32)
        two = jnp.concatenate([jnp.zeros((64, 128), F32), two, jnp.zeros((32, 128), F32)], axis=0)
        ropes.append(two.T)
    key = jnp.where(lane < NOPE_DIM, kn, jnp.concatenate(ropes, axis=0))
    inv = lax.rsqrt(jnp.sum(key * key, axis=1, keepdims=True) * (1.0 / QK_DIM) + EPS)
    gain = jnp.concatenate([kg_ref[...], jnp.zeros((1, 32), F32)], axis=1)
    lift = jnp.full((1, 128), lift_ref[b] * LOG2E, F32)
    high = lift.astype(BF16).astype(F32)
    middle = (lift - high).astype(BF16).astype(F32)
    low = lift - high - middle
    extra = jnp.where(lane == 96, high, jnp.where(lane == 97, middle, jnp.where(lane == 98, low, 0.0)))
    k_s[0, 0:1024, :] = (key * inv * gain + extra).astype(BF16)
    vv = jnp.dot(clat, own_head(vup_ref), preferred_element_type=F32).T
    v_s[0, 0:VALUE_DIM, 0:1024] = vv[:VALUE_DIM].astype(BF16)
    for i in range(2):
        v_s[i, VALUE_DIM:80, :] = jnp.ones((16, CHUNK), BF16)
    for t in range(4):
        q_s[t, QK_DIM:128, :] = jnp.ones((32, TILE), BF16)
    m_s[...] = jnp.full(m_s.shape, -1e30, F32)
    acc_s[...] = jnp.zeros(acc_s.shape, F32)

    def place(chunk, first, blocks):
        for i, (slot, r) in enumerate(blocks):
            at_key = first + 128 * i
            block = kvs[slot, r]
            kt = jnp.concatenate([block[:QK_DIM].astype(F32), jnp.zeros((32, 128), F32)], axis=0)
            k_s[chunk % 2, at_key : at_key + 128, :] = kt.T.astype(BF16)
            v_s[chunk % 2, 0:VALUE_DIM, at_key : at_key + 128] = block[QK_DIM:]

    ups, downs, far, wides = [], [], [], []

    def spread(g):
        for r in range(max(1, 4 * g), 4 * g + 4):
            kv_copies[r].wait_recv()
        rows = pl.ds(4 * g, 4)
        ups.append(send(kvs.at[0, rows], kvs.at[1, rows], s_up.at[g], r_up.at[g], up))
        downs.append(send(kvs.at[0, rows], kvs.at[2, rows], s_down.at[g], r_down.at[g], down))

    def farther(g):
        rows = pl.ds(4 * g, 4)
        slot, to = (1, up) if g < 2 else (2, down)
        far.append(send(kvs.at[slot, rows], kvs.at[3, rows], s_far.at[g], r_far.at[g], to))

    def rows_of(slot, *groups):
        return [(slot, 4 * g + i) for g in groups for i in range(4)]

    y_up, y_down = at(0, 0, 1), at(0, 0, 3)

    def weights_near():
        own[3].wait()
        own[4].wait()
        wides.append(send(w_s.at[0, core], w_s.at[3, core], s_w.at[0], r_w.at[0], y_up))
        wides.append(send(w_s.at[0, core], w_s.at[1, core], s_w.at[1], r_w.at[1], y_down))

    wide_far, shared = [], []

    def weights_far():
        wides[0].wait_recv()
        wides[1].wait_recv()
        wide_far.append(
            send(w_s.at[3, core, 0:64], w_s.at[2, core, 0:64], s_w.at[2], r_w.at[2], y_up)
        )
        wide_far.append(
            send(w_s.at[1, core, 64:128], w_s.at[2, core, 64:128], s_w.at[3], r_w.at[3], y_down)
        )
        for k in (3, 1):
            shared.append(send(w_s.at[k, core], w_s.at[k, core], s_wc.at[k], r_wc.at[k], partner))

    def weights_share():
        for c in wide_far:
            c.wait_recv()
        shared.append(send(w_s.at[2, core], w_s.at[2, core], s_wc.at[2], r_wc.at[2], partner))

    def prepare(chunk):
        if chunk == 0:
            own[1].wait()
            spread(0)
            place(0, 1024, rows_of(0, 0))
        elif chunk == 1:
            for g in range(1, 4):
                spread(g)
            weights_near()
            place(1, 0, rows_of(0, 1, 2, 3))
        elif chunk == 2:
            for g in range(3):
                ups[g].wait_recv()
            farther(0)
            farther(1)
            place(2, 0, rows_of(1, 0, 1, 2))
        elif chunk == 3:
            for g in range(1, 4):
                downs[g].wait_recv()
            farther(2)
            farther(3)
            place(3, 0, rows_of(2, 1, 2, 3))
        elif chunk == 4:
            ups[3].wait_recv()
            downs[0].wait_recv()
            far[0].wait_recv()
            place(4, 0, rows_of(1, 3) + rows_of(2, 0) + rows_of(3, 0))
            weights_far()
        else:
            for g in range(1, 4):
                far[g].wait_recv()
            place(5, 0, rows_of(3, 1, 2, 3))

    def score(chunk, t, i):
        rows = slice(i * SUB, (i + 1) * SUB)
        s = jnp.dot(k_s[chunk % 2, rows], q_s[t], preferred_element_type=F32)
        s_s[rows] = s
        return jnp.max(s.reshape(SUB // 8, 8, TILE), axis=0)

    def step(chunk, t, later_chunk, later):
        old = m_s[t]
        new = jnp.maximum(old, jnp.max(top_s[...], axis=0, keepdims=True))
        m_s[t] = new
        acc = acc_s[t] * jnp.exp2(old - new)
        top = None
        for i in range(STEPS):
            rows = slice(i * SUB, (i + 1) * SUB)
            p = jnp.exp2(s_s[rows] - new).astype(BF16)
            acc = acc + jnp.dot(v_s[chunk % 2, :, rows], p, preferred_element_type=F32)
            if later is not None:
                part = score(later_chunk, later, i)
                top = part if top is None else jnp.maximum(top, part)
        acc_s[t] = acc
        if later is not None:
            top_s[...] = top

    att_copies = []

    def finish(t):
        acc = acc_s[t]
        o = (acc[:VALUE_DIM] / acc[VALUE_DIM : VALUE_DIM + 1]).astype(BF16)
        for i in range(4):
            att_s[4 * t + i] = o[:, 128 * i : 128 * i + 128]

    def give(t):
        for r in range(4 * t, 4 * t + 4):
            db, dy = PLANE[r]
            if r:
                att_copies.append(
                    send(
                        att_s.at[r], slots.at[dy, b], s_att.at[r], r_att.at[r],
                        at(0, (4 - db) % 4, (4 - dy) % 4),
                    )
                )
            else:
                slots[0, b] = att_s[0]

    own[0].wait()
    q_s[0, 0:QK_DIM, 0:128] = q_in[0]
    for r in range(1, 16):
        q_copies[r].wait_recv()
        q_s[r // 4, 0:QK_DIM, 128 * (r % 4) : 128 * (r % 4) + 128] = q_in[r]
    prepare(0)
    top = None
    for i in range(STEPS):
        part = score(0, 0, i)
        top = part if top is None else jnp.maximum(top, part)
    top_s[...] = top
    for chunk in range(6):
        if chunk < 5:

            def some_tile(t, carry, chunk=chunk):
                step(chunk, t, chunk, t + 1)
                return carry

            lax.fori_loop(0, 3, some_tile, 0)
            prepare(chunk + 1)
            step(chunk, 3, chunk + 1, 0)
        else:
            for t in range(4):
                step(chunk, t, chunk, t + 1 if t < 3 else None)
                finish(t)
                if t:
                    give(t - 1)
                if t == 1:
                    weights_share()
            give(3)

    own[2].wait()
    for c in shared:
        c.wait_recv()
    for c in att_copies:
        c.wait_recv()
    atts = []
    for k in range(4):
        atts.append(slots[k].reshape(256, 128).astype(F32).T.astype(BF16))
    gate = [gate_ref[i, j : j + 1, :] for i in range(4) for j in range(4)]
    for n in range(4):
        cols = slice(512 * n, 512 * n + 512)
        mixed = None
        for k in range(4):
            w = w_s[k, :, :, cols].reshape(256, 512)
            term = jnp.dot(atts[k], w, preferred_element_type=F32).astype(BF16).astype(F32)
            mixed = term if mixed is None else mixed + term
        gated = jnp.concatenate(gate[4 * n : 4 * n + 4], axis=1)
        out_ref[:, cols] = (x_s[:, cols].astype(F32) + gated * mixed).astype(BF16)
    for c in q_copies[1:] + kv_copies[1:] + ups + downs + far + wides + wide_far + shared + att_copies:
        c.wait_send()


def back(*args):
    dma = pltpu.SemaphoreType.DMA
    hbm = pl.BlockSpec(memory_space=pltpu.HBM)
    return pl.pallas_call(
        back_kernel,
        out_shape=jax.ShapeDtypeStruct((128, 2048), BF16),
        in_specs=[VMEM] * 6 + [pl.BlockSpec(memory_space=pltpu.SMEM), hbm, VMEM, hbm],
        out_specs=VMEM,
        scratch_shapes=[
            pltpu.VMEM((16, QK_DIM, 128), BF16),
            pltpu.VMEM((4, 16, 160, 128), BF16),
            pltpu.VMEM((4, 128, TILE), BF16),
            pltpu.VMEM((2, CHUNK, 128), BF16),
            pltpu.VMEM((2, 80, CHUNK), BF16),
            pltpu.VMEM((CHUNK, TILE), F32),
            pltpu.VMEM((4, 1, TILE), F32),
            pltpu.VMEM((8, TILE), F32),
            pltpu.VMEM((4, 80, TILE), F32),
            pltpu.VMEM((16, VALUE_DIM, 128), BF16),
            pltpu.VMEM((4, 4, VALUE_DIM, 128), BF16),
            pltpu.VMEM((4, 2, 128, 2048), BF16),
            pltpu.VMEM((128, 2048), BF16),
            dma((16,)), dma((16,)), dma((16,)), dma((16,)),
            dma((4,)), dma((4,)), dma((4,)), dma((4,)), dma((4,)), dma((4,)), dma((16,)), dma((16,)),
            dma((4,)), dma((4,)), dma((4,)), dma((4,)), dma((5,)),
        ],
        compiler_params=pltpu.CompilerParams(
            collective_id=1, has_side_effects=True, vmem_limit_bytes=48 * 1024 * 1024
        ),
        cost_estimate=pl.CostEstimate(
            flops=10_000_000_000, bytes_accessed=8_000_000, transcendentals=19_000_000
        ),
        name="back",
    )(*args)


def local(
    latent_tokens, condition, shift_weight, scale_weight, gate_weight, norm_gain, query_down, query_gain,
    kv_down, kv_gain, rope_down, query_up, key_up, value_up, query_norm_gain, key_norm_gain, out_weight,
    context_latent, context_rope, context_lift,
):
    frequency = THETA ** (-4.0 * jnp.arange(8, dtype=F32) / ROPE_DIM)
    qkv, gates, clat, crope = front(
        condition.reshape(1, 128), shift_weight, scale_weight, gate_weight,
        norm_gain.reshape(1, -1), query_gain.reshape(1, -1), kv_gain.reshape(1, -1),
        query_norm_gain.reshape(1, -1), key_norm_gain.reshape(1, -1),
        jnp.broadcast_to(frequency[:, None], (8, 128)),
        latent_tokens, query_down, kv_down, rope_down.T, query_up, key_up, value_up,
        context_latent, context_rope.T,
    )
    return back(
        qkv, clat, crope, key_up, value_up, key_norm_gain.reshape(1, -1), context_lift,
        latent_tokens, gates, out_weight,
    )


def solution(mesh):
    in_specs = (
        P(("dp", "sp", "tp"), None), P(("dp", "sp")), P("sp", "tp"), P("sp", "tp"), P("sp", "tp"),
        P(), P(), P(), P(), P(), P(), P(None, "tp"), P(None, "tp"), P(None, "tp"), P(), P(),
        P("tp", None), P(("dp", "sp"), None), P(("dp", "sp"), None), P("tp"),
    )
    return jax.shard_map(
        local, mesh=mesh, in_specs=in_specs, out_specs=P(("dp", "sp", "tp"), None), check_vma=False
    )
```

```python
import jax
import jax.numpy as jnp
from jax import lax
from jax.experimental import pallas as pl
from jax.experimental.pallas import tpu as pltpu
from jax.sharding import PartitionSpec as P

NOPE_DIM = 64
ROPE_DIM = 32
VALUE_DIM = 64
QK_DIM = 96
GRID_W = 64
EPS = 1e-06
THETA = 10000.0
LOG2E = 1.4426950408889634

F32 = jnp.float32
BF16 = jnp.bfloat16
MESH = pl.DeviceIdType.MESH
VMEM = pl.BlockSpec(memory_space=pltpu.VMEM)


CHUNK = 1536
TILE = 512
SUB = 256
STEPS = CHUNK // SUB
PIECE = (0, 3, 1, 2)
OPPOSITE = (0, 2, 1, 3)


def send(src, dst, send_sem, recv_sem, to):
    c = pltpu.make_async_remote_copy(
        src_ref=src, dst_ref=dst, send_sem=send_sem, recv_sem=recv_sem, device_id=to, device_id_type=MESH
    )
    c.start()
    return c


def dot(a, b):
    return jnp.dot(a, b, preferred_element_type=F32)


def turned(rows, cosine, sine):
    out = []
    for a in range(2):
        u, w = rows[16 * a : 16 * a + 8], rows[16 * a + 8 : 16 * a + 16]
        out += [u * cosine[a] - w * sine[a], w * cosine[a] + u * sine[a]]
    return jnp.concatenate(out, axis=0)


def column(row):
    row = jnp.concatenate([row, jnp.zeros((1, 32), F32)], axis=1)
    return jnp.broadcast_to(row, (128, 128)).T[:QK_DIM]


def kernel(
    cond_hbm, shift_hbm, scale_hbm, gate_hbm, ng_hbm, qgain_hbm, kvgain_hbm, qng_hbm, kng_hbm, freq_hbm,
    x_hbm, qd_hbm, kvd_hbm, rd_hbm, qw_hbm, kw_hbm, vw_hbm, lat_hbm, rope_hbm, wout_hbm, lift_ref,
    out_ref,
    cond_s, mw_s, ng_s, qgain_s, kvgain_s, qng_s, kng_s, freq_s,
    x_s, qd_s, kvd_s, rd_s, qw_s, kw_s, vw_s, clat_s, crope_s,
    near_s, near_g, wide_s, wide_g, gates_s, ql_s, kl_s, rk_s,
    qkv_s, q_in, kvs, q_s, k_s, v_s, s_s, m_s, top_s, acc_s, att_s, slots, w_s,
    s_near, r_near, s_neg, r_neg, s_wide, r_wide, s_wig, r_wig, s_lat, r_lat, s_rope, r_rope,
    s_ql, r_ql, s_kl, r_kl, s_rk, r_rk, s_q, r_q, s_kv, r_kv,
    s_up, r_up, s_down, r_down, s_far, r_far, s_att, r_att, s_w, r_w, s_wc, r_wc, local_sem, block_sem,
):
    sp, tp, core = lax.axis_index("sp"), lax.axis_index("tp"), lax.axis_index("dp")
    z, x = sp // 4, lax.rem(sp, 4)
    a, b = z + core * (x - z), x + core * (z - x)

    def at(da, db, dy):
        aa, bb = lax.rem(a + da, 4), lax.rem(b + db, 4)
        return {"sp": aa * (4 - 3 * core) + bb * (1 + 3 * core), "tp": lax.rem(tp + dy, 4)}

    def along_tp(k):
        return {"tp": lax.rem(tp + k, 4)}

    def along_sp(r):
        return {"sp": lax.rem(sp + r, 16)}

    partner, y_up, y_down = {"dp": 1 - core}, along_tp(1), along_tp(3)
    a_up, a_down = at(1, 0, 0), at(3, 0, 0)
    barrier = pltpu.get_barrier_semaphore()
    greeted = [along_tp(k) for k in range(1, 4)] + [along_sp(r) for r in range(1, 16)] + [partner]
    greeted += [at(0, db, dy) for dy in range(1, 4) for db in range(1, 4)]
    for to in greeted:
        pl.semaphore_signal(barrier, inc=1, device_id=to, device_id_type=MESH)
    own = []

    def fetch(src, dst):
        c = pltpu.make_async_copy(src, dst, local_sem.at[len(own)])
        c.start()
        own.append(c)

    for src, dst in (
        (cond_hbm, cond_s), (shift_hbm, mw_s.at[0]), (scale_hbm, mw_s.at[1]), (gate_hbm, mw_s.at[2]),
        (freq_hbm, freq_s), (qng_hbm, qng_s), (kng_hbm, kng_s), (x_hbm, x_s), (ng_hbm, ng_s),
        (qd_hbm, qd_s), (kvd_hbm, kvd_s), (rd_hbm, rd_s), (qgain_hbm, qgain_s), (kvgain_hbm, kvgain_s),
        (qw_hbm, qw_s), (kw_hbm, kw_s), (vw_hbm, vw_s), (lat_hbm, clat_s.at[0]), (rope_hbm, crope_s.at[0]),
        (wout_hbm.at[0:128], w_s.at[0, 0]), (wout_hbm.at[128:256], w_s.at[0, 1]),
    ):
        fetch(src, dst)

    for c in own[:4]:
        c.wait()
    cond = cond_s[...].astype(F32)
    active = cond / (1.0 + jnp.exp(-cond))
    active = jnp.broadcast_to(active, (16, 128)).astype(BF16)
    for i in range(3):
        row = dot(active, mw_s[i])
        for j in range(4):
            piece = row[0:1, 128 * j : 128 * j + 128]
            if i < 2:
                near_s[tp, 4 * i + j : 4 * i + j + 1, :] = piece
            else:
                near_g[tp, j : j + 1, :] = piece
    near_g[tp, 4:8, :] = jnp.zeros((4, 128), F32)
    pl.semaphore_wait(barrier, len(greeted))

    nears, negs = [], []
    for k in range(1, 4):
        nears.append(send(near_s.at[tp], near_s.at[tp], s_near.at[k], r_near.at[k], along_tp(k)))
    for k in range(1, 4):
        negs.append(send(near_g.at[tp], near_g.at[tp], s_neg.at[k], r_neg.at[k], along_tp(k)))

    weights = [[], []]

    def weights_near(part):
        rows, src = pl.ds(64 * part, 64), wout_hbm.at[pl.ds(core * 128 + 64 * part, 64)]
        i = 2 * part
        weights[part].append(send(src, w_s.at[1, core, rows], s_w.at[i], r_w.at[i], y_up))
        weights[part].append(send(src, w_s.at[2, core, rows], s_w.at[i + 1], r_w.at[i + 1], y_down))

    weights_near(0)

    for c in nears:
        c.wait_recv()
    wides, wigs, rest = [], [], []
    for r in range(1, 16):
        wides.append(send(near_s, wide_s.at[r], s_wide.at[r], r_wide.at[r], along_sp(r)))
    for c in negs:
        c.wait_recv()
    for r in range(1, 16):
        wigs.append(send(near_g, wide_g.at[r], s_wig.at[r], r_wig.at[r], along_sp(r)))
    for r in range(1, 16):
        rest.append(send(lat_hbm, clat_s.at[r], s_lat.at[r], r_lat.at[r], along_sp(r)))
        rest.append(send(rope_hbm, crope_s.at[r], s_rope.at[r], r_rope.at[r], along_sp(r)))

    for c in own[4:]:
        c.wait()
    lane = lax.broadcasted_iota(jnp.int32, (8, 128), 1)
    column_angle = lax.rem(lane, GRID_W).astype(F32) * freq_s[...]
    column_cosine, column_sine = jnp.cos(column_angle), jnp.sin(column_angle)
    tables = []
    for p in range(4):
        row = (sp * 4 + lax.rem(tp + PIECE[p], 4)) * 2 + lane // GRID_W
        angle = row.astype(F32) * freq_s[...]
        tables.append(((jnp.cos(angle), column_cosine), (jnp.sin(angle), column_sine)))
    q_gain = column(qng_s[...] * (LOG2E * QK_DIM**-0.5))
    k_gain = column(kng_s[...])
    for i in range(2):
        v_s[i, VALUE_DIM:80, :] = jnp.ones((16, CHUNK), BF16)
    for t in range(4):
        q_s[t, QK_DIM:128, :] = jnp.ones((32, TILE), BF16)
    m_s[...] = jnp.full(m_s.shape, -1e30, F32)
    acc_s[...] = jnp.zeros(acc_s.shape, F32)
    values = x_s[...].astype(F32)
    mean_square = jnp.mean(values * values, axis=-1, keepdims=True)
    scaled = values * lax.rsqrt(mean_square + EPS) * ng_s[...]

    total = near_s[...]
    for r in range(1, 16):
        wides[r - 1].wait_recv()
        total = total + wide_s[r]
    mod = [
        jnp.concatenate([total[i, 4 * k + j : 4 * k + j + 1] for i in range(4) for j in range(4)], axis=1)
        for k in range(2)
    ]
    normed = (scaled * (1.0 + mod[1]) + mod[0]).astype(BF16)

    def latent(w, gain_ref):
        y = dot(normed, w[...])
        m = jnp.mean(y * y, axis=-1, keepdims=True)
        return (y * lax.rsqrt(m + EPS) * gain_ref[...]).astype(BF16)

    rk = lax.dot_general(rd_s[...], normed, (((1,), (1,)), ((), ())), preferred_element_type=F32)
    rk_s[0] = rk.astype(BF16)
    kl_s[0] = latent(kvd_s, kvgain_s)
    ql_s[0] = latent(qd_s, qgain_s)
    gates = near_g[...]
    for r in range(1, 16):
        wigs[r - 1].wait_recv()
        gates = gates + wide_g[r]
    gates_s[...] = gates
    latents = [[], [], [], []]
    for p, to in ((1, y_up), (2, y_down)):
        latents[p].append(send(kl_s.at[0], kl_s.at[p], s_kl.at[p], r_kl.at[p], to))
        latents[p].append(send(rk_s.at[0], rk_s.at[p], s_rk.at[p], r_rk.at[p], to))
        latents[p].append(send(ql_s.at[0], ql_s.at[p], s_ql.at[p], r_ql.at[p], to))

    q_copies, kv_copies, own_kv = {}, {}, []

    def expand(p):
        for c in latents[p]:
            c.wait_recv()
        if p == 2:
            latents[3].append(send(ql_s.at[1], ql_s.at[3], s_ql.at[3], r_ql.at[3], y_up))
            latents[3].append(send(kl_s.at[2], kl_s.at[3], s_kl.at[3], r_kl.at[3], y_down))
            latents[3].append(send(rk_s.at[2], rk_s.at[3], s_rk.at[3], r_rk.at[3], y_down))
            weights_near(1)
        cosine, sine = tables[p]
        rk = rk_s[p].astype(F32)
        rk_square = jnp.sum(rk * rk, axis=0, keepdims=True)
        q, kn, vv = dot(ql_s[p], qw_s[...]).T, dot(kl_s[p], kw_s[...]).T, dot(kl_s[p], vw_s[...]).T
        for j in range(4):
            qh = q[QK_DIM * j : QK_DIM * (j + 1)]
            inv = lax.rsqrt(jnp.sum(qh * qh, axis=0, keepdims=True) * (1.0 / QK_DIM) + EPS)
            qh = qh * inv * q_gain
            qh = jnp.concatenate([qh[:NOPE_DIM], turned(qh[NOPE_DIM:], cosine, sine)], axis=0)
            qkv_s[p, j, 0:QK_DIM, :] = qh.astype(BF16)
            kh = kn[NOPE_DIM * j : NOPE_DIM * (j + 1)]
            square = jnp.sum(kh * kh, axis=0, keepdims=True) + rk_square
            inv = lax.rsqrt(square * (1.0 / QK_DIM) + EPS)
            kr = turned(rk * inv * k_gain[NOPE_DIM:], cosine, sine)
            kh = kh * inv * k_gain[:NOPE_DIM]
            qkv_s[p, j, QK_DIM : QK_DIM + NOPE_DIM, :] = kh.astype(BF16)
            qkv_s[p, j, QK_DIM + NOPE_DIM : 2 * QK_DIM, :] = kr.astype(BF16)
            qkv_s[p, j, 2 * QK_DIM : 256, :] = vv[VALUE_DIM * j : VALUE_DIM * (j + 1)].astype(BF16)
        c = pltpu.make_async_copy(qkv_s.at[p, b, QK_DIM:256], kvs.at[0, 4 * p], block_sem.at[p])
        c.start()
        own_kv.append(c)
        for db in range(1, 4):
            r, block = 4 * p + db, qkv_s.at[p, lax.rem(b + db, 4)]
            q_copies[r] = send(block.at[0:QK_DIM], q_in.at[r], s_q.at[r], r_q.at[r], at(0, db, 0))
        for db in range(1, 4):
            r, block = 4 * p + db, qkv_s.at[p, lax.rem(b + db, 4)]
            kv_copies[r] = send(block.at[QK_DIM:256], kvs.at[0, r], s_kv.at[r], r_kv.at[r], at(0, db, 0))

    expand(0)

    def own_head(w_ref):
        w = w_ref[...].astype(F32)
        w = jnp.where(b < 2, w[:, :128], w[:, 128:])
        return jnp.where(lax.rem(b, 2) == 0, w, pltpu.roll(w, 64, 1)).astype(BF16)

    for c in rest:
        c.wait_recv()
    clat = clat_s[...].reshape(1024, 256)
    kn = dot(clat, own_head(kw_s))
    lane = lax.broadcasted_iota(jnp.int32, (1, 128), 1)
    ropes = []
    for i in range(8):
        two = jnp.concatenate([crope_s[2 * i], crope_s[2 * i + 1]], axis=1).astype(F32)
        two = jnp.concatenate([jnp.zeros((64, 128), F32), two, jnp.zeros((32, 128), F32)], axis=0)
        ropes.append(two.T)
    key = jnp.where(lane < NOPE_DIM, kn, jnp.concatenate(ropes, axis=0))
    inv = lax.rsqrt(jnp.sum(key * key, axis=1, keepdims=True) * (1.0 / QK_DIM) + EPS)
    gain = jnp.concatenate([kng_s[...], jnp.zeros((1, 32), F32)], axis=1)
    lift = jnp.full((1, 128), lift_ref[b] * LOG2E, F32)
    high = lift.astype(BF16).astype(F32)
    middle = (lift - high).astype(BF16).astype(F32)
    low = lift - high - middle
    extra = jnp.where(lane == 96, high, jnp.where(lane == 97, middle, jnp.where(lane == 98, low, 0.0)))
    k_s[0, 0:1024, :] = (key * inv * gain + extra).astype(BF16)
    vv = dot(clat, own_head(vw_s)).T
    v_s[0, 0:VALUE_DIM, 0:1024] = vv[:VALUE_DIM].astype(BF16)

    def place(chunk, first, blocks):
        for i, (slot, r) in enumerate(blocks):
            at_key = first + 128 * i
            block = kvs[slot, r]
            kt = jnp.concatenate([block[:QK_DIM].astype(F32), jnp.zeros((32, 128), F32)], axis=0)
            k_s[chunk % 2, at_key : at_key + 128, :] = kt.T.astype(BF16)
            v_s[chunk % 2, 0:VALUE_DIM, at_key : at_key + 128] = block[QK_DIM:]

    def take_queries(p):
        q_s[p, 0:QK_DIM, 0:128] = qkv_s[p, b, 0:QK_DIM]
        for db in range(1, 4):
            q_copies[4 * p + db].wait_recv()
            q_s[p, 0:QK_DIM, 128 * db : 128 * db + 128] = q_in[4 * p + db]

    ups, downs, far = [], [], []

    def spread(g):
        own_kv[g].wait()
        for db in range(1, 4):
            kv_copies[4 * g + db].wait_recv()
        rows = pl.ds(4 * g, 4)
        ups.append(send(kvs.at[0, rows], kvs.at[1, rows], s_up.at[g], r_up.at[g], a_up))
        downs.append(send(kvs.at[0, rows], kvs.at[2, rows], s_down.at[g], r_down.at[g], a_down))

    def farther(g):
        rows = pl.ds(4 * g, 4)
        slot, to = (1, a_up) if g < 2 else (2, a_down)
        far.append(send(kvs.at[slot, rows], kvs.at[3, rows], s_far.at[g], r_far.at[g], to))

    def rows_of(slot, *groups):
        return [(slot, 4 * g + i) for g in groups for i in range(4)]

    weights_far, shared = [], []

    def forward_weights(part):
        for c in weights[part]:
            c.wait_recv()
        rows = pl.ds(64 * part, 64)
        to = y_down if part else y_up
        weights_far.append(
            send(w_s.at[1 + part, core, rows], w_s.at[3, core, rows], s_w.at[4 + part], r_w.at[4 + part], to)
        )

    def share_weights(k):
        shared.append(send(w_s.at[k, core], w_s.at[k, core], s_wc.at[k], r_wc.at[k], partner))

    def prepare(chunk):
        if chunk == 0:
            spread(0)
            place(0, 1024, rows_of(0, 0))
        elif chunk == 1:
            for g in range(1, 4):
                spread(g)
            place(1, 0, rows_of(0, 1, 2, 3))
        elif chunk == 2:
            for g in range(3):
                ups[g].wait_recv()
            farther(0)
            farther(1)
            place(2, 0, rows_of(1, 0, 1, 2))
        elif chunk == 3:
            for g in range(1, 4):
                downs[g].wait_recv()
            farther(2)
            farther(3)
            place(3, 0, rows_of(2, 1, 2, 3))
        elif chunk == 4:
            ups[3].wait_recv()
            downs[0].wait_recv()
            far[0].wait_recv()
            place(4, 0, rows_of(1, 3) + rows_of(2, 0) + rows_of(3, 0))
            forward_weights(1)
            share_weights(1)
            share_weights(2)
        else:
            for g in range(1, 4):
                far[g].wait_recv()
            place(5, 0, rows_of(3, 1, 2, 3))

    def score(chunk, t, i):
        rows = slice(i * SUB, (i + 1) * SUB)
        s = dot(k_s[chunk % 2, rows], q_s[t])
        s_s[rows] = s
        return jnp.max(s.reshape(SUB // 8, 8, TILE), axis=0)

    def step(chunk, t, later_chunk, later):
        old = m_s[t]
        new = jnp.maximum(old, jnp.max(top_s[...], axis=0, keepdims=True))
        m_s[t] = new
        acc = acc_s[t] * jnp.exp2(old - new)
        top = None
        for i in range(STEPS):
            rows = slice(i * SUB, (i + 1) * SUB)
            p = jnp.exp2(s_s[rows] - new).astype(BF16)
            acc = acc + dot(v_s[chunk % 2, :, rows], p)
            if later is not None:
                part = score(later_chunk, later, i)
                top = part if top is None else jnp.maximum(top, part)
        acc_s[t] = acc
        if later is not None:
            top_s[...] = top

    att_copies = []

    def finish(t):
        acc = acc_s[t]
        o = (acc[:VALUE_DIM] / acc[VALUE_DIM : VALUE_DIM + 1]).astype(BF16)
        for i in range(4):
            att_s[4 * t + i] = o[:, 128 * i : 128 * i + 128]

    def give(p):
        for db in range(4):
            r = 4 * p + db
            if r:
                att_copies.append(
                    send(
                        att_s.at[r], slots.at[OPPOSITE[p], b], s_att.at[r], r_att.at[r],
                        at(0, (4 - db) % 4, PIECE[p]),
                    )
                )
            else:
                slots[0, b] = att_s[0]

    expand(1)
    expand(2)
    take_queries(0)
    prepare(0)
    top = None
    for i in range(STEPS):
        part = score(0, 0, i)
        top = part if top is None else jnp.maximum(top, part)
    top_s[...] = top
    take_queries(1)
    step(0, 0, 0, 1)
    expand(3)
    forward_weights(0)
    take_queries(2)
    step(0, 1, 0, 2)
    take_queries(3)
    step(0, 2, 0, 3)
    prepare(1)
    step(0, 3, 1, 0)
    for chunk in range(1, 6):
        if chunk < 5:

            def some_tile(t, carry, chunk=chunk):
                step(chunk, t, chunk, t + 1)
                return carry

            lax.fori_loop(0, 3, some_tile, 0)
            prepare(chunk + 1)
            step(chunk, 3, chunk + 1, 0)
        else:
            for t in range(4):
                step(chunk, t, chunk, t + 1 if t < 3 else None)
                finish(t)
                if t:
                    give(t - 1)
                if t == 1:
                    for c in weights_far:
                        c.wait_recv()
                    share_weights(3)
            give(3)

    for c in shared + att_copies:
        c.wait_recv()
    atts = [slots[k].reshape(256, 128).astype(F32).T.astype(BF16) for k in range(4)]
    gate = [gates_s[i, j : j + 1, :] for i in range(4) for j in range(4)]
    for n in range(4):
        cols = slice(512 * n, 512 * n + 512)
        mixed = None
        for k in range(4):
            term = dot(atts[k], w_s[k, :, :, cols].reshape(256, 512)).astype(BF16).astype(F32)
            mixed = term if mixed is None else mixed + term
        gated = jnp.concatenate(gate[4 * n : 4 * n + 4], axis=1)
        out_ref[:, cols] = (x_s[:, cols].astype(F32) + gated * mixed).astype(BF16)
    sent = nears + negs + wides + wigs + rest + list(q_copies.values()) + list(kv_copies.values())
    sent += ups + downs + far + weights[0] + weights[1] + weights_far + shared + att_copies
    for group in latents:
        sent += group
    for c in sent:
        c.wait_send()


def everything(*args):
    dma, vmem = pltpu.SemaphoreType.DMA, pltpu.VMEM
    hbm = pl.BlockSpec(memory_space=pltpu.HBM)
    return pl.pallas_call(
        kernel,
        out_shape=jax.ShapeDtypeStruct((128, 2048), BF16),
        in_specs=[hbm] * 20 + [pl.BlockSpec(memory_space=pltpu.SMEM)],
        out_specs=VMEM,
        scratch_shapes=[
            vmem((1, 128), BF16), vmem((3, 128, 512), BF16), vmem((1, 2048), F32), vmem((1, 512), F32),
            vmem((1, 256), F32), vmem((1, 96), F32), vmem((1, 96), F32), vmem((8, 128), F32),
            vmem((128, 2048), BF16), vmem((2048, 512), BF16), vmem((2048, 256), BF16), vmem((32, 2048), BF16),
            vmem((512, 384), BF16), vmem((256, 256), BF16), vmem((256, 256), BF16),
            vmem((16, 64, 256), BF16), vmem((16, 32, 64), BF16),
            vmem((4, 8, 128), F32), vmem((4, 8, 128), F32),
            vmem((16, 4, 8, 128), F32), vmem((16, 4, 8, 128), F32), vmem((4, 8, 128), F32),
            vmem((4, 128, 512), BF16), vmem((4, 128, 256), BF16), vmem((4, 32, 128), BF16),
            vmem((4, 4, 256, 128), BF16), vmem((16, QK_DIM, 128), BF16), vmem((4, 16, 160, 128), BF16),
            vmem((4, 128, TILE), BF16), vmem((2, CHUNK, 128), BF16), vmem((2, 80, CHUNK), BF16),
            vmem((CHUNK, TILE), F32), vmem((4, 1, TILE), F32), vmem((8, TILE), F32), vmem((4, 80, TILE), F32),
            vmem((16, VALUE_DIM, 128), BF16), vmem((4, 4, VALUE_DIM, 128), BF16), vmem((4, 2, 128, 2048), BF16),
            dma((4,)), dma((4,)), dma((4,)), dma((4,)),
            dma((16,)), dma((16,)), dma((16,)), dma((16,)), dma((16,)), dma((16,)), dma((16,)), dma((16,)),
            dma((4,)), dma((4,)), dma((4,)), dma((4,)), dma((4,)), dma((4,)),
            dma((16,)), dma((16,)), dma((16,)), dma((16,)),
            dma((4,)), dma((4,)), dma((4,)), dma((4,)), dma((4,)), dma((4,)), dma((16,)), dma((16,)),
            dma((6,)), dma((6,)), dma((4,)), dma((4,)), dma((21,)), dma((4,)),
        ],
        compiler_params=pltpu.CompilerParams(
            collective_id=0, has_side_effects=True, vmem_limit_bytes=67_043_328
        ),
        cost_estimate=pl.CostEstimate(
            flops=10_000_000_000, bytes_accessed=8_000_000, transcendentals=19_000_000
        ),
        name="everything",
    )(*args)


def local(
    latent_tokens, condition, shift_weight, scale_weight, gate_weight, norm_gain, query_down, query_gain,
    kv_down, kv_gain, rope_down, query_up, key_up, value_up, query_norm_gain, key_norm_gain, out_weight,
    context_latent, context_rope, context_lift,
):
    frequency = THETA ** (-4.0 * jnp.arange(8, dtype=F32) / ROPE_DIM)
    return everything(
        condition.reshape(1, 128), shift_weight, scale_weight, gate_weight,
        norm_gain.reshape(1, -1), query_gain.reshape(1, -1), kv_gain.reshape(1, -1),
        query_norm_gain.reshape(1, -1), key_norm_gain.reshape(1, -1),
        jnp.broadcast_to(frequency[:, None], (8, 128)),
        latent_tokens, query_down, kv_down, rope_down.T, query_up, key_up, value_up,
        context_latent, context_rope.T, out_weight, context_lift,
    )


def solution(mesh):
    in_specs = (
        P(("dp", "sp", "tp"), None), P(("dp", "sp")), P("sp", "tp"), P("sp", "tp"), P("sp", "tp"),
        P(), P(), P(), P(), P(), P(), P(None, "tp"), P(None, "tp"), P(None, "tp"), P(), P(),
        P("tp", None), P(("dp", "sp"), None), P(("dp", "sp"), None), P("tp"),
    )
    return jax.shard_map(
        local, mesh=mesh, in_specs=in_specs, out_specs=P(("dp", "sp", "tp"), None), check_vma=False
    )
```

```python
import jax
import jax.numpy as jnp
from jax import lax
from jax.experimental import pallas as pl
from jax.experimental.pallas import tpu as pltpu
from jax.sharding import PartitionSpec as P

NOPE_DIM = 64
ROPE_DIM = 32
VALUE_DIM = 64
QK_DIM = 96
GRID_W = 64
EPS = 1e-06
THETA = 10000.0
LOG2E = 1.4426950408889634

F32 = jnp.float32
BF16 = jnp.bfloat16
MESH = pl.DeviceIdType.MESH
VMEM = pl.BlockSpec(memory_space=pltpu.VMEM)


CHUNK = 1536
TILE = 512
SUB = 256
STEPS = CHUNK // SUB
PIECE = (0, 3, 1, 2)
OPPOSITE = (0, 2, 1, 3)


def send(src, dst, send_sem, recv_sem, to):
    c = pltpu.make_async_remote_copy(
        src_ref=src, dst_ref=dst, send_sem=send_sem, recv_sem=recv_sem, device_id=to, device_id_type=MESH
    )
    c.start()
    return c


def dot(a, b):
    return jnp.dot(a, b, preferred_element_type=F32)


def turned(rows, cosine, sine):
    out = []
    for a in range(2):
        u, w = rows[16 * a : 16 * a + 8], rows[16 * a + 8 : 16 * a + 16]
        out += [u * cosine[a] - w * sine[a], w * cosine[a] + u * sine[a]]
    return jnp.concatenate(out, axis=0)


def column(row):
    row = jnp.concatenate([row, jnp.zeros((1, 32), F32)], axis=1)
    return jnp.broadcast_to(row, (128, 128)).T[:QK_DIM]


def kernel(
    cond_hbm, shift_hbm, scale_hbm, gate_hbm, ng_hbm, qgain_hbm, kvgain_hbm, qng_hbm, kng_hbm, freq_hbm,
    x_hbm, qd_hbm, kvd_hbm, rd_hbm, qw_hbm, kw_hbm, vw_hbm, lat_hbm, rope_hbm, wout_hbm, lift_ref,
    out_ref,
    cond_s, mw_s, ng_s, qgain_s, kvgain_s, qng_s, kng_s, freq_s,
    x_s, qd_s, kvd_s, rd_s, qw_s, kw_s, vw_s, clat_s, crope_s,
    part_s, wide_s, mods_s, ql_s, kl_s, rk_s,
    qkv_s, q_in, kvs, q_s, k_s, v_s, s_s, m_s, top_s, acc_s, att_s, slots, w_s,
    s_near, r_near, s_wide, r_wide, s_lat, r_lat, s_rope, r_rope,
    s_ql, r_ql, s_kl, r_kl, s_rk, r_rk, s_q, r_q, s_kv, r_kv,
    s_up, r_up, s_down, r_down, s_far, r_far, s_att, r_att, s_w, r_w, s_wc, r_wc, local_sem, block_sem,
):
    sp, tp, core = lax.axis_index("sp"), lax.axis_index("tp"), lax.axis_index("dp")
    z, x = sp // 4, lax.rem(sp, 4)
    a, b = z + core * (x - z), x + core * (z - x)

    def at(da, db, dy):
        aa, bb = lax.rem(a + da, 4), lax.rem(b + db, 4)
        return {"sp": aa * (4 - 3 * core) + bb * (1 + 3 * core), "tp": lax.rem(tp + dy, 4)}

    def along_tp(k):
        return {"tp": lax.rem(tp + k, 4)}

    def along_sp(r):
        return {"sp": lax.rem(sp + r, 16)}

    partner, y_up, y_down = {"dp": 1 - core}, along_tp(1), along_tp(3)
    a_up, a_down = at(1, 0, 0), at(3, 0, 0)
    barrier = pltpu.get_barrier_semaphore()
    greeted = [along_tp(k) for k in range(1, 4)] + [along_sp(r) for r in range(1, 16)] + [partner]
    greeted += [at(0, db, dy) for dy in range(1, 4) for db in range(1, 4)]
    for to in greeted:
        pl.semaphore_signal(barrier, inc=1, device_id=to, device_id_type=MESH)
    own = []

    def fetch(src, dst):
        c = pltpu.make_async_copy(src, dst, local_sem.at[len(own)])
        c.start()
        own.append(c)

    for src, dst in (
        (cond_hbm, cond_s), (shift_hbm, mw_s.at[0]), (scale_hbm, mw_s.at[1]), (gate_hbm, mw_s.at[2]),
        (freq_hbm, freq_s), (qng_hbm, qng_s), (kng_hbm, kng_s), (x_hbm, x_s), (ng_hbm, ng_s),
        (qd_hbm, qd_s), (kvd_hbm, kvd_s), (rd_hbm, rd_s), (qgain_hbm, qgain_s), (kvgain_hbm, kvgain_s),
        (qw_hbm, qw_s), (kw_hbm, kw_s), (vw_hbm, vw_s), (lat_hbm, clat_s.at[0]), (rope_hbm, crope_s.at[0]),
        (wout_hbm.at[0:128], w_s.at[0, 0]), (wout_hbm.at[128:256], w_s.at[0, 1]),
    ):
        fetch(src, dst)

    for c in own[:4]:
        c.wait()
    cond = cond_s[...].astype(F32)
    active = cond / (1.0 + jnp.exp(-cond))
    active = jnp.broadcast_to(active, (16, 128)).astype(BF16)
    for i in range(3):
        row = dot(active, mw_s[i])
        for j in range(4):
            piece = row[0:1, 128 * j : 128 * j + 128]
            part_s[4 * i + j : 4 * i + j + 1, :] = piece
    part_s[12:16, :] = jnp.zeros((4, 128), F32)
    pl.semaphore_wait(barrier, len(greeted))

    wides, nears, rest = [], [], []
    for r in range(1, 16):
        wides.append(send(part_s, wide_s.at[r], s_wide.at[r], r_wide.at[r], along_sp(r)))
    for r in range(1, 16):
        rest.append(send(lat_hbm, clat_s.at[r], s_lat.at[r], r_lat.at[r], along_sp(r)))
        rest.append(send(rope_hbm, crope_s.at[r], s_rope.at[r], r_rope.at[r], along_sp(r)))
    total = part_s[...]
    for r in range(1, 16):
        wides[r - 1].wait_recv()
        total = total + wide_s[r]
    mods_s[tp] = total
    for k in range(1, 4):
        nears.append(send(mods_s.at[tp], mods_s.at[tp], s_near.at[k], r_near.at[k], along_tp(k)))

    weights = [[], []]

    def weights_near(part):
        rows, src = pl.ds(64 * part, 64), wout_hbm.at[pl.ds(core * 128 + 64 * part, 64)]
        i = 2 * part
        weights[part].append(send(src, w_s.at[1, core, rows], s_w.at[i], r_w.at[i], y_up))
        weights[part].append(send(src, w_s.at[2, core, rows], s_w.at[i + 1], r_w.at[i + 1], y_down))

    for c in own[4:]:
        c.wait()
    lane = lax.broadcasted_iota(jnp.int32, (8, 128), 1)
    column_angle = lax.rem(lane, GRID_W).astype(F32) * freq_s[...]
    column_cosine, column_sine = jnp.cos(column_angle), jnp.sin(column_angle)
    tables = []
    for p in range(4):
        row = (sp * 4 + lax.rem(tp + PIECE[p], 4)) * 2 + lane // GRID_W
        angle = row.astype(F32) * freq_s[...]
        tables.append(((jnp.cos(angle), column_cosine), (jnp.sin(angle), column_sine)))
    q_gain = column(qng_s[...] * (LOG2E * QK_DIM**-0.5))
    k_gain = column(kng_s[...])
    for i in range(2):
        v_s[i, VALUE_DIM:80, :] = jnp.ones((16, CHUNK), BF16)
    for t in range(4):
        q_s[t, QK_DIM:128, :] = jnp.ones((32, TILE), BF16)
    m_s[...] = jnp.full(m_s.shape, -1e30, F32)
    acc_s[...] = jnp.zeros(acc_s.shape, F32)
    values = x_s[...].astype(F32)
    mean_square = jnp.mean(values * values, axis=-1, keepdims=True)
    scaled = values * lax.rsqrt(mean_square + EPS) * ng_s[...]

    for c in nears:
        c.wait_recv()
    shift, scale = [
        jnp.concatenate([mods_s[i, j : j + 1, :] for i in range(4) for j in range(4 * k, 4 * k + 4)], axis=1)
        for k in range(2)
    ]
    normed = (scaled * (1.0 + scale) + shift).astype(BF16)

    def latent(w, gain_ref):
        y = dot(normed, w[...])
        m = jnp.mean(y * y, axis=-1, keepdims=True)
        return (y * lax.rsqrt(m + EPS) * gain_ref[...]).astype(BF16)

    rk = lax.dot_general(rd_s[...], normed, (((1,), (1,)), ((), ())), preferred_element_type=F32)
    rk_s[0] = rk.astype(BF16)
    kl_s[0] = latent(kvd_s, kvgain_s)
    ql_s[0] = latent(qd_s, qgain_s)
    latents = [[], [], [], []]
    for p, to in ((1, y_up), (2, y_down)):
        latents[p].append(send(kl_s.at[0], kl_s.at[p], s_kl.at[p], r_kl.at[p], to))
        latents[p].append(send(rk_s.at[0], rk_s.at[p], s_rk.at[p], r_rk.at[p], to))
        latents[p].append(send(ql_s.at[0], ql_s.at[p], s_ql.at[p], r_ql.at[p], to))

    q_copies, kv_copies, own_kv = {}, {}, []

    def expand(p):
        for c in latents[p][2:] if p == 2 else latents[p][:2] if p == 1 else latents[p]:
            c.wait_recv()
        cosine, sine = tables[p]
        rk = rk_s[p].astype(F32)
        rk_square = jnp.sum(rk * rk, axis=0, keepdims=True)
        q, kn, vv = dot(ql_s[p], qw_s[...]).T, dot(kl_s[p], kw_s[...]).T, dot(kl_s[p], vw_s[...]).T
        for j in range(4):
            qh = q[QK_DIM * j : QK_DIM * (j + 1)]
            inv = lax.rsqrt(jnp.sum(qh * qh, axis=0, keepdims=True) * (1.0 / QK_DIM) + EPS)
            qh = qh * inv * q_gain
            qh = jnp.concatenate([qh[:NOPE_DIM], turned(qh[NOPE_DIM:], cosine, sine)], axis=0)
            qkv_s[p, j, 0:QK_DIM, :] = qh.astype(BF16)
            kh = kn[NOPE_DIM * j : NOPE_DIM * (j + 1)]
            square = jnp.sum(kh * kh, axis=0, keepdims=True) + rk_square
            inv = lax.rsqrt(square * (1.0 / QK_DIM) + EPS)
            kr = turned(rk * inv * k_gain[NOPE_DIM:], cosine, sine)
            kh = kh * inv * k_gain[:NOPE_DIM]
            qkv_s[p, j, QK_DIM : QK_DIM + NOPE_DIM, :] = kh.astype(BF16)
            qkv_s[p, j, QK_DIM + NOPE_DIM : 2 * QK_DIM, :] = kr.astype(BF16)
            qkv_s[p, j, 2 * QK_DIM : 256, :] = vv[VALUE_DIM * j : VALUE_DIM * (j + 1)].astype(BF16)
        c = pltpu.make_async_copy(qkv_s.at[p, b, QK_DIM:256], kvs.at[0, 4 * p], block_sem.at[p])
        c.start()
        own_kv.append(c)
        for db in range(1, 4):
            r, block = 4 * p + db, qkv_s.at[p, lax.rem(b + db, 4)]
            q_copies[r] = send(block.at[0:QK_DIM], q_in.at[r], s_q.at[r], r_q.at[r], at(0, db, 0))
        for db in range(1, 4):
            r, block = 4 * p + db, qkv_s.at[p, lax.rem(b + db, 4)]
            kv_copies[r] = send(block.at[QK_DIM:256], kvs.at[0, r], s_kv.at[r], r_kv.at[r], at(0, db, 0))

    def place(chunk, first, blocks):
        for i, (slot, r) in enumerate(blocks):
            at_key = first + 128 * i
            block = kvs[slot, r]
            kt = jnp.concatenate([block[:QK_DIM].astype(F32), jnp.zeros((32, 128), F32)], axis=0)
            k_s[chunk % 2, at_key : at_key + 128, :] = kt.T.astype(BF16)
            v_s[chunk % 2, 0:VALUE_DIM, at_key : at_key + 128] = block[QK_DIM:]

    def take_queries(p):
        q_s[p, 0:QK_DIM, 0:128] = qkv_s[p, b, 0:QK_DIM]
        for db in range(1, 4):
            q_copies[4 * p + db].wait_recv()
            q_s[p, 0:QK_DIM, 128 * db : 128 * db + 128] = q_in[4 * p + db]

    ups, downs, far = {}, {}, {}

    def spread(g):
        own_kv[g].wait()
        for db in range(1, 4):
            kv_copies[4 * g + db].wait_recv()
        rows = pl.ds(4 * g, 4)
        ups[g] = send(kvs.at[0, rows], kvs.at[1, rows], s_up.at[g], r_up.at[g], a_up)
        downs[g] = send(kvs.at[0, rows], kvs.at[2, rows], s_down.at[g], r_down.at[g], a_down)

    def near(slot, g):
        (ups if slot == 1 else downs)[g].wait_recv()
        if (g < 2) == (slot == 1):
            rows, to = pl.ds(4 * g, 4), a_up if slot == 1 else a_down
            far[g] = send(kvs.at[slot, rows], kvs.at[3, rows], s_far.at[g], r_far.at[g], to)

    def rows_of(slot, *groups):
        return [(slot, 4 * g + i) for g in groups for i in range(4)]

    weights_far, shared = [], []

    def forward_weights(part):
        for c in weights[part]:
            c.wait_recv()
        rows = pl.ds(64 * part, 64)
        to = y_down if part else y_up
        weights_far.append(
            send(w_s.at[1 + part, core, rows], w_s.at[3, core, rows], s_w.at[4 + part], r_w.at[4 + part], to)
        )

    def share_weights(k):
        shared.append(send(w_s.at[k, core], w_s.at[k, core], s_wc.at[k], r_wc.at[k], partner))

    def prepare(chunk):
        if chunk == 0:
            spread(0)
            place(0, 1024, rows_of(0, 0))
        elif chunk == 1:
            near(1, 0)
            spread(3)
            place(1, 0, rows_of(0, 1, 2) + rows_of(1, 0))
        elif chunk == 2:
            near(1, 1)
            near(2, 2)
            near(2, 0)
            place(2, 0, rows_of(2, 0) + rows_of(0, 3) + rows_of(1, 1))
            forward_weights(0)
        elif chunk == 3:
            near(2, 3)
            near(1, 2)
            near(2, 1)
            place(3, 0, rows_of(2, 1, 2) + rows_of(1, 2))
        elif chunk == 4:
            near(1, 3)
            far[0].wait_recv()
            far[1].wait_recv()
            place(4, 0, rows_of(3, 0, 1) + rows_of(1, 3))
            forward_weights(1)
            share_weights(1)
            share_weights(2)
        else:
            far[2].wait_recv()
            far[3].wait_recv()
            place(5, 0, rows_of(3, 2, 3) + rows_of(2, 3))

    def score(chunk, t, i):
        rows = slice(i * SUB, (i + 1) * SUB)
        s = dot(k_s[chunk % 2, rows], q_s[t])
        s_s[rows] = s
        return jnp.max(s.reshape(SUB // 8, 8, TILE), axis=0)

    def step(chunk, t, later_chunk, later):
        old = m_s[t]
        new = jnp.maximum(old, jnp.max(top_s[...], axis=0, keepdims=True))
        m_s[t] = new
        acc = acc_s[t] * jnp.exp2(old - new)
        top = None
        for i in range(STEPS):
            rows = slice(i * SUB, (i + 1) * SUB)
            p = jnp.exp2(s_s[rows] - new).astype(BF16)
            acc = acc + dot(v_s[chunk % 2, :, rows], p)
            if later is not None:
                part = score(later_chunk, later, i)
                top = part if top is None else jnp.maximum(top, part)
        acc_s[t] = acc
        if later is not None:
            top_s[...] = top

    att_copies = []

    def finish(t):
        acc = acc_s[t]
        o = (acc[:VALUE_DIM] / acc[VALUE_DIM : VALUE_DIM + 1]).astype(BF16)
        for i in range(4):
            att_s[4 * t + i] = o[:, 128 * i : 128 * i + 128]

    def give(p):
        for db in range(4):
            r = 4 * p + db
            if r:
                att_copies.append(
                    send(
                        att_s.at[r], slots.at[OPPOSITE[p], b], s_att.at[r], r_att.at[r],
                        at(0, (4 - db) % 4, PIECE[p]),
                    )
                )
            else:
                slots[0, b] = att_s[0]

    expand(0)
    def own_head(w_ref):
        w = w_ref[...].astype(F32)
        w = jnp.where(b < 2, w[:, :128], w[:, 128:])
        return jnp.where(lax.rem(b, 2) == 0, w, pltpu.roll(w, 64, 1)).astype(BF16)

    for c in rest:
        c.wait_recv()
    clat = clat_s[...].reshape(1024, 256)
    kn = dot(clat, own_head(kw_s))
    lane = lax.broadcasted_iota(jnp.int32, (1, 128), 1)
    ropes = []
    for i in range(8):
        two = jnp.concatenate([crope_s[2 * i], crope_s[2 * i + 1]], axis=1).astype(F32)
        two = jnp.concatenate([jnp.zeros((64, 128), F32), two, jnp.zeros((32, 128), F32)], axis=0)
        ropes.append(two.T)
    key = jnp.where(lane < NOPE_DIM, kn, jnp.concatenate(ropes, axis=0))
    inv = lax.rsqrt(jnp.sum(key * key, axis=1, keepdims=True) * (1.0 / QK_DIM) + EPS)
    gain = jnp.concatenate([kng_s[...], jnp.zeros((1, 32), F32)], axis=1)
    lift = jnp.full((1, 128), lift_ref[b] * LOG2E, F32)
    high = lift.astype(BF16).astype(F32)
    middle = (lift - high).astype(BF16).astype(F32)
    low = lift - high - middle
    extra = jnp.where(lane == 96, high, jnp.where(lane == 97, middle, jnp.where(lane == 98, low, 0.0)))
    k_s[0, 0:1024, :] = (key * inv * gain + extra).astype(BF16)
    vv = dot(clat, own_head(vw_s)).T
    v_s[0, 0:VALUE_DIM, 0:1024] = vv[:VALUE_DIM].astype(BF16)

    for c in latents[2][:2]:
        c.wait_recv()
    latents[3].append(send(kl_s.at[2], kl_s.at[3], s_kl.at[3], r_kl.at[3], y_down))
    latents[3].append(send(rk_s.at[2], rk_s.at[3], s_rk.at[3], r_rk.at[3], y_down))
    latents[1][2].wait_recv()
    latents[3].append(send(ql_s.at[1], ql_s.at[3], s_ql.at[3], r_ql.at[3], y_up))
    weights_near(0)
    weights_near(1)
    expand(1)
    expand(2)
    take_queries(0)
    prepare(0)
    top = None
    for i in range(STEPS):
        part = score(0, 0, i)
        top = part if top is None else jnp.maximum(top, part)
    top_s[...] = top
    take_queries(1)
    expand(3)
    step(0, 0, 0, 1)
    spread(1)
    spread(2)
    take_queries(2)
    step(0, 1, 0, 2)
    take_queries(3)
    step(0, 2, 0, 3)
    prepare(1)
    step(0, 3, 1, 0)
    for chunk in range(1, 6):
        if chunk < 5:

            def some_tile(t, carry, chunk=chunk):
                step(chunk, t, chunk, t + 1)
                return carry

            lax.fori_loop(0, 3, some_tile, 0)
            prepare(chunk + 1)
            step(chunk, 3, chunk + 1, 0)
        else:
            for t in range(4):
                step(chunk, t, chunk, t + 1 if t < 3 else None)
                finish(t)
                if t:
                    give(t - 1)
                if t == 1:
                    for c in weights_far:
                        c.wait_recv()
                    share_weights(3)
            give(3)

    for c in shared + att_copies:
        c.wait_recv()
    atts = [slots[k].reshape(256, 128).astype(F32).T.astype(BF16) for k in range(4)]
    gate = [mods_s[i, j : j + 1, :] for i in range(4) for j in range(8, 12)]
    for n in range(4):
        cols = slice(512 * n, 512 * n + 512)
        mixed = None
        for k in range(4):
            term = dot(atts[k], w_s[k, :, :, cols].reshape(256, 512)).astype(BF16).astype(F32)
            mixed = term if mixed is None else mixed + term
        gated = jnp.concatenate(gate[4 * n : 4 * n + 4], axis=1)
        out_ref[:, cols] = (x_s[:, cols].astype(F32) + gated * mixed).astype(BF16)
    sent = nears + wides + rest + list(q_copies.values()) + list(kv_copies.values())
    sent += list(ups.values()) + list(downs.values()) + list(far.values()) + weights[0] + weights[1] + weights_far + shared + att_copies
    for group in latents:
        sent += group
    for c in sent:
        c.wait_send()


def everything(*args):
    dma, vmem = pltpu.SemaphoreType.DMA, pltpu.VMEM
    hbm = pl.BlockSpec(memory_space=pltpu.HBM)
    return pl.pallas_call(
        kernel,
        out_shape=jax.ShapeDtypeStruct((128, 2048), BF16),
        in_specs=[hbm] * 20 + [pl.BlockSpec(memory_space=pltpu.SMEM)],
        out_specs=VMEM,
        scratch_shapes=[
            vmem((1, 128), BF16), vmem((3, 128, 512), BF16), vmem((1, 2048), F32), vmem((1, 512), F32),
            vmem((1, 256), F32), vmem((1, 96), F32), vmem((1, 96), F32), vmem((8, 128), F32),
            vmem((128, 2048), BF16), vmem((2048, 512), BF16), vmem((2048, 256), BF16), vmem((32, 2048), BF16),
            vmem((512, 384), BF16), vmem((256, 256), BF16), vmem((256, 256), BF16),
            vmem((16, 64, 256), BF16), vmem((16, 32, 64), BF16),
            vmem((16, 128), F32), vmem((16, 16, 128), F32), vmem((4, 16, 128), F32),
            vmem((4, 128, 512), BF16), vmem((4, 128, 256), BF16), vmem((4, 32, 128), BF16),
            vmem((4, 4, 256, 128), BF16), vmem((16, QK_DIM, 128), BF16), vmem((4, 16, 160, 128), BF16),
            vmem((4, 128, TILE), BF16), vmem((2, CHUNK, 128), BF16), vmem((2, 80, CHUNK), BF16),
            vmem((CHUNK, TILE), F32), vmem((4, 1, TILE), F32), vmem((8, TILE), F32), vmem((4, 80, TILE), F32),
            vmem((16, VALUE_DIM, 128), BF16), vmem((4, 4, VALUE_DIM, 128), BF16), vmem((4, 2, 128, 2048), BF16),
            dma((4,)), dma((4,)), dma((16,)), dma((16,)), dma((16,)), dma((16,)), dma((16,)), dma((16,)),
            dma((4,)), dma((4,)), dma((4,)), dma((4,)), dma((4,)), dma((4,)),
            dma((16,)), dma((16,)), dma((16,)), dma((16,)),
            dma((4,)), dma((4,)), dma((4,)), dma((4,)), dma((4,)), dma((4,)), dma((16,)), dma((16,)),
            dma((6,)), dma((6,)), dma((4,)), dma((4,)), dma((21,)), dma((4,)),
        ],
        compiler_params=pltpu.CompilerParams(
            collective_id=0, has_side_effects=True, vmem_limit_bytes=67_043_328
        ),
        cost_estimate=pl.CostEstimate(
            flops=10_000_000_000, bytes_accessed=8_000_000, transcendentals=19_000_000
        ),
        name="everything",
    )(*args)


def local(
    latent_tokens, condition, shift_weight, scale_weight, gate_weight, norm_gain, query_down, query_gain,
    kv_down, kv_gain, rope_down, query_up, key_up, value_up, query_norm_gain, key_norm_gain, out_weight,
    context_latent, context_rope, context_lift,
):
    frequency = THETA ** (-4.0 * jnp.arange(8, dtype=F32) / ROPE_DIM)
    return everything(
        condition.reshape(1, 128), shift_weight, scale_weight, gate_weight,
        norm_gain.reshape(1, -1), query_gain.reshape(1, -1), kv_gain.reshape(1, -1),
        query_norm_gain.reshape(1, -1), key_norm_gain.reshape(1, -1),
        jnp.broadcast_to(frequency[:, None], (8, 128)),
        latent_tokens, query_down, kv_down, rope_down.T, query_up, key_up, value_up,
        context_latent, context_rope.T, out_weight, context_lift,
    )


def solution(mesh):
    in_specs = (
        P(("dp", "sp", "tp"), None), P(("dp", "sp")), P("sp", "tp"), P("sp", "tp"), P("sp", "tp"),
        P(), P(), P(), P(), P(), P(), P(None, "tp"), P(None, "tp"), P(None, "tp"), P(), P(),
        P("tp", None), P(("dp", "sp"), None), P(("dp", "sp"), None), P("tp"),
    )
    return jax.shard_map(
        local, mesh=mesh, in_specs=in_specs, out_specs=P(("dp", "sp", "tp"), None), check_vma=False
    )
```

```python
import jax
import jax.numpy as jnp
from jax import lax
from jax.experimental import pallas as pl
from jax.experimental.pallas import tpu as pltpu
from jax.sharding import PartitionSpec as P

NOPE_DIM = 64
ROPE_DIM = 32
VALUE_DIM = 64
QK_DIM = 96
GRID_W = 64
EPS = 1e-06
THETA = 10000.0
LOG2E = 1.4426950408889634

F32 = jnp.float32
BF16 = jnp.bfloat16
MESH = pl.DeviceIdType.MESH
VMEM = pl.BlockSpec(memory_space=pltpu.VMEM)


CHUNK = 1536
TILE = 512
SUB = 256
STEPS = CHUNK // SUB
PIECE = (0, 3, 1, 2)
OPPOSITE = (0, 2, 1, 3)


def send(src, dst, send_sem, recv_sem, to):
    c = pltpu.make_async_remote_copy(
        src_ref=src, dst_ref=dst, send_sem=send_sem, recv_sem=recv_sem, device_id=to, device_id_type=MESH
    )
    c.start()
    return c


def dot(a, b):
    return jnp.dot(a, b, preferred_element_type=F32)


def turned(rows, cosine, sine):
    out = []
    for a in range(2):
        u, w = rows[16 * a : 16 * a + 8], rows[16 * a + 8 : 16 * a + 16]
        out += [u * cosine[a] - w * sine[a], w * cosine[a] + u * sine[a]]
    return jnp.concatenate(out, axis=0)


def column(row):
    row = jnp.concatenate([row, jnp.zeros((1, 32), F32)], axis=1)
    return jnp.broadcast_to(row, (128, 128)).T[:QK_DIM]


def kernel(
    cond_hbm, shift_hbm, scale_hbm, gate_hbm, ng_hbm, qgain_hbm, kvgain_hbm, qng_hbm, kng_hbm,
    x_hbm, qd_hbm, kvd_hbm, rd_hbm, qw_hbm, kw_hbm, vw_hbm, lat_hbm, rope_hbm, wout_hbm, lift_ref,
    out_ref,
    cond_s, mw_s, ng_s, qgain_s, kvgain_s, qng_s, kng_s,
    x_s, qd_s, kvd_s, rd_s, qw_s, kw_s, vw_s, clat_s, crope_s,
    part_s, wide_s, mods_s, ql_s, kl_s, rk_s,
    qkv_s, q_in, kvs, q_s, k_s, v_s, s_s, m_s, top_s, acc_s, att_s, slots, w_s, mixed_s,
    s_near, r_near, s_wide, r_wide, s_lat, r_lat, s_rope, r_rope,
    s_ql, r_ql, s_kl, r_kl, s_rk, r_rk, s_q, r_q, s_kv, r_kv,
    s_up, r_up, s_down, r_down, s_far, r_far, s_att, r_att, s_w, r_w, s_wc, r_wc, local_sem, block_sem,
):
    sp, tp, core = lax.axis_index("sp"), lax.axis_index("tp"), lax.axis_index("dp")
    z, x = sp // 4, lax.rem(sp, 4)
    a, b = z + core * (x - z), x + core * (z - x)

    def at(da, db, dy):
        aa, bb = lax.rem(a + da, 4), lax.rem(b + db, 4)
        return {"sp": aa * (4 - 3 * core) + bb * (1 + 3 * core), "tp": lax.rem(tp + dy, 4)}

    def along_tp(k):
        return {"tp": lax.rem(tp + k, 4)}

    def along_sp(r):
        return {"sp": lax.rem(sp + r, 16)}

    partner, y_up, y_down = {"dp": 1 - core}, along_tp(1), along_tp(3)
    a_up, a_down = at(1, 0, 0), at(3, 0, 0)
    barrier = pltpu.get_barrier_semaphore()
    greeted = [along_tp(k) for k in range(1, 4)] + [along_sp(r) for r in range(1, 16)] + [partner]
    greeted += [at(0, db, dy) for dy in range(1, 4) for db in range(1, 4)]
    for to in greeted:
        pl.semaphore_signal(barrier, inc=1, device_id=to, device_id_type=MESH)
    own = []

    def fetch(src, dst):
        c = pltpu.make_async_copy(src, dst, local_sem.at[len(own)])
        c.start()
        own.append(c)

    for src, dst in (
        (cond_hbm, cond_s), (shift_hbm, mw_s.at[0]), (scale_hbm, mw_s.at[1]), (gate_hbm, mw_s.at[2]),
        (qng_hbm, qng_s), (kng_hbm, kng_s), (x_hbm, x_s), (ng_hbm, ng_s),
        (qd_hbm, qd_s), (kvd_hbm, kvd_s), (rd_hbm, rd_s), (qgain_hbm, qgain_s), (kvgain_hbm, kvgain_s),
        (qw_hbm, qw_s), (kw_hbm, kw_s), (vw_hbm, vw_s), (lat_hbm, clat_s.at[0]), (rope_hbm, crope_s.at[0]),
        (wout_hbm.at[0:128], w_s.at[0, 0]), (wout_hbm.at[128:256], w_s.at[0, 1]),
    ):
        fetch(src, dst)

    for c in own[:4]:
        c.wait()
    cond = cond_s[...].astype(F32)
    active = cond / (1.0 + jnp.exp(-cond))
    active = jnp.broadcast_to(active, (16, 128)).astype(BF16)
    for i in range(3):
        row = dot(active, mw_s[i])
        for j in range(4):
            piece = row[0:1, 128 * j : 128 * j + 128]
            part_s[4 * i + j : 4 * i + j + 1, :] = piece
    part_s[12:16, :] = jnp.zeros((4, 128), F32)
    pl.semaphore_wait(barrier, len(greeted))

    weights = [[], []]

    def weights_near(part):
        rows, src = pl.ds(64 * part, 64), wout_hbm.at[pl.ds(core * 128 + 64 * part, 64)]
        i = 2 * part
        weights[part].append(send(src, w_s.at[1, core, rows], s_w.at[i], r_w.at[i], y_up))
        weights[part].append(send(src, w_s.at[2, core, rows], s_w.at[i + 1], r_w.at[i + 1], y_down))

    weights_far, shared = [], {}

    def forward_weights(part):
        for c in weights[part]:
            c.wait_recv()
        rows = pl.ds(64 * part, 64)
        to = y_down if part else y_up
        weights_far.append(
            send(w_s.at[1 + part, core, rows], w_s.at[3, core, rows], s_w.at[4 + part], r_w.at[4 + part], to)
        )

    weights_near(0)
    wides, nears, rest = [], [], []
    for r in range(1, 16):
        wides.append(send(part_s, wide_s.at[r], s_wide.at[r], r_wide.at[r], along_sp(r)))
    for r in range(1, 16):
        rest.append(send(lat_hbm, clat_s.at[r], s_lat.at[r], r_lat.at[r], along_sp(r)))
        rest.append(send(rope_hbm, crope_s.at[r], s_rope.at[r], r_rope.at[r], along_sp(r)))
    total = part_s[...]
    for r in range(1, 16):
        wides[r - 1].wait_recv()
        total = total + wide_s[r]
    mods_s[tp] = total
    for k in range(1, 4):
        nears.append(send(mods_s.at[tp], mods_s.at[tp], s_near.at[k], r_near.at[k], along_tp(k)))

    for c in own[4:]:
        c.wait()
    lane = lax.broadcasted_iota(jnp.int32, (8, 128), 1)
    which = lax.broadcasted_iota(jnp.int32, (8, 128), 0)
    frequency = jnp.full((8, 128), 1.0, F32)
    for f in range(1, 8):
        frequency = jnp.where(which == f, THETA ** (-4.0 * f / ROPE_DIM), frequency)
    column_angle = lax.rem(lane, GRID_W).astype(F32) * frequency
    column_cosine, column_sine = jnp.cos(column_angle), jnp.sin(column_angle)
    tables = []
    for p in range(4):
        row = (sp * 4 + lax.rem(tp + PIECE[p], 4)) * 2 + lane // GRID_W
        angle = row.astype(F32) * frequency
        tables.append(((jnp.cos(angle), column_cosine), (jnp.sin(angle), column_sine)))
    q_gain = column(qng_s[...] * (LOG2E * QK_DIM**-0.5))
    k_gain = column(kng_s[...])
    for i in range(3):
        v_s[i, VALUE_DIM:80, :] = jnp.ones((16, CHUNK), BF16)
    for t in range(4):
        q_s[t, QK_DIM:128, :] = jnp.ones((32, TILE), BF16)
    m_s[...] = jnp.full(m_s.shape, -1e30, F32)
    acc_s[...] = jnp.zeros(acc_s.shape, F32)
    values = x_s[...].astype(F32)
    mean_square = jnp.mean(values * values, axis=-1, keepdims=True)
    scaled = values * lax.rsqrt(mean_square + EPS) * ng_s[...]

    for c in nears:
        c.wait_recv()
    shift, scale = [
        jnp.concatenate([mods_s[i, j : j + 1, :] for i in range(4) for j in range(4 * k, 4 * k + 4)], axis=1)
        for k in range(2)
    ]
    normed = (scaled * (1.0 + scale) + shift).astype(BF16)

    def latent(w, gain_ref):
        y = dot(normed, w[...])
        m = jnp.mean(y * y, axis=-1, keepdims=True)
        return (y * lax.rsqrt(m + EPS) * gain_ref[...]).astype(BF16)

    rk = lax.dot_general(rd_s[...], normed, (((1,), (1,)), ((), ())), preferred_element_type=F32)
    rk_s[0] = rk.astype(BF16)
    kl_s[0] = latent(kvd_s, kvgain_s)
    ql_s[0] = latent(qd_s, qgain_s)
    latents = [[], [], [], []]
    for p, to in ((1, y_up), (2, y_down)):
        latents[p].append(send(kl_s.at[0], kl_s.at[p], s_kl.at[p], r_kl.at[p], to))
        latents[p].append(send(rk_s.at[0], rk_s.at[p], s_rk.at[p], r_rk.at[p], to))
        latents[p].append(send(ql_s.at[0], ql_s.at[p], s_ql.at[p], r_ql.at[p], to))

    q_copies, kv_copies, own_kv = {}, {}, []

    def expand(p):
        for c in latents[p][2:] if p == 2 else latents[p][:2] if p == 1 else latents[p]:
            c.wait_recv()
        cosine, sine = tables[p]
        rk = rk_s[p].astype(F32)
        rk_square = jnp.sum(rk * rk, axis=0, keepdims=True)
        q, kn, vv = dot(ql_s[p], qw_s[...]).T, dot(kl_s[p], kw_s[...]).T, dot(kl_s[p], vw_s[...]).T
        for j in range(4):
            qh = q[QK_DIM * j : QK_DIM * (j + 1)]
            inv = lax.rsqrt(jnp.sum(qh * qh, axis=0, keepdims=True) * (1.0 / QK_DIM) + EPS)
            qh = qh * inv * q_gain
            qh = jnp.concatenate([qh[:NOPE_DIM], turned(qh[NOPE_DIM:], cosine, sine)], axis=0)
            qkv_s[p, j, 0:QK_DIM, :] = qh.astype(BF16)
            kh = kn[NOPE_DIM * j : NOPE_DIM * (j + 1)]
            square = jnp.sum(kh * kh, axis=0, keepdims=True) + rk_square
            inv = lax.rsqrt(square * (1.0 / QK_DIM) + EPS)
            kr = turned(rk * inv * k_gain[NOPE_DIM:], cosine, sine)
            kh = kh * inv * k_gain[:NOPE_DIM]
            qkv_s[p, j, QK_DIM : QK_DIM + NOPE_DIM, :] = kh.astype(BF16)
            qkv_s[p, j, QK_DIM + NOPE_DIM : 2 * QK_DIM, :] = kr.astype(BF16)
            qkv_s[p, j, 2 * QK_DIM : 256, :] = vv[VALUE_DIM * j : VALUE_DIM * (j + 1)].astype(BF16)
        c = pltpu.make_async_copy(qkv_s.at[p, b, QK_DIM:256], kvs.at[0, 4 * p], block_sem.at[p])
        c.start()
        own_kv.append(c)
        for db in range(1, 4):
            r, block = 4 * p + db, qkv_s.at[p, lax.rem(b + db, 4)]
            q_copies[r] = send(block.at[0:QK_DIM], q_in.at[r], s_q.at[r], r_q.at[r], at(0, db, 0))
        for db in range(1, 4):
            r, block = 4 * p + db, qkv_s.at[p, lax.rem(b + db, 4)]
            kv_copies[r] = send(block.at[QK_DIM:256], kvs.at[0, r], s_kv.at[r], r_kv.at[r], at(0, db, 0))

    def place(chunk, first, blocks):
        for i, (slot, r) in enumerate(blocks):
            at_key = first + 128 * i
            block = kvs[slot, r]
            kt = jnp.concatenate([block[:QK_DIM].astype(F32), jnp.zeros((32, 128), F32)], axis=0)
            k_s[chunk % 3, at_key : at_key + 128, :] = kt.T.astype(BF16)
            v_s[chunk % 3, 0:VALUE_DIM, at_key : at_key + 128] = block[QK_DIM:]

    def take_queries(p):
        q_s[p, 0:QK_DIM, 0:128] = qkv_s[p, b, 0:QK_DIM]
        for db in range(1, 4):
            q_copies[4 * p + db].wait_recv()
            q_s[p, 0:QK_DIM, 128 * db : 128 * db + 128] = q_in[4 * p + db]

    ups, downs, far = {}, {}, {}

    def spread(g):
        own_kv[g].wait()
        for db in range(1, 4):
            kv_copies[4 * g + db].wait_recv()
        rows = pl.ds(4 * g, 4)
        ups[g] = send(kvs.at[0, rows], kvs.at[1, rows], s_up.at[g], r_up.at[g], a_up)
        downs[g] = send(kvs.at[0, rows], kvs.at[2, rows], s_down.at[g], r_down.at[g], a_down)

    def near(slot, g):
        (ups if slot == 1 else downs)[g].wait_recv()
        if (g < 2) == (slot == 1):
            rows, to = pl.ds(4 * g, 4), a_up if slot == 1 else a_down
            far[g] = send(kvs.at[slot, rows], kvs.at[3, rows], s_far.at[g], r_far.at[g], to)

    def rows_of(slot, *groups):
        return [(slot, 4 * g + i) for g in groups for i in range(4)]

    def share_weights(k):
        shared[k] = send(w_s.at[k, core], w_s.at[k, core], s_wc.at[k], r_wc.at[k], partner)

    def prepare(chunk):
        if chunk == 0:
            spread(0)
            place(0, 1024, rows_of(0, 0))
        elif chunk == 1:
            near(1, 0)
            place(1, 0, rows_of(0, 1, 2) + rows_of(1, 0))
        elif chunk == 2:
            near(1, 1)
            near(2, 2)
            near(2, 0)
            place(2, 0, rows_of(2, 0) + rows_of(0, 3) + rows_of(1, 1))
        elif chunk == 3:
            near(2, 3)
            near(1, 2)
            near(2, 1)
            place(3, 0, rows_of(2, 1, 2) + rows_of(1, 2))
            forward_weights(1)
            share_weights(1)
            share_weights(2)
        elif chunk == 4:
            near(1, 3)
            far[0].wait_recv()
            far[1].wait_recv()
            place(4, 0, rows_of(3, 0, 1) + rows_of(1, 3))
        else:
            far[2].wait_recv()
            far[3].wait_recv()
            place(5, 0, rows_of(3, 2, 3) + rows_of(2, 3))
            for c in weights_far:
                c.wait_recv()
            share_weights(3)

    def score(chunk, t, i):
        rows = slice(i * SUB, (i + 1) * SUB)
        s = dot(k_s[chunk % 3, rows], q_s[t])
        s_s[rows] = s
        return jnp.max(s.reshape(SUB // 8, 8, TILE), axis=0)

    def step(chunk, t, later_chunk, later):
        old = m_s[t]
        new = jnp.maximum(old, jnp.max(top_s[...], axis=0, keepdims=True))
        m_s[t] = new
        acc = acc_s[t] * jnp.exp2(old - new)
        top = None
        for i in range(STEPS):
            rows = slice(i * SUB, (i + 1) * SUB)
            p = jnp.exp2(s_s[rows] - new).astype(BF16)
            acc = acc + dot(v_s[chunk % 3, :, rows], p)
            if later is not None:
                part = score(later_chunk, later, i)
                top = part if top is None else jnp.maximum(top, part)
        acc_s[t] = acc
        if later is not None:
            top_s[...] = top

    att_copies = {}

    def finish(t):
        acc = acc_s[t]
        o = (acc[:VALUE_DIM] / acc[VALUE_DIM : VALUE_DIM + 1]).astype(BF16)
        for i in range(4):
            att_s[4 * t + i] = o[:, 128 * i : 128 * i + 128]

    def give(p):
        for db in range(4):
            r = 4 * p + db
            if r:
                att_copies[r] = send(
                    att_s.at[r], slots.at[OPPOSITE[p], b], s_att.at[r], r_att.at[r],
                    at(0, (4 - db) % 4, PIECE[p]),
                )
            else:
                slots[0, b] = att_s[0]

    expand(0)
    def own_head(w_ref):
        w = w_ref[...].astype(F32)
        w = jnp.where(b < 2, w[:, :128], w[:, 128:])
        return jnp.where(lax.rem(b, 2) == 0, w, pltpu.roll(w, 64, 1)).astype(BF16)

    for c in rest:
        c.wait_recv()
    clat = clat_s[...].reshape(1024, 256)
    kn = dot(clat, own_head(kw_s))
    lane = lax.broadcasted_iota(jnp.int32, (1, 128), 1)
    ropes = []
    for i in range(8):
        two = jnp.concatenate([crope_s[2 * i], crope_s[2 * i + 1]], axis=1).astype(F32)
        two = jnp.concatenate([jnp.zeros((64, 128), F32), two, jnp.zeros((32, 128), F32)], axis=0)
        ropes.append(two.T)
    key = jnp.where(lane < NOPE_DIM, kn, jnp.concatenate(ropes, axis=0))
    inv = lax.rsqrt(jnp.sum(key * key, axis=1, keepdims=True) * (1.0 / QK_DIM) + EPS)
    gain = jnp.concatenate([kng_s[...], jnp.zeros((1, 32), F32)], axis=1)
    lift = jnp.full((1, 128), lift_ref[b] * LOG2E, F32)
    high = lift.astype(BF16).astype(F32)
    middle = (lift - high).astype(BF16).astype(F32)
    low = lift - high - middle
    extra = jnp.where(lane == 96, high, jnp.where(lane == 97, middle, jnp.where(lane == 98, low, 0.0)))
    k_s[0, 0:1024, :] = (key * inv * gain + extra).astype(BF16)
    vv = dot(clat, own_head(vw_s)).T
    v_s[0, 0:VALUE_DIM, 0:1024] = vv[:VALUE_DIM].astype(BF16)

    for c in latents[2][:2]:
        c.wait_recv()
    latents[3].append(send(kl_s.at[2], kl_s.at[3], s_kl.at[3], r_kl.at[3], y_down))
    latents[3].append(send(rk_s.at[2], rk_s.at[3], s_rk.at[3], r_rk.at[3], y_down))
    latents[1][2].wait_recv()
    latents[3].append(send(ql_s.at[1], ql_s.at[3], s_ql.at[3], r_ql.at[3], y_up))
    weights_near(1)
    forward_weights(0)
    expand(1)
    expand(2)
    take_queries(0)
    prepare(0)
    top = None
    for i in range(STEPS):
        part = score(0, 0, i)
        top = part if top is None else jnp.maximum(top, part)
    top_s[...] = top
    take_queries(1)
    expand(3)
    step(0, 0, 0, 1)
    spread(1)
    spread(2)
    take_queries(2)
    step(0, 1, 0, 2)
    prepare(1)
    step(0, 2, 1, 0)
    step(1, 0, 1, 1)
    step(1, 1, 1, 2)
    take_queries(3)
    spread(3)
    step(1, 2, 0, 3)
    step(0, 3, 1, 3)
    prepare(2)
    step(1, 3, 2, 0)
    for chunk in range(2, 6):
        if chunk < 5:

            def some_tile(t, carry, chunk=chunk):
                step(chunk, t, chunk, t + 1)
                return carry

            lax.fori_loop(0, 3, some_tile, 0)
            prepare(chunk + 1)
            step(chunk, 3, chunk + 1, 0)
        else:
            for t in range(4):
                step(chunk, t, chunk, t + 1 if t < 3 else None)
                finish(t)
                if t:
                    give(t - 1)
            give(3)

    gate = [mods_s[i, j : j + 1, :] for i in range(4) for j in range(8, 12)]
    for p in range(4):
        k = OPPOSITE[p]
        for r in range(max(1, 4 * p), 4 * p + 4):
            att_copies[r].wait_recv()
        if p:
            shared[k].wait_recv()
        att = slots[k].reshape(256, 128).astype(F32).T.astype(BF16)
        for n in range(4):
            cols = slice(512 * n, 512 * n + 512)
            term = dot(att, w_s[k, :, :, cols].reshape(256, 512)).astype(BF16).astype(F32)
            if p:
                term = mixed_s[:, cols] + term
            if p < 3:
                mixed_s[:, cols] = term
            else:
                gated = jnp.concatenate(gate[4 * n : 4 * n + 4], axis=1)
                out_ref[:, cols] = (x_s[:, cols].astype(F32) + gated * term).astype(BF16)
    sent = nears + wides + rest + list(q_copies.values()) + list(kv_copies.values())
    sent += list(ups.values()) + list(downs.values()) + list(far.values()) + weights[0] + weights[1] + weights_far + list(shared.values()) + list(att_copies.values())
    for group in latents:
        sent += group
    for c in sent:
        c.wait_send()


def everything(*args):
    dma, vmem = pltpu.SemaphoreType.DMA, pltpu.VMEM
    hbm = pl.BlockSpec(memory_space=pltpu.HBM)
    return pl.pallas_call(
        kernel,
        out_shape=jax.ShapeDtypeStruct((128, 2048), BF16),
        in_specs=[hbm] * 19 + [pl.BlockSpec(memory_space=pltpu.SMEM)],
        out_specs=VMEM,
        scratch_shapes=[
            vmem((1, 128), BF16), vmem((3, 128, 512), BF16), vmem((1, 2048), F32), vmem((1, 512), F32),
            vmem((1, 256), F32), vmem((1, 96), F32), vmem((1, 96), F32),
            vmem((128, 2048), BF16), vmem((2048, 512), BF16), vmem((2048, 256), BF16), vmem((32, 2048), BF16),
            vmem((512, 384), BF16), vmem((256, 256), BF16), vmem((256, 256), BF16),
            vmem((16, 64, 256), BF16), vmem((16, 32, 64), BF16),
            vmem((16, 128), F32), vmem((16, 16, 128), F32), vmem((4, 16, 128), F32),
            vmem((4, 128, 512), BF16), vmem((4, 128, 256), BF16), vmem((4, 32, 128), BF16),
            vmem((4, 4, 256, 128), BF16), vmem((16, QK_DIM, 128), BF16), vmem((4, 16, 160, 128), BF16),
            vmem((4, 128, TILE), BF16), vmem((3, CHUNK, 128), BF16), vmem((3, 80, CHUNK), BF16),
            vmem((CHUNK, TILE), F32), vmem((4, 1, TILE), F32), vmem((8, TILE), F32), vmem((4, 80, TILE), F32),
            vmem((16, VALUE_DIM, 128), BF16), vmem((4, 4, VALUE_DIM, 128), BF16), vmem((4, 2, 128, 2048), BF16),
            vmem((128, 2048), F32),
            dma((4,)), dma((4,)), dma((16,)), dma((16,)), dma((16,)), dma((16,)), dma((16,)), dma((16,)),
            dma((4,)), dma((4,)), dma((4,)), dma((4,)), dma((4,)), dma((4,)),
            dma((16,)), dma((16,)), dma((16,)), dma((16,)),
            dma((4,)), dma((4,)), dma((4,)), dma((4,)), dma((4,)), dma((4,)), dma((16,)), dma((16,)),
            dma((6,)), dma((6,)), dma((4,)), dma((4,)), dma((21,)), dma((4,)),
        ],
        compiler_params=pltpu.CompilerParams(
            collective_id=0, has_side_effects=True, vmem_limit_bytes=67_043_328
        ),
        cost_estimate=pl.CostEstimate(
            flops=10_000_000_000, bytes_accessed=8_000_000, transcendentals=19_000_000
        ),
        name="everything",
    )(*args)


def local(
    latent_tokens, condition, shift_weight, scale_weight, gate_weight, norm_gain, query_down, query_gain,
    kv_down, kv_gain, rope_down, query_up, key_up, value_up, query_norm_gain, key_norm_gain, out_weight,
    context_latent, context_rope, context_lift,
):
    return everything(
        condition.reshape(1, 128), shift_weight, scale_weight, gate_weight,
        norm_gain.reshape(1, -1), query_gain.reshape(1, -1), kv_gain.reshape(1, -1),
        query_norm_gain.reshape(1, -1), key_norm_gain.reshape(1, -1),
        latent_tokens, query_down, kv_down, rope_down.T, query_up, key_up, value_up,
        context_latent, context_rope.T, out_weight, context_lift,
    )


def solution(mesh):
    in_specs = (
        P(("dp", "sp", "tp"), None), P(("dp", "sp")), P("sp", "tp"), P("sp", "tp"), P("sp", "tp"),
        P(), P(), P(), P(), P(), P(), P(None, "tp"), P(None, "tp"), P(None, "tp"), P(), P(),
        P("tp", None), P(("dp", "sp"), None), P(("dp", "sp"), None), P("tp"),
    )
    return jax.shard_map(
        local, mesh=mesh, in_specs=in_specs, out_specs=P(("dp", "sp", "tp"), None), check_vma=False
    )
```

```python
import jax
import jax.numpy as jnp
from jax import lax
from jax.experimental import pallas as pl
from jax.experimental.pallas import tpu as pltpu
from jax.sharding import PartitionSpec as P

NOPE_DIM = 64
ROPE_DIM = 32
VALUE_DIM = 64
QK_DIM = 96
GRID_W = 64
EPS = 1e-06
THETA = 10000.0
LOG2E = 1.4426950408889634

F32 = jnp.float32
BF16 = jnp.bfloat16
MESH = pl.DeviceIdType.MESH
VMEM = pl.BlockSpec(memory_space=pltpu.VMEM)


CHUNK = 1536
TILE = 512
SUB = 256
STEPS = CHUNK // SUB
PIECE = (0, 3, 1, 2)
OPPOSITE = (0, 2, 1, 3)


def send(src, dst, send_sem, recv_sem, to):
    c = pltpu.make_async_remote_copy(
        src_ref=src, dst_ref=dst, send_sem=send_sem, recv_sem=recv_sem, device_id=to, device_id_type=MESH
    )
    c.start()
    return c


def dot(a, b):
    return jnp.dot(a, b, preferred_element_type=F32)


def turned(rows, cosine, sine):
    out = []
    for a in range(2):
        u, w = rows[16 * a : 16 * a + 8], rows[16 * a + 8 : 16 * a + 16]
        out += [u * cosine[a] - w * sine[a], w * cosine[a] + u * sine[a]]
    return jnp.concatenate(out, axis=0)


def column(row):
    row = jnp.concatenate([row, jnp.zeros((1, 32), F32)], axis=1)
    return jnp.broadcast_to(row, (128, 128)).T[:QK_DIM]


def kernel(
    cond_hbm, shift_hbm, scale_hbm, gate_hbm, ng_hbm, qgain_hbm, kvgain_hbm, qng_hbm, kng_hbm,
    x_hbm, qd_hbm, kvd_hbm, rd_hbm, qw_hbm, kw_hbm, vw_hbm, lat_hbm, rope_hbm, wout_hbm, lift_ref,
    out_ref,
    cond_s, mw_s, ng_s, qgain_s, kvgain_s, qng_s, kng_s,
    x_s, qd_s, kvd_s, rd_s, qw_s, kw_s, vw_s, clat_s, crope_s,
    part_s, wide_s, mods_s, ql_s, kl_s, rk_s,
    qkv_s, q_in, kvs, q_s, k_s, v_s, s_s, m_s, top_s, acc_s, att_s, slots, w_s, mixed_s,
    s_near, r_near, s_wide, r_wide, s_lat, r_lat, s_rope, r_rope,
    s_ql, r_ql, s_kl, r_kl, s_rk, r_rk, s_q, r_q, s_kv, r_kv,
    s_up, r_up, s_down, r_down, s_far, r_far, s_att, r_att, s_w, r_w, s_wc, r_wc, local_sem, block_sem,
):
    sp, tp, core = lax.axis_index("sp"), lax.axis_index("tp"), lax.axis_index("dp")
    z, x = sp // 4, lax.rem(sp, 4)
    a, b = z + core * (x - z), x + core * (z - x)

    def at(da, db, dy):
        aa, bb = lax.rem(a + da, 4), lax.rem(b + db, 4)
        return {"sp": aa * (4 - 3 * core) + bb * (1 + 3 * core), "tp": lax.rem(tp + dy, 4)}

    def along_tp(k):
        return {"tp": lax.rem(tp + k, 4)}

    def along_sp(r):
        return {"sp": lax.rem(sp + r, 16)}

    partner, y_up, y_down = {"dp": 1 - core}, along_tp(1), along_tp(3)
    a_up, a_down = at(1, 0, 0), at(3, 0, 0)
    barrier = pltpu.get_barrier_semaphore()
    greeted = [along_tp(k) for k in range(1, 4)] + [along_sp(r) for r in range(1, 16)] + [partner]
    greeted += [at(0, db, dy) for dy in range(1, 4) for db in range(1, 4)]
    for to in greeted:
        pl.semaphore_signal(barrier, inc=1, device_id=to, device_id_type=MESH)
    own = []

    def fetch(src, dst):
        c = pltpu.make_async_copy(src, dst, local_sem.at[len(own)])
        c.start()
        own.append(c)

    for src, dst in (
        (cond_hbm, cond_s), (shift_hbm, mw_s.at[0]), (scale_hbm, mw_s.at[1]), (gate_hbm, mw_s.at[2]),
        (qng_hbm, qng_s), (kng_hbm, kng_s), (x_hbm, x_s), (ng_hbm, ng_s),
        (qd_hbm, qd_s), (kvd_hbm, kvd_s), (rd_hbm, rd_s), (qgain_hbm, qgain_s), (kvgain_hbm, kvgain_s),
        (qw_hbm, qw_s), (kw_hbm, kw_s), (vw_hbm, vw_s), (lat_hbm, clat_s.at[0]), (rope_hbm, crope_s.at[0]),
        (wout_hbm.at[0:128], w_s.at[0, 0]), (wout_hbm.at[128:256], w_s.at[0, 1]),
    ):
        fetch(src, dst)

    for c in own[:4]:
        c.wait()
    cond = cond_s[...].astype(F32)
    active = cond / (1.0 + jnp.exp(-cond))
    active = jnp.broadcast_to(active, (16, 128)).astype(BF16)
    for i in range(3):
        row = dot(active, mw_s[i])
        for j in range(4):
            piece = row[0:1, 128 * j : 128 * j + 128]
            part_s[4 * i + j : 4 * i + j + 1, :] = piece
    part_s[12:16, :] = jnp.zeros((4, 128), F32)
    pl.semaphore_wait(barrier, len(greeted))

    weights = [[], []]

    def weights_near(part):
        rows, src = pl.ds(64 * part, 64), wout_hbm.at[pl.ds(core * 128 + 64 * part, 64)]
        i = 2 * part
        weights[part].append(send(src, w_s.at[1, core, rows], s_w.at[i], r_w.at[i], y_up))
        weights[part].append(send(src, w_s.at[2, core, rows], s_w.at[i + 1], r_w.at[i + 1], y_down))

    weights_far, shared = [], {}

    def forward_weights(part):
        for c in weights[part]:
            c.wait_recv()
        rows = pl.ds(64 * part, 64)
        to = y_down if part else y_up
        weights_far.append(
            send(w_s.at[1 + part, core, rows], w_s.at[3, core, rows], s_w.at[4 + part], r_w.at[4 + part], to)
        )

    weights_near(0)
    wides, nears, rest = [], [], []
    for r in range(1, 16):
        wides.append(send(part_s, wide_s.at[r], s_wide.at[r], r_wide.at[r], along_sp(r)))
    total = part_s[...]
    for r in range(1, 16):
        wides[r - 1].wait_recv()
        total = total + wide_s[r]
    mods_s[tp] = total
    for k in range(1, 4):
        nears.append(send(mods_s.at[tp], mods_s.at[tp], s_near.at[k], r_near.at[k], along_tp(k)))
    for r in range(1, 16):
        rest.append(send(lat_hbm, clat_s.at[r], s_lat.at[r], r_lat.at[r], along_sp(r)))
        rest.append(send(rope_hbm, crope_s.at[r], s_rope.at[r], r_rope.at[r], along_sp(r)))

    for c in own[4:]:
        c.wait()
    lane = lax.broadcasted_iota(jnp.int32, (8, 128), 1)
    which = lax.broadcasted_iota(jnp.int32, (8, 128), 0)
    frequency = jnp.full((8, 128), 1.0, F32)
    for f in range(1, 8):
        frequency = jnp.where(which == f, THETA ** (-4.0 * f / ROPE_DIM), frequency)
    column_angle = lax.rem(lane, GRID_W).astype(F32) * frequency
    column_cosine, column_sine = jnp.cos(column_angle), jnp.sin(column_angle)
    tables = []
    for p in range(4):
        row = (sp * 4 + lax.rem(tp + PIECE[p], 4)) * 2 + lane // GRID_W
        angle = row.astype(F32) * frequency
        tables.append(((jnp.cos(angle), column_cosine), (jnp.sin(angle), column_sine)))
    q_gain = column(qng_s[...] * (LOG2E * QK_DIM**-0.5))
    k_gain = column(kng_s[...])
    for i in range(3):
        v_s[i, VALUE_DIM:80, :] = jnp.ones((16, CHUNK), BF16)
    for t in range(4):
        q_s[t, QK_DIM:128, :] = jnp.ones((32, TILE), BF16)
    m_s[...] = jnp.full(m_s.shape, -1e30, F32)
    acc_s[...] = jnp.zeros(acc_s.shape, F32)
    values = x_s[...].astype(F32)
    mean_square = jnp.mean(values * values, axis=-1, keepdims=True)
    scaled = values * lax.rsqrt(mean_square + EPS) * ng_s[...]

    for c in nears:
        c.wait_recv()
    shift, scale = [
        jnp.concatenate([mods_s[i, j : j + 1, :] for i in range(4) for j in range(4 * k, 4 * k + 4)], axis=1)
        for k in range(2)
    ]
    normed = (scaled * (1.0 + scale) + shift).astype(BF16)

    def latent(w, gain_ref):
        y = dot(normed, w[...])
        m = jnp.mean(y * y, axis=-1, keepdims=True)
        return (y * lax.rsqrt(m + EPS) * gain_ref[...]).astype(BF16)

    rk = lax.dot_general(rd_s[...], normed, (((1,), (1,)), ((), ())), preferred_element_type=F32)
    rk_s[0] = rk.astype(BF16)
    kl_s[0] = latent(kvd_s, kvgain_s)
    ql_s[0] = latent(qd_s, qgain_s)
    latents = [[], [], [], []]
    for p, to in ((1, y_up), (2, y_down)):
        latents[p].append(send(kl_s.at[0], kl_s.at[p], s_kl.at[p], r_kl.at[p], to))
        latents[p].append(send(rk_s.at[0], rk_s.at[p], s_rk.at[p], r_rk.at[p], to))
        latents[p].append(send(ql_s.at[0], ql_s.at[p], s_ql.at[p], r_ql.at[p], to))

    q_copies, kv_copies, own_kv = {}, {}, []

    def expand(p):
        for c in latents[p][2:] if p == 2 else latents[p][:2] if p == 1 else latents[p]:
            c.wait_recv()
        cosine, sine = tables[p]
        rk = rk_s[p].astype(F32)
        rk_square = jnp.sum(rk * rk, axis=0, keepdims=True)
        q, kn, vv = dot(ql_s[p], qw_s[...]).T, dot(kl_s[p], kw_s[...]).T, dot(kl_s[p], vw_s[...]).T
        for j in range(4):
            qh = q[QK_DIM * j : QK_DIM * (j + 1)]
            inv = lax.rsqrt(jnp.sum(qh * qh, axis=0, keepdims=True) * (1.0 / QK_DIM) + EPS)
            qh = qh * inv * q_gain
            qh = jnp.concatenate([qh[:NOPE_DIM], turned(qh[NOPE_DIM:], cosine, sine)], axis=0)
            qkv_s[p, j, 0:QK_DIM, :] = qh.astype(BF16)
            kh = kn[NOPE_DIM * j : NOPE_DIM * (j + 1)]
            square = jnp.sum(kh * kh, axis=0, keepdims=True) + rk_square
            inv = lax.rsqrt(square * (1.0 / QK_DIM) + EPS)
            kr = turned(rk * inv * k_gain[NOPE_DIM:], cosine, sine)
            kh = kh * inv * k_gain[:NOPE_DIM]
            qkv_s[p, j, QK_DIM : QK_DIM + NOPE_DIM, :] = kh.astype(BF16)
            qkv_s[p, j, QK_DIM + NOPE_DIM : 2 * QK_DIM, :] = kr.astype(BF16)
            qkv_s[p, j, 2 * QK_DIM : 256, :] = vv[VALUE_DIM * j : VALUE_DIM * (j + 1)].astype(BF16)
        c = pltpu.make_async_copy(qkv_s.at[p, b, QK_DIM:256], kvs.at[0, 4 * p], block_sem.at[p])
        c.start()
        own_kv.append(c)
        for db in range(1, 4):
            r, block = 4 * p + db, qkv_s.at[p, lax.rem(b + db, 4)]
            q_copies[r] = send(block.at[0:QK_DIM], q_in.at[r], s_q.at[r], r_q.at[r], at(0, db, 0))
        for db in range(1, 4):
            r, block = 4 * p + db, qkv_s.at[p, lax.rem(b + db, 4)]
            kv_copies[r] = send(block.at[QK_DIM:256], kvs.at[0, r], s_kv.at[r], r_kv.at[r], at(0, db, 0))

    def place(chunk, first, blocks):
        for i, (slot, r) in enumerate(blocks):
            at_key = first + 128 * i
            block = kvs[slot, r]
            kt = jnp.concatenate([block[:QK_DIM].astype(F32), jnp.zeros((32, 128), F32)], axis=0)
            k_s[chunk % 3, at_key : at_key + 128, :] = kt.T.astype(BF16)
            v_s[chunk % 3, 0:VALUE_DIM, at_key : at_key + 128] = block[QK_DIM:]

    def take_queries(p):
        q_s[p, 0:QK_DIM, 0:128] = qkv_s[p, b, 0:QK_DIM]
        for db in range(1, 4):
            q_copies[4 * p + db].wait_recv()
            q_s[p, 0:QK_DIM, 128 * db : 128 * db + 128] = q_in[4 * p + db]

    ups, downs, far = {}, {}, {}

    def spread(g):
        own_kv[g].wait()
        for db in range(1, 4):
            kv_copies[4 * g + db].wait_recv()
        rows = pl.ds(4 * g, 4)
        ups[g] = send(kvs.at[0, rows], kvs.at[1, rows], s_up.at[g], r_up.at[g], a_up)
        downs[g] = send(kvs.at[0, rows], kvs.at[2, rows], s_down.at[g], r_down.at[g], a_down)

    def near(slot, g):
        (ups if slot == 1 else downs)[g].wait_recv()
        if (g < 2) == (slot == 1):
            rows, to = pl.ds(4 * g, 4), a_up if slot == 1 else a_down
            far[g] = send(kvs.at[slot, rows], kvs.at[3, rows], s_far.at[g], r_far.at[g], to)

    def rows_of(slot, *groups):
        return [(slot, 4 * g + i) for g in groups for i in range(4)]

    def share_weights(k):
        shared[k] = send(w_s.at[k, core], w_s.at[k, core], s_wc.at[k], r_wc.at[k], partner)

    def prepare(chunk):
        if chunk == 0:
            spread(0)
            place(0, 1024, rows_of(0, 0))
        elif chunk == 1:
            near(1, 0)
            place(1, 0, rows_of(0, 1, 2) + rows_of(1, 0))
        elif chunk == 2:
            near(1, 1)
            near(2, 2)
            near(2, 0)
            place(2, 0, rows_of(2, 0) + rows_of(0, 3) + rows_of(1, 1))
        elif chunk == 3:
            near(2, 3)
            near(1, 2)
            near(2, 1)
            place(3, 0, rows_of(2, 1, 2) + rows_of(1, 2))
            forward_weights(1)
            share_weights(1)
            share_weights(2)
        elif chunk == 4:
            near(1, 3)
            far[0].wait_recv()
            far[1].wait_recv()
            place(4, 0, rows_of(3, 0, 1) + rows_of(1, 3))
        else:
            far[2].wait_recv()
            far[3].wait_recv()
            place(5, 0, rows_of(3, 2, 3) + rows_of(2, 3))
            for c in weights_far:
                c.wait_recv()
            share_weights(3)

    def score(chunk, t, i):
        rows = slice(i * SUB, (i + 1) * SUB)
        s = dot(k_s[chunk % 3, rows], q_s[t])
        s_s[rows] = s
        return jnp.max(s.reshape(SUB // 8, 8, TILE), axis=0)

    def step(chunk, t, later_chunk, later):
        old = m_s[t]
        new = jnp.maximum(old, jnp.max(top_s[...], axis=0, keepdims=True))
        m_s[t] = new
        acc = acc_s[t] * jnp.exp2(old - new)
        top = None
        for i in range(STEPS):
            rows = slice(i * SUB, (i + 1) * SUB)
            p = jnp.exp2(s_s[rows] - new).astype(BF16)
            acc = acc + dot(v_s[chunk % 3, :, rows], p)
            if later is not None:
                part = score(later_chunk, later, i)
                top = part if top is None else jnp.maximum(top, part)
        acc_s[t] = acc
        if later is not None:
            top_s[...] = top

    att_copies = {}

    def finish(t):
        acc = acc_s[t]
        o = (acc[:VALUE_DIM] / acc[VALUE_DIM : VALUE_DIM + 1]).astype(BF16)
        for i in range(4):
            att_s[4 * t + i] = o[:, 128 * i : 128 * i + 128]

    def give(p):
        for db in range(4):
            r = 4 * p + db
            if r:
                att_copies[r] = send(
                    att_s.at[r], slots.at[OPPOSITE[p], b], s_att.at[r], r_att.at[r],
                    at(0, (4 - db) % 4, PIECE[p]),
                )
            else:
                slots[0, b] = att_s[0]

    expand(0)
    def own_head(w_ref):
        w = w_ref[...].astype(F32)
        w = jnp.where(b < 2, w[:, :128], w[:, 128:])
        return jnp.where(lax.rem(b, 2) == 0, w, pltpu.roll(w, 64, 1)).astype(BF16)

    for c in rest:
        c.wait_recv()
    clat = clat_s[...].reshape(1024, 256)
    kn = dot(clat, own_head(kw_s))
    lane = lax.broadcasted_iota(jnp.int32, (1, 128), 1)
    ropes = []
    for i in range(8):
        two = jnp.concatenate([crope_s[2 * i], crope_s[2 * i + 1]], axis=1).astype(F32)
        two = jnp.concatenate([jnp.zeros((64, 128), F32), two, jnp.zeros((32, 128), F32)], axis=0)
        ropes.append(two.T)
    key = jnp.where(lane < NOPE_DIM, kn, jnp.concatenate(ropes, axis=0))
    inv = lax.rsqrt(jnp.sum(key * key, axis=1, keepdims=True) * (1.0 / QK_DIM) + EPS)
    gain = jnp.concatenate([kng_s[...], jnp.zeros((1, 32), F32)], axis=1)
    lift = jnp.full((1, 128), lift_ref[b] * LOG2E, F32)
    high = lift.astype(BF16).astype(F32)
    middle = (lift - high).astype(BF16).astype(F32)
    low = lift - high - middle
    extra = jnp.where(lane == 96, high, jnp.where(lane == 97, middle, jnp.where(lane == 98, low, 0.0)))
    k_s[0, 0:1024, :] = (key * inv * gain + extra).astype(BF16)
    vv = dot(clat, own_head(vw_s)).T
    v_s[0, 0:VALUE_DIM, 0:1024] = vv[:VALUE_DIM].astype(BF16)

    for c in latents[2][:2]:
        c.wait_recv()
    latents[3].append(send(kl_s.at[2], kl_s.at[3], s_kl.at[3], r_kl.at[3], y_down))
    latents[3].append(send(rk_s.at[2], rk_s.at[3], s_rk.at[3], r_rk.at[3], y_down))
    latents[1][2].wait_recv()
    latents[3].append(send(ql_s.at[1], ql_s.at[3], s_ql.at[3], r_ql.at[3], y_up))
    weights_near(1)
    forward_weights(0)
    expand(1)
    expand(2)
    take_queries(0)
    prepare(0)
    top = None
    for i in range(STEPS):
        part = score(0, 0, i)
        top = part if top is None else jnp.maximum(top, part)
    top_s[...] = top
    take_queries(1)
    expand(3)
    step(0, 0, 0, 1)
    spread(1)
    spread(2)
    take_queries(2)
    step(0, 1, 0, 2)
    prepare(1)
    step(0, 2, 1, 0)
    step(1, 0, 1, 1)
    step(1, 1, 1, 2)
    take_queries(3)
    spread(3)
    step(1, 2, 0, 3)
    step(0, 3, 1, 3)
    prepare(2)
    step(1, 3, 2, 0)
    for chunk in range(2, 6):
        if chunk < 5:

            def some_tile(t, carry, chunk=chunk):
                step(chunk, t, chunk, t + 1)
                return carry

            lax.fori_loop(0, 3, some_tile, 0)
            prepare(chunk + 1)
            step(chunk, 3, chunk + 1, 0)
        else:
            for t in range(4):
                step(chunk, t, chunk, t + 1 if t < 3 else None)
                finish(t)
                if t:
                    give(t - 1)
            give(3)

    gate = [mods_s[i, j : j + 1, :] for i in range(4) for j in range(8, 12)]
    for p in range(4):
        k = OPPOSITE[p]
        for r in range(max(1, 4 * p), 4 * p + 4):
            att_copies[r].wait_recv()
        if p:
            shared[k].wait_recv()
        att = slots[k].reshape(256, 128).astype(F32).T.astype(BF16)
        for n in range(4):
            cols = slice(512 * n, 512 * n + 512)
            term = dot(att, w_s[k, :, :, cols].reshape(256, 512)).astype(BF16).astype(F32)
            if p:
                term = mixed_s[:, cols] + term
            if p < 3:
                mixed_s[:, cols] = term
            else:
                gated = jnp.concatenate(gate[4 * n : 4 * n + 4], axis=1)
                out_ref[:, cols] = (x_s[:, cols].astype(F32) + gated * term).astype(BF16)
    sent = nears + wides + rest + list(q_copies.values()) + list(kv_copies.values())
    sent += list(ups.values()) + list(downs.values()) + list(far.values()) + weights[0] + weights[1] + weights_far + list(shared.values()) + list(att_copies.values())
    for group in latents:
        sent += group
    for c in sent:
        c.wait_send()


def everything(*args):
    dma, vmem = pltpu.SemaphoreType.DMA, pltpu.VMEM
    hbm = pl.BlockSpec(memory_space=pltpu.HBM)
    return pl.pallas_call(
        kernel,
        out_shape=jax.ShapeDtypeStruct((128, 2048), BF16),
        in_specs=[hbm] * 19 + [pl.BlockSpec(memory_space=pltpu.SMEM)],
        out_specs=VMEM,
        scratch_shapes=[
            vmem((1, 128), BF16), vmem((3, 128, 512), BF16), vmem((1, 2048), F32), vmem((1, 512), F32),
            vmem((1, 256), F32), vmem((1, 96), F32), vmem((1, 96), F32),
            vmem((128, 2048), BF16), vmem((2048, 512), BF16), vmem((2048, 256), BF16), vmem((32, 2048), BF16),
            vmem((512, 384), BF16), vmem((256, 256), BF16), vmem((256, 256), BF16),
            vmem((16, 64, 256), BF16), vmem((16, 32, 64), BF16),
            vmem((16, 128), F32), vmem((16, 16, 128), F32), vmem((4, 16, 128), F32),
            vmem((4, 128, 512), BF16), vmem((4, 128, 256), BF16), vmem((4, 32, 128), BF16),
            vmem((4, 4, 256, 128), BF16), vmem((16, QK_DIM, 128), BF16), vmem((4, 16, 160, 128), BF16),
            vmem((4, 128, TILE), BF16), vmem((3, CHUNK, 128), BF16), vmem((3, 80, CHUNK), BF16),
            vmem((CHUNK, TILE), F32), vmem((4, 1, TILE), F32), vmem((8, TILE), F32), vmem((4, 80, TILE), F32),
            vmem((16, VALUE_DIM, 128), BF16), vmem((4, 4, VALUE_DIM, 128), BF16), vmem((4, 2, 128, 2048), BF16),
            vmem((128, 2048), F32),
            dma((4,)), dma((4,)), dma((16,)), dma((16,)), dma((16,)), dma((16,)), dma((16,)), dma((16,)),
            dma((4,)), dma((4,)), dma((4,)), dma((4,)), dma((4,)), dma((4,)),
            dma((16,)), dma((16,)), dma((16,)), dma((16,)),
            dma((4,)), dma((4,)), dma((4,)), dma((4,)), dma((4,)), dma((4,)), dma((16,)), dma((16,)),
            dma((6,)), dma((6,)), dma((4,)), dma((4,)), dma((21,)), dma((4,)),
        ],
        compiler_params=pltpu.CompilerParams(
            collective_id=0, has_side_effects=True, vmem_limit_bytes=67_043_328
        ),
        cost_estimate=pl.CostEstimate(
            flops=10_000_000_000, bytes_accessed=8_000_000, transcendentals=19_000_000
        ),
        name="everything",
    )(*args)


def local(
    latent_tokens, condition, shift_weight, scale_weight, gate_weight, norm_gain, query_down, query_gain,
    kv_down, kv_gain, rope_down, query_up, key_up, value_up, query_norm_gain, key_norm_gain, out_weight,
    context_latent, context_rope, context_lift,
):
    return everything(
        condition.reshape(1, 128), shift_weight, scale_weight, gate_weight,
        norm_gain.reshape(1, -1), query_gain.reshape(1, -1), kv_gain.reshape(1, -1),
        query_norm_gain.reshape(1, -1), key_norm_gain.reshape(1, -1),
        latent_tokens, query_down, kv_down, rope_down.T, query_up, key_up, value_up,
        context_latent, context_rope.T, out_weight, context_lift,
    )


def solution(mesh):
    in_specs = (
        P(("dp", "sp", "tp"), None), P(("dp", "sp")), P("sp", "tp"), P("sp", "tp"), P("sp", "tp"),
        P(), P(), P(), P(), P(), P(), P(None, "tp"), P(None, "tp"), P(None, "tp"), P(), P(),
        P("tp", None), P(("dp", "sp"), None), P(("dp", "sp"), None), P("tp"),
    )
    return jax.shard_map(
        local, mesh=mesh, in_specs=in_specs, out_specs=P(("dp", "sp", "tp"), None), check_vma=False
    )
```

```python
import jax
import jax.numpy as jnp
from jax import lax
from jax.experimental import pallas as pl
from jax.experimental.pallas import tpu as pltpu
from jax.sharding import PartitionSpec as P

NOPE_DIM = 64
ROPE_DIM = 32
VALUE_DIM = 64
QK_DIM = 96
GRID_W = 64
EPS = 1e-06
THETA = 10000.0
LOG2E = 1.4426950408889634

F32 = jnp.float32
BF16 = jnp.bfloat16
MESH = pl.DeviceIdType.MESH
VMEM = pl.BlockSpec(memory_space=pltpu.VMEM)


CHUNK = 1536
TILE = 512
SUB = 256
STEPS = CHUNK // SUB
PIECE = (0, 3, 1, 2)
OPPOSITE = (0, 2, 1, 3)


def send(src, dst, send_sem, recv_sem, to):
    c = pltpu.make_async_remote_copy(
        src_ref=src, dst_ref=dst, send_sem=send_sem, recv_sem=recv_sem, device_id=to, device_id_type=MESH
    )
    c.start()
    return c


def dot(a, b):
    return jnp.dot(a, b, preferred_element_type=F32)


def turned(rows, cosine, sine):
    out = []
    for a in range(2):
        u, w = rows[16 * a : 16 * a + 8], rows[16 * a + 8 : 16 * a + 16]
        out += [u * cosine[a] - w * sine[a], w * cosine[a] + u * sine[a]]
    return jnp.concatenate(out, axis=0)


def column(row):
    row = jnp.concatenate([row, jnp.zeros((1, 32), F32)], axis=1)
    return jnp.broadcast_to(row, (128, 128)).T[:QK_DIM]


def kernel(
    cond_hbm, shift_hbm, scale_hbm, gate_hbm, ng_hbm, qgain_hbm, kvgain_hbm, qng_hbm, kng_hbm,
    x_hbm, qd_hbm, kvd_hbm, rd_hbm, qw_hbm, kw_hbm, vw_hbm, lat_hbm, rope_hbm, wout_hbm, lift_ref,
    out_ref,
    cond_s, mw_s, ng_s, qgain_s, kvgain_s, qng_s, kng_s,
    x_s, qd_s, kvd_s, rd_s, qw_s, kw_s, vw_s, clat_s, crope_s,
    part_s, wide_s, mods_s, ql_s, kl_s, rk_s,
    qkv_s, q_in, kvs, q_s, k_s, v_s, s_s, m_s, top_s, acc_s, att_s, slots, w_s, mixed_s,
    s_near, r_near, s_wide, r_wide, s_lat, r_lat, s_rope, r_rope,
    s_ql, r_ql, s_kl, r_kl, s_rk, r_rk, s_q, r_q, s_kv, r_kv,
    s_up, r_up, s_down, r_down, s_far, r_far, s_att, r_att, s_w, r_w, s_wc, r_wc, local_sem, block_sem,
):
    sp, tp, core = lax.axis_index("sp"), lax.axis_index("tp"), lax.axis_index("dp")
    z, x = sp // 4, lax.rem(sp, 4)
    a, b = z + core * (x - z), x + core * (z - x)

    def at(da, db, dy):
        aa, bb = lax.rem(a + da, 4), lax.rem(b + db, 4)
        return {"sp": aa * (4 - 3 * core) + bb * (1 + 3 * core), "tp": lax.rem(tp + dy, 4)}

    def along_tp(k):
        return {"tp": lax.rem(tp + k, 4)}

    def along_sp(r):
        return {"sp": lax.rem(sp + r, 16)}

    partner, y_up, y_down = {"dp": 1 - core}, along_tp(1), along_tp(3)
    a_up, a_down = at(1, 0, 0), at(3, 0, 0)
    barrier = pltpu.get_barrier_semaphore()
    greeted = [along_tp(k) for k in range(1, 4)] + [along_sp(r) for r in range(1, 16)] + [partner]
    greeted += [at(0, db, dy) for dy in range(1, 4) for db in range(1, 4)]
    for to in greeted:
        pl.semaphore_signal(barrier, inc=1, device_id=to, device_id_type=MESH)
    own = []

    def fetch(src, dst):
        c = pltpu.make_async_copy(src, dst, local_sem.at[len(own)])
        c.start()
        own.append(c)

    for src, dst in (
        (cond_hbm, cond_s), (shift_hbm, mw_s.at[0]), (scale_hbm, mw_s.at[1]), (gate_hbm, mw_s.at[2]),
        (qng_hbm, qng_s), (kng_hbm, kng_s), (x_hbm, x_s), (ng_hbm, ng_s),
        (qd_hbm, qd_s), (kvd_hbm, kvd_s), (rd_hbm, rd_s), (qgain_hbm, qgain_s), (kvgain_hbm, kvgain_s),
        (qw_hbm, qw_s), (kw_hbm, kw_s), (vw_hbm, vw_s), (lat_hbm, clat_s.at[0]), (rope_hbm, crope_s.at[0]),
        (wout_hbm.at[0:128], w_s.at[0, 0]), (wout_hbm.at[128:256], w_s.at[0, 1]),
    ):
        fetch(src, dst)

    for c in own[:4]:
        c.wait()
    cond = cond_s[...].astype(F32)
    active = cond / (1.0 + jnp.exp(-cond))
    active = jnp.broadcast_to(active, (16, 128)).astype(BF16)
    for i in range(3):
        row = dot(active, mw_s[i])
        for j in range(4):
            piece = row[0:1, 128 * j : 128 * j + 128]
            part_s[4 * i + j : 4 * i + j + 1, :] = piece
    part_s[12:16, :] = jnp.zeros((4, 128), F32)
    pl.semaphore_wait(barrier, len(greeted))

    weights = [[], []]

    def weights_near(part):
        rows, src = pl.ds(64 * part, 64), wout_hbm.at[pl.ds(core * 128 + 64 * part, 64)]
        i = 2 * part
        weights[part].append(send(src, w_s.at[1, core, rows], s_w.at[i], r_w.at[i], y_up))
        weights[part].append(send(src, w_s.at[2, core, rows], s_w.at[i + 1], r_w.at[i + 1], y_down))

    weights_far, shared = [], {}

    def forward_weights(part):
        for c in weights[part]:
            c.wait_recv()
        rows = pl.ds(64 * part, 64)
        to = y_down if part else y_up
        weights_far.append(
            send(w_s.at[1 + part, core, rows], w_s.at[3, core, rows], s_w.at[4 + part], r_w.at[4 + part], to)
        )

    wides, nears, rest = [], [], []
    for r in range(1, 16):
        wides.append(send(part_s, wide_s.at[r], s_wide.at[r], r_wide.at[r], along_sp(r)))
    total = part_s[...]
    for r in range(1, 16):
        wides[r - 1].wait_recv()
        total = total + wide_s[r]
    mods_s[tp] = total
    for k in range(1, 4):
        nears.append(send(mods_s.at[tp], mods_s.at[tp], s_near.at[k], r_near.at[k], along_tp(k)))
    weights_near(0)
    for r in range(1, 16):
        rest.append(send(lat_hbm, clat_s.at[r], s_lat.at[r], r_lat.at[r], along_sp(r)))
        rest.append(send(rope_hbm, crope_s.at[r], s_rope.at[r], r_rope.at[r], along_sp(r)))

    for c in own[4:]:
        c.wait()
    lane = lax.broadcasted_iota(jnp.int32, (8, 128), 1)
    which = lax.broadcasted_iota(jnp.int32, (8, 128), 0)
    frequency = jnp.full((8, 128), 1.0, F32)
    for f in range(1, 8):
        frequency = jnp.where(which == f, THETA ** (-4.0 * f / ROPE_DIM), frequency)
    column_angle = lax.rem(lane, GRID_W).astype(F32) * frequency
    column_cosine, column_sine = jnp.cos(column_angle), jnp.sin(column_angle)
    tables = []
    for p in range(4):
        row = (sp * 4 + lax.rem(tp + PIECE[p], 4)) * 2 + lane // GRID_W
        angle = row.astype(F32) * frequency
        tables.append(((jnp.cos(angle), column_cosine), (jnp.sin(angle), column_sine)))
    q_gain = column(qng_s[...] * (LOG2E * QK_DIM**-0.5))
    k_gain = column(kng_s[...])
    for i in range(3):
        v_s[i, VALUE_DIM:80, :] = jnp.ones((16, CHUNK), BF16)
    for t in range(4):
        q_s[t, QK_DIM:128, :] = jnp.ones((32, TILE), BF16)
    m_s[...] = jnp.full(m_s.shape, -1e30, F32)
    acc_s[...] = jnp.zeros(acc_s.shape, F32)
    values = x_s[...].astype(F32)
    mean_square = jnp.mean(values * values, axis=-1, keepdims=True)
    scaled = values * lax.rsqrt(mean_square + EPS) * ng_s[...]

    for c in nears:
        c.wait_recv()
    shift, scale = [
        jnp.concatenate([mods_s[i, j : j + 1, :] for i in range(4) for j in range(4 * k, 4 * k + 4)], axis=1)
        for k in range(2)
    ]
    normed = (scaled * (1.0 + scale) + shift).astype(BF16)

    def latent(w, gain_ref):
        y = dot(normed, w[...])
        m = jnp.mean(y * y, axis=-1, keepdims=True)
        return (y * lax.rsqrt(m + EPS) * gain_ref[...]).astype(BF16)

    rk = lax.dot_general(rd_s[...], normed, (((1,), (1,)), ((), ())), preferred_element_type=F32)
    rk_s[0] = rk.astype(BF16)
    kl_s[0] = latent(kvd_s, kvgain_s)
    ql_s[0] = latent(qd_s, qgain_s)
    latents = [[], [], [], []]
    for p, to in ((1, y_up), (2, y_down)):
        latents[p].append(send(kl_s.at[0], kl_s.at[p], s_kl.at[p], r_kl.at[p], to))
        latents[p].append(send(rk_s.at[0], rk_s.at[p], s_rk.at[p], r_rk.at[p], to))
        latents[p].append(send(ql_s.at[0], ql_s.at[p], s_ql.at[p], r_ql.at[p], to))

    q_copies, kv_copies, own_kv = {}, {}, []

    def expand(p):
        for c in latents[p][2:] if p == 2 else latents[p][:2] if p == 1 else latents[p]:
            c.wait_recv()
        cosine, sine = tables[p]
        rk = rk_s[p].astype(F32)
        rk_square = jnp.sum(rk * rk, axis=0, keepdims=True)
        q, kn, vv = dot(ql_s[p], qw_s[...]).T, dot(kl_s[p], kw_s[...]).T, dot(kl_s[p], vw_s[...]).T
        for j in range(4):
            qh = q[QK_DIM * j : QK_DIM * (j + 1)]
            inv = lax.rsqrt(jnp.sum(qh * qh, axis=0, keepdims=True) * (1.0 / QK_DIM) + EPS)
            qh = qh * inv * q_gain
            qh = jnp.concatenate([qh[:NOPE_DIM], turned(qh[NOPE_DIM:], cosine, sine)], axis=0)
            qkv_s[p, j, 0:QK_DIM, :] = qh.astype(BF16)
            kh = kn[NOPE_DIM * j : NOPE_DIM * (j + 1)]
            square = jnp.sum(kh * kh, axis=0, keepdims=True) + rk_square
            inv = lax.rsqrt(square * (1.0 / QK_DIM) + EPS)
            kr = turned(rk * inv * k_gain[NOPE_DIM:], cosine, sine)
            kh = kh * inv * k_gain[:NOPE_DIM]
            qkv_s[p, j, QK_DIM : QK_DIM + NOPE_DIM, :] = kh.astype(BF16)
            qkv_s[p, j, QK_DIM + NOPE_DIM : 2 * QK_DIM, :] = kr.astype(BF16)
            qkv_s[p, j, 2 * QK_DIM : 256, :] = vv[VALUE_DIM * j : VALUE_DIM * (j + 1)].astype(BF16)
        c = pltpu.make_async_copy(qkv_s.at[p, b, QK_DIM:256], kvs.at[0, 4 * p], block_sem.at[p])
        c.start()
        own_kv.append(c)
        for db in range(1, 4):
            r, block = 4 * p + db, qkv_s.at[p, lax.rem(b + db, 4)]
            q_copies[r] = send(block.at[0:QK_DIM], q_in.at[r], s_q.at[r], r_q.at[r], at(0, db, 0))
        for db in range(1, 4):
            r, block = 4 * p + db, qkv_s.at[p, lax.rem(b + db, 4)]
            kv_copies[r] = send(block.at[QK_DIM:256], kvs.at[0, r], s_kv.at[r], r_kv.at[r], at(0, db, 0))

    def place(chunk, first, blocks):
        for i, (slot, r) in enumerate(blocks):
            at_key = first + 128 * i
            block = kvs[slot, r]
            kt = jnp.concatenate([block[:QK_DIM].astype(F32), jnp.zeros((32, 128), F32)], axis=0)
            k_s[chunk % 3, at_key : at_key + 128, :] = kt.T.astype(BF16)
            v_s[chunk % 3, 0:VALUE_DIM, at_key : at_key + 128] = block[QK_DIM:]

    def take_queries(p):
        q_s[p, 0:QK_DIM, 0:128] = qkv_s[p, b, 0:QK_DIM]
        for db in range(1, 4):
            q_copies[4 * p + db].wait_recv()
            q_s[p, 0:QK_DIM, 128 * db : 128 * db + 128] = q_in[4 * p + db]

    ups, downs, far = {}, {}, {}

    def spread(g):
        own_kv[g].wait()
        for db in range(1, 4):
            kv_copies[4 * g + db].wait_recv()
        rows = pl.ds(4 * g, 4)
        ups[g] = send(kvs.at[0, rows], kvs.at[1, rows], s_up.at[g], r_up.at[g], a_up)
        downs[g] = send(kvs.at[0, rows], kvs.at[2, rows], s_down.at[g], r_down.at[g], a_down)

    def near(slot, g):
        (ups if slot == 1 else downs)[g].wait_recv()
        if (g < 2) == (slot == 1):
            rows, to = pl.ds(4 * g, 4), a_up if slot == 1 else a_down
            far[g] = send(kvs.at[slot, rows], kvs.at[3, rows], s_far.at[g], r_far.at[g], to)

    def rows_of(slot, *groups):
        return [(slot, 4 * g + i) for g in groups for i in range(4)]

    def share_weights(k):
        shared[k] = send(w_s.at[k, core], w_s.at[k, core], s_wc.at[k], r_wc.at[k], partner)

    def prepare(chunk):
        if chunk == 0:
            spread(0)
            place(0, 1024, rows_of(0, 0))
        elif chunk == 1:
            near(1, 0)
            place(1, 0, rows_of(0, 1, 2) + rows_of(1, 0))
        elif chunk == 2:
            near(1, 1)
            near(2, 2)
            near(2, 0)
            place(2, 0, rows_of(2, 0) + rows_of(0, 3) + rows_of(1, 1))
        elif chunk == 3:
            near(2, 3)
            near(1, 2)
            near(2, 1)
            place(3, 0, rows_of(2, 1, 2) + rows_of(1, 2))
            forward_weights(1)
            share_weights(1)
            share_weights(2)
        elif chunk == 4:
            near(1, 3)
            far[0].wait_recv()
            far[1].wait_recv()
            place(4, 0, rows_of(3, 0, 1) + rows_of(1, 3))
        else:
            far[2].wait_recv()
            far[3].wait_recv()
            place(5, 0, rows_of(3, 2, 3) + rows_of(2, 3))
            for c in weights_far:
                c.wait_recv()
            share_weights(3)

    def score(chunk, t, i):
        rows = slice(i * SUB, (i + 1) * SUB)
        s = dot(k_s[chunk % 3, rows], q_s[t])
        s_s[rows] = s
        return jnp.max(s.reshape(SUB // 8, 8, TILE), axis=0)

    def step(chunk, t, later_chunk, later):
        old = m_s[t]
        new = jnp.maximum(old, jnp.max(top_s[...], axis=0, keepdims=True))
        m_s[t] = new
        acc = acc_s[t] * jnp.exp2(old - new)
        top = None
        for i in range(STEPS):
            rows = slice(i * SUB, (i + 1) * SUB)
            p = jnp.exp2(s_s[rows] - new).astype(BF16)
            acc = acc + dot(v_s[chunk % 3, :, rows], p)
            if later is not None:
                part = score(later_chunk, later, i)
                top = part if top is None else jnp.maximum(top, part)
        acc_s[t] = acc
        if later is not None:
            top_s[...] = top

    att_copies = {}

    def finish(t):
        acc = acc_s[t]
        o = (acc[:VALUE_DIM] / acc[VALUE_DIM : VALUE_DIM + 1]).astype(BF16)
        for i in range(4):
            att_s[4 * t + i] = o[:, 128 * i : 128 * i + 128]

    def give(p):
        for db in range(4):
            r = 4 * p + db
            if r:
                att_copies[r] = send(
                    att_s.at[r], slots.at[OPPOSITE[p], b], s_att.at[r], r_att.at[r],
                    at(0, (4 - db) % 4, PIECE[p]),
                )
            else:
                slots[0, b] = att_s[0]

    expand(0)
    def own_head(w_ref):
        w = w_ref[...].astype(F32)
        w = jnp.where(b < 2, w[:, :128], w[:, 128:])
        return jnp.where(lax.rem(b, 2) == 0, w, pltpu.roll(w, 64, 1)).astype(BF16)

    for c in rest:
        c.wait_recv()
    clat = clat_s[...].reshape(1024, 256)
    kn = dot(clat, own_head(kw_s))
    lane = lax.broadcasted_iota(jnp.int32, (1, 128), 1)
    ropes = []
    for i in range(8):
        two = jnp.concatenate([crope_s[2 * i], crope_s[2 * i + 1]], axis=1).astype(F32)
        two = jnp.concatenate([jnp.zeros((64, 128), F32), two, jnp.zeros((32, 128), F32)], axis=0)
        ropes.append(two.T)
    key = jnp.where(lane < NOPE_DIM, kn, jnp.concatenate(ropes, axis=0))
    inv = lax.rsqrt(jnp.sum(key * key, axis=1, keepdims=True) * (1.0 / QK_DIM) + EPS)
    gain = jnp.concatenate([kng_s[...], jnp.zeros((1, 32), F32)], axis=1)
    lift = jnp.full((1, 128), lift_ref[b] * LOG2E, F32)
    high = lift.astype(BF16).astype(F32)
    middle = (lift - high).astype(BF16).astype(F32)
    low = lift - high - middle
    extra = jnp.where(lane == 96, high, jnp.where(lane == 97, middle, jnp.where(lane == 98, low, 0.0)))
    k_s[0, 0:1024, :] = (key * inv * gain + extra).astype(BF16)
    vv = dot(clat, own_head(vw_s)).T
    v_s[0, 0:VALUE_DIM, 0:1024] = vv[:VALUE_DIM].astype(BF16)

    for c in latents[2][:2]:
        c.wait_recv()
    latents[3].append(send(kl_s.at[2], kl_s.at[3], s_kl.at[3], r_kl.at[3], y_down))
    latents[3].append(send(rk_s.at[2], rk_s.at[3], s_rk.at[3], r_rk.at[3], y_down))
    latents[1][2].wait_recv()
    latents[3].append(send(ql_s.at[1], ql_s.at[3], s_ql.at[3], r_ql.at[3], y_up))
    weights_near(1)
    forward_weights(0)
    expand(1)
    expand(2)
    take_queries(0)
    prepare(0)
    top = None
    for i in range(STEPS):
        part = score(0, 0, i)
        top = part if top is None else jnp.maximum(top, part)
    top_s[...] = top
    take_queries(1)
    expand(3)
    step(0, 0, 0, 1)
    spread(1)
    spread(2)
    take_queries(2)
    step(0, 1, 0, 2)
    prepare(1)
    step(0, 2, 1, 0)
    step(1, 0, 1, 1)
    step(1, 1, 1, 2)
    take_queries(3)
    spread(3)
    step(1, 2, 0, 3)
    step(0, 3, 1, 3)
    prepare(2)
    step(1, 3, 2, 0)
    for chunk in range(2, 6):
        if chunk < 5:

            def some_tile(t, carry, chunk=chunk):
                step(chunk, t, chunk, t + 1)
                return carry

            lax.fori_loop(0, 3, some_tile, 0)
            prepare(chunk + 1)
            step(chunk, 3, chunk + 1, 0 if chunk < 4 else 3)
        else:
            order = (3, 1, 2, 0)
            for i, t in enumerate(order):
                step(chunk, t, chunk, order[i + 1] if i < 3 else None)
                finish(t)
                if i:
                    give(order[i - 1])
            give(0)

    gate = [mods_s[i, j : j + 1, :] for i in range(4) for j in range(8, 12)]
    for done, p in enumerate((3, 1, 2, 0)):
        k = OPPOSITE[p]
        for r in range(max(1, 4 * p), 4 * p + 4):
            att_copies[r].wait_recv()
        if p:
            shared[k].wait_recv()
        att = slots[k].reshape(256, 128).astype(F32).T.astype(BF16)
        for n in range(4):
            cols = slice(512 * n, 512 * n + 512)
            term = dot(att, w_s[k, :, :, cols].reshape(256, 512)).astype(BF16).astype(F32)
            if done:
                term = mixed_s[:, cols] + term
            if done < 3:
                mixed_s[:, cols] = term
            else:
                gated = jnp.concatenate(gate[4 * n : 4 * n + 4], axis=1)
                out_ref[:, cols] = (x_s[:, cols].astype(F32) + gated * term).astype(BF16)
    sent = nears + wides + rest + list(q_copies.values()) + list(kv_copies.values())
    sent += list(ups.values()) + list(downs.values()) + list(far.values()) + weights[0] + weights[1] + weights_far + list(shared.values()) + list(att_copies.values())
    for group in latents:
        sent += group
    for c in sent:
        c.wait_send()


def everything(*args):
    dma, vmem = pltpu.SemaphoreType.DMA, pltpu.VMEM
    hbm = pl.BlockSpec(memory_space=pltpu.HBM)
    return pl.pallas_call(
        kernel,
        out_shape=jax.ShapeDtypeStruct((128, 2048), BF16),
        in_specs=[hbm] * 19 + [pl.BlockSpec(memory_space=pltpu.SMEM)],
        out_specs=VMEM,
        scratch_shapes=[
            vmem((1, 128), BF16), vmem((3, 128, 512), BF16), vmem((1, 2048), F32), vmem((1, 512), F32),
            vmem((1, 256), F32), vmem((1, 96), F32), vmem((1, 96), F32),
            vmem((128, 2048), BF16), vmem((2048, 512), BF16), vmem((2048, 256), BF16), vmem((32, 2048), BF16),
            vmem((512, 384), BF16), vmem((256, 256), BF16), vmem((256, 256), BF16),
            vmem((16, 64, 256), BF16), vmem((16, 32, 64), BF16),
            vmem((16, 128), F32), vmem((16, 16, 128), F32), vmem((4, 16, 128), F32),
            vmem((4, 128, 512), BF16), vmem((4, 128, 256), BF16), vmem((4, 32, 128), BF16),
            vmem((4, 4, 256, 128), BF16), vmem((16, QK_DIM, 128), BF16), vmem((4, 16, 160, 128), BF16),
            vmem((4, 128, TILE), BF16), vmem((3, CHUNK, 128), BF16), vmem((3, 80, CHUNK), BF16),
            vmem((CHUNK, TILE), F32), vmem((4, 1, TILE), F32), vmem((8, TILE), F32), vmem((4, 80, TILE), F32),
            vmem((16, VALUE_DIM, 128), BF16), vmem((4, 4, VALUE_DIM, 128), BF16), vmem((4, 2, 128, 2048), BF16),
            vmem((128, 2048), F32),
            dma((4,)), dma((4,)), dma((16,)), dma((16,)), dma((16,)), dma((16,)), dma((16,)), dma((16,)),
            dma((4,)), dma((4,)), dma((4,)), dma((4,)), dma((4,)), dma((4,)),
            dma((16,)), dma((16,)), dma((16,)), dma((16,)),
            dma((4,)), dma((4,)), dma((4,)), dma((4,)), dma((4,)), dma((4,)), dma((16,)), dma((16,)),
            dma((6,)), dma((6,)), dma((4,)), dma((4,)), dma((21,)), dma((4,)),
        ],
        compiler_params=pltpu.CompilerParams(
            collective_id=0, has_side_effects=True, vmem_limit_bytes=67_043_328
        ),
        cost_estimate=pl.CostEstimate(
            flops=10_000_000_000, bytes_accessed=8_000_000, transcendentals=19_000_000
        ),
        name="everything",
    )(*args)


def local(
    latent_tokens, condition, shift_weight, scale_weight, gate_weight, norm_gain, query_down, query_gain,
    kv_down, kv_gain, rope_down, query_up, key_up, value_up, query_norm_gain, key_norm_gain, out_weight,
    context_latent, context_rope, context_lift,
):
    return everything(
        condition.reshape(1, 128), shift_weight, scale_weight, gate_weight,
        norm_gain.reshape(1, -1), query_gain.reshape(1, -1), kv_gain.reshape(1, -1),
        query_norm_gain.reshape(1, -1), key_norm_gain.reshape(1, -1),
        latent_tokens, query_down, kv_down, rope_down.T, query_up, key_up, value_up,
        context_latent, context_rope.T, out_weight, context_lift,
    )


def solution(mesh):
    in_specs = (
        P(("dp", "sp", "tp"), None), P(("dp", "sp")), P("sp", "tp"), P("sp", "tp"), P("sp", "tp"),
        P(), P(), P(), P(), P(), P(), P(None, "tp"), P(None, "tp"), P(None, "tp"), P(), P(),
        P("tp", None), P(("dp", "sp"), None), P(("dp", "sp"), None), P("tp"),
    )
    return jax.shard_map(
        local, mesh=mesh, in_specs=in_specs, out_specs=P(("dp", "sp", "tp"), None), check_vma=False
    )
```
